128 devices in a mesh: sp: 16 (over z, y), tp: 8 (over x, core).
Axes of the slice: x: 4, y: 4, z: 4, core: 2. Of those that a mesh axis runs over, the one named last changes fastest.
Arguments:
- layer_input_rows: bfloat16 [4096, 2048], P('sp'), may hold values from -6 to 6
- input_norm_gain: float32 [2048], replicated, may hold values from 0.1 to 1.9
- query_weight: bfloat16 [2048, 1024], P(None, 'tp'), may hold values from -0.125 to 0.125
- key_weight: bfloat16 [2048, 1024], P(None, 'tp'), may hold values from -0.125 to 0.125
- value_weight: bfloat16 [2048, 1024], P(None, 'tp'), may hold values from -0.125 to 0.125
- query_norm_gain: float32 [64], replicated, may hold values from 0.5 to 9
- key_norm_gain: float32 [64], replicated, may hold values from 0.5 to 9
- cumulative_gate: float32 [4096, 16], P('sp', 'tp'), may hold values from -575.44 to 0, as said below
- attention_norm_gain: float32 [1024], P('tp'), may hold values from 0.1 to 1.9
- recurrence_query_weight: bfloat16 [2048, 1024], P(None, 'tp'), may hold values from -0.125 to 0.125
- forget_weight: bfloat16 [2048, 1024], P(None, 'tp'), may hold values from -0.125 to 0.125
- recurrence_value_weight: bfloat16 [2048, 1024], P(None, 'tp'), may hold values from -0.125 to 0.125
- output_gate_weight: bfloat16 [2048, 1024], P(None, 'tp'), may hold values from -0.125 to 0.125
- gate_lower_slack: float32 [1024], P('tp'), may hold values from 0 to 0.06
- extra_log_decay: float32 [4096, 8], P('sp', 'tp'), may hold values from -1.5 to 0
- recurrence_norm_gain: float32 [1024], P('tp'), may hold values from 0.1 to 1.9
- attention_output_weight: bfloat16 [1024, 2048], P('tp'), may hold values from -0.125 to 0.125
- recurrence_output_weight: bfloat16 [1024, 2048], P('tp'), may hold values from -0.125 to 0.125
Outputs:
- mixed: bfloat16 [4096, 2048], P(('sp', 'tp'))
- log_sum: float32 [4096, 16], P('sp', 'tp')
The draws below stay inside these ranges and needn't reach their ends.
Inputs may be any that keep to these rules, and one draw needn't show every extreme that they name: `cumulative_gate`: each column never rises along positions.
All inputs are finite; a program needn't handle non-finite values.
Results may differ from the reference program's by a relative error of at most 0.015.
The reference program's roundings to bfloat16 on the way count: a program that leaves them out, or rounds other values in their place, can miss the bound.
Values may be sent and summed in bfloat16 or wider, within the bound.
A program may use at most 64 MiB of HBM per device.

```python
import math
import jax
import jax.numpy as jnp
from jax import lax

D = 2048
ATT_HEADS = 16
HEAD_DIM = 64
RECURRENCE_HEADS = 8
STATE_ROWS = 128
VAL_DIM = 128
BLOCK = 64
TOKEN_COUNT = 4096
N_TP = 8


def gain_draw(base_key, salt_value):
    subkey = jax.random.fold_in(base_key, salt_value)
    return 1.0 + 0.18 * jax.random.truncated_normal(subkey, -2.5, 2.5, (HEAD_DIM,), jnp.float32)


def draw_query_norm_gain(key, part):
    return gain_draw(key, 11)


def draw_key_norm_gain(key, part):
    return gain_draw(key, 12)


def rough_logs(base_key, head_number, rates):
    random_subkeys = jax.random.split(base_key, 4)
    position_index = jnp.arange(TOKEN_COUNT, dtype=jnp.int32)
    block_of = position_index * 32 // TOKEN_COUNT
    factors = jnp.exp(jax.random.uniform(random_subkeys[0], (32, head_number), jnp.float32, -0.7, 0.7))
    block_scale = jnp.take(factors, block_of, axis=0)
    roughness = jax.random.uniform(random_subkeys[1], (TOKEN_COUNT, head_number), jnp.float32, 0.0, 2.0)
    logit_values = -rates[None, :] * block_scale * roughness
    spike_position = jax.random.randint(random_subkeys[2], (2, head_number), 0, TOKEN_COUNT)
    spike_depth = jnp.log(jax.random.uniform(random_subkeys[3], (2, head_number), jnp.float32, 0.5, 0.8))
    spike_hits = (position_index[:, None, None] == spike_position[None]).astype(jnp.float32)
    return logit_values + jnp.sum(spike_hits * spike_depth[None], axis=1)


def draw_cumulative_gate(key, part):
    random_subkeys = jax.random.split(jax.random.fold_in(key, 21), 4)
    ranking = jax.random.permutation(random_subkeys[0], ATT_HEADS)
    fast_count = ATT_HEADS // 2
    slow_heads = ranking >= fast_count
    slow_rate = jnp.exp(jax.random.uniform(random_subkeys[1], (ATT_HEADS,), jnp.float32, -0.69, 0.69)) / TOKEN_COUNT
    fast_rate = jnp.exp(jax.random.uniform(random_subkeys[2], (ATT_HEADS,), jnp.float32, -4.6, -3.4))
    rates = jnp.where(slow_heads, slow_rate, fast_rate)
    return jnp.cumsum(rough_logs(random_subkeys[3], ATT_HEADS, rates), axis=0)


def draw_extra_log_decay(key, part):
    random_subkeys = jax.random.split(jax.random.fold_in(key, 31), 2)
    rates = jnp.exp(jax.random.uniform(random_subkeys[0], (RECURRENCE_HEADS,), jnp.float32, -2.3, -0.22)) / TOKEN_COUNT
    return rough_logs(random_subkeys[1], RECURRENCE_HEADS, rates)


def draw_gate_lower_slack(key, part):
    random_subkeys = jax.random.split(jax.random.fold_in(key, 41), 3)
    channels = RECURRENCE_HEADS * STATE_ROWS
    ranking = jax.random.permutation(random_subkeys[0], channels)
    fast_count = channels // 2
    slow_rows = ranking >= fast_count
    slow_gap = jnp.exp(jax.random.uniform(random_subkeys[1], (channels,), jnp.float32, -1.6, 0.0)) / TOKEN_COUNT
    fast_gap = jnp.exp(jax.random.uniform(random_subkeys[2], (channels,), jnp.float32, -3.9, -2.82))
    return jnp.where(slow_rows, slow_gap, fast_gap)


def steps_of(rng, shape, cuts, smallest, high):
    loudness = 1.0
    for axis_at, parts in cuts:
        steps = jax.random.uniform(jax.random.fold_in(jax.random.fold_in(rng, 6), axis_at), (parts,), jnp.float32, smallest / len(cuts), high / len(cuts))
        loudness = loudness * jnp.repeat(jnp.exp(steps), shape[axis_at] // parts).reshape((-1,) + (1,) * (len(shape) - 1 - axis_at))
    return loudness


def centred(own_key, extent, spread, limit, pieces=(), kind=jnp.bfloat16):
    level = steps_of(own_key, extent, pieces, -0.22, 0.18) if pieces else 1.0
    array = jax.random.normal(own_key, extent, jnp.float32) * spread * level
    return jnp.minimum(jnp.maximum(array, -limit), limit).astype(kind)


def setup_inputs(seed: int = 0) -> dict:
    arg_keys = jax.random.split(jax.random.key(seed), 19)
    return {
        "layer_input_rows": centred(arg_keys[0], (TOKEN_COUNT, D), 1.0, 6.0, ((0, 16),)),
        "input_norm_gain": jnp.clip(1.0 + 0.18 * jax.random.normal(arg_keys[1], (D,), jnp.float32), 0.1, 1.9),
        "query_weight": centred(arg_keys[2], (D, ATT_HEADS * HEAD_DIM), D ** -0.5, 0.125, ((1, 8),)),
        "key_weight": centred(arg_keys[3], (D, ATT_HEADS * HEAD_DIM), D ** -0.5, 0.125, ((1, 8),)),
        "value_weight": centred(arg_keys[4], (D, ATT_HEADS * HEAD_DIM), D ** -0.5, 0.125, ((1, 8),)),
        "query_norm_gain": draw_query_norm_gain(jax.random.fold_in(arg_keys[18], 71), 0),
        "key_norm_gain": draw_key_norm_gain(jax.random.fold_in(arg_keys[18], 71), 0),
        "cumulative_gate": draw_cumulative_gate(jax.random.fold_in(arg_keys[18], 71), 0),
        "attention_norm_gain": jnp.clip(1.0 + 0.18 * jax.random.normal(arg_keys[8], (ATT_HEADS * HEAD_DIM,), jnp.float32), 0.1, 1.9),
        "recurrence_query_weight": centred(arg_keys[9], (D, RECURRENCE_HEADS * STATE_ROWS), D ** -0.5, 0.125, ((1, 8),)),
        "forget_weight": centred(arg_keys[10], (D, RECURRENCE_HEADS * STATE_ROWS), D ** -0.5, 0.125, ((1, 8),)),
        "recurrence_value_weight": centred(arg_keys[11], (D, RECURRENCE_HEADS * VAL_DIM), D ** -0.5, 0.125, ((1, 8),)),
        "output_gate_weight": centred(arg_keys[12], (D, RECURRENCE_HEADS * VAL_DIM), D ** -0.5, 0.125, ((1, 8),)),
        "gate_lower_slack": draw_gate_lower_slack(jax.random.fold_in(arg_keys[18], 71), 0),
        "extra_log_decay": draw_extra_log_decay(jax.random.fold_in(arg_keys[18], 71), 0),
        "recurrence_norm_gain": jnp.clip(1.0 + 0.18 * jax.random.normal(arg_keys[15], (RECURRENCE_HEADS * VAL_DIM,), jnp.float32), 0.1, 1.9),
        "attention_output_weight": centred(arg_keys[16], (ATT_HEADS * HEAD_DIM, D), (ATT_HEADS * HEAD_DIM + RECURRENCE_HEADS * VAL_DIM) ** -0.5, 0.125, ((0, 8),)),
        "recurrence_output_weight": centred(arg_keys[17], (RECURRENCE_HEADS * VAL_DIM, D), (ATT_HEADS * HEAD_DIM + RECURRENCE_HEADS * VAL_DIM) ** -0.5, 0.125, ((0, 8),)),
    }


EPSILON = 1e-06
HIGHEST_ACCURACY = lax.Precision.HIGHEST

def rms_rows(values, gain):
    squares = lax.optimization_barrier(jnp.mean(values * values, axis=-1, keepdims=True))
    return values * lax.rsqrt(squares + EPSILON) * gain

def recur_blocks(rec_query, forget_fraction, rec_value, decay_logarithm, states):
    length, head_number, keydim = rec_query.shape
    span_rows = BLOCK
    blocks = length // span_rows
    lower_tri = jnp.arange(span_rows)[:, None] >= jnp.arange(span_rows)[None, :]

    def to_blocks(values):
        return values.reshape(blocks, span_rows, head_number, values.shape[-1])

    def advance(carried, inputs):
        current_states, running = carried
        query_block, share_block, value_block, decay_blk = inputs
        within_block = jnp.cumsum(decay_blk, axis=0)
        differ = within_block[:, None] - within_block[None, :]
        fading = jnp.exp(jnp.where(lower_tri[:, :, None, None], differ, -jnp.inf))
        scores = jnp.einsum('thk,tshk,shk->tsh', query_block, fading, share_block, precision=HIGHEST_ACCURACY)
        inner_part = jnp.einsum('tsh,shv->thv', scores, value_block, precision=HIGHEST_ACCURACY)
        carried_piece = jnp.einsum('zbf,bfw->zbw', query_block * jnp.exp(within_block), current_states, precision=HIGHEST_ACCURACY)
        closing_state = within_block[-1]
        current_states = jnp.exp(closing_state)[:, :, None] * current_states + jnp.einsum('tfo,tfw->fow', share_block * jnp.exp(closing_state[None] - within_block), value_block, precision=HIGHEST_ACCURACY)
        visible_query = query_block * jnp.exp(running[None] + within_block)
        return ((current_states, running + closing_state), (inner_part + carried_piece, visible_query))
    zeros_run = jnp.zeros((head_number, keydim), jnp.float32)
    (states, running), (outputs, visible_query) = lax.scan(advance, (states, zeros_run), (to_blocks(rec_query), to_blocks(forget_fraction), to_blocks(rec_value), to_blocks(decay_logarithm)))
    return (outputs.reshape(length, head_number, -1), states, running, visible_query.reshape(length, head_number, keydim))

def attend_head(operands):
    head_query, head_key, head_value, head_cum = operands
    rows_blk = math.gcd(TOKEN_COUNT, 1024)
    score_scale = HEAD_DIM ** (-0.5)
    key_pos = jnp.arange(TOKEN_COUNT, dtype=jnp.int32)

    def one_block(block_index):
        first_row = (block_index * rows_blk).astype(jnp.int32)
        query_block = lax.dynamic_slice_in_dim(head_query, first_row, rows_blk, 0)
        cum_blk = lax.dynamic_slice_in_dim(head_cum, first_row, rows_blk, 0)
        scores = jnp.dot(query_block, head_key.T, preferred_element_type=jnp.float32) * score_scale
        scores = scores + cum_blk[:, None] - head_cum[None, :]
        query_pos = first_row + jnp.arange(rows_blk, dtype=jnp.int32)
        causal = key_pos[None, :] <= query_pos[:, None]
        scores = jnp.where(causal, scores, -jnp.inf)
        row_top = lax.optimization_barrier(jnp.max(scores, axis=-1))
        weights = jnp.exp(scores - row_top[:, None])
        totals = lax.optimization_barrier(jnp.sum(weights, axis=-1))
        summed = jnp.dot(weights.astype(jnp.bfloat16), head_value, preferred_element_type=jnp.float32)
        return (summed / totals[:, None], row_top + jnp.log(totals))
    outputs, log_sums = lax.map(one_block, jnp.arange(TOKEN_COUNT // rows_blk, dtype=jnp.int32))
    return (outputs.reshape(TOKEN_COUNT, HEAD_DIM), log_sums.reshape(TOKEN_COUNT))

def reference(layer_input_rows, input_norm_gain, query_weight, key_weight, value_weight, query_norm_gain, key_norm_gain, cumulative_gate, attention_norm_gain, recurrence_query_weight, forget_weight, recurrence_value_weight, output_gate_weight, gate_lower_slack, extra_log_decay, recurrence_norm_gain, attention_output_weight, recurrence_output_weight):
    normalized_input = rms_rows(layer_input_rows.astype(jnp.float32), input_norm_gain).astype(jnp.bfloat16)

    def project(weight):
        return jnp.dot(normalized_input, weight, preferred_element_type=jnp.float32)
    queries = rms_rows(project(query_weight).reshape(TOKEN_COUNT, ATT_HEADS, HEAD_DIM), query_norm_gain).astype(jnp.bfloat16)
    keys = rms_rows(project(key_weight).reshape(TOKEN_COUNT, ATT_HEADS, HEAD_DIM), key_norm_gain).astype(jnp.bfloat16)
    values = project(value_weight).astype(jnp.bfloat16).reshape(TOKEN_COUNT, ATT_HEADS, HEAD_DIM)
    attention, log_sum = lax.map(attend_head, (queries.transpose(1, 0, 2), keys.transpose(1, 0, 2), values.transpose(1, 0, 2), cumulative_gate.T))
    attn_out = rms_rows(attention.transpose(1, 0, 2), attention_norm_gain.reshape(ATT_HEADS, HEAD_DIM))
    attn_out = attn_out.astype(jnp.bfloat16).reshape(TOKEN_COUNT, ATT_HEADS * HEAD_DIM)
    rec_query = jax.nn.silu(project(recurrence_query_weight)).reshape(TOKEN_COUNT, RECURRENCE_HEADS, STATE_ROWS)
    forget_fraction = gate_lower_slack * jax.nn.sigmoid(-project(forget_weight))
    decay_logarithm = jnp.log1p(-forget_fraction).reshape(TOKEN_COUNT, RECURRENCE_HEADS, STATE_ROWS) + extra_log_decay[:, :, None]
    rec_value = lax.optimization_barrier(project(recurrence_value_weight).astype(jnp.bfloat16)).astype(jnp.float32)
    rec_value = rec_value.reshape(TOKEN_COUNT, RECURRENCE_HEADS, VAL_DIM)
    start_states = jnp.zeros((RECURRENCE_HEADS, STATE_ROWS, VAL_DIM), jnp.float32)
    recurrent_output = recur_blocks(rec_query, forget_fraction.reshape(TOKEN_COUNT, RECURRENCE_HEADS, STATE_ROWS), rec_value, decay_logarithm, start_states)[0]
    out_gate = jax.nn.silu(project(output_gate_weight)).reshape(TOKEN_COUNT, RECURRENCE_HEADS, VAL_DIM)
    rec_out = rms_rows(recurrent_output, recurrence_norm_gain.reshape(RECURRENCE_HEADS, VAL_DIM)) * out_gate
    rec_out = rec_out.astype(jnp.bfloat16).reshape(TOKEN_COUNT, RECURRENCE_HEADS * VAL_DIM)
    attn_cols = ATT_HEADS * HEAD_DIM // N_TP
    rec_cols = RECURRENCE_HEADS * VAL_DIM // N_TP

    def add_group(group_index, running_sum):
        first_attn = (group_index * attn_cols).astype(jnp.int32)
        first_rec = (group_index * rec_cols).astype(jnp.int32)
        attn_part = lax.dynamic_slice_in_dim(attn_out, first_attn, attn_cols, 1)
        attn_rows = lax.dynamic_slice_in_dim(attention_output_weight, first_attn, attn_cols, 0)
        rec_part = lax.dynamic_slice_in_dim(rec_out, first_rec, rec_cols, 1)
        rec_rows = lax.dynamic_slice_in_dim(recurrence_output_weight, first_rec, rec_cols, 0)
        partial_value = jnp.dot(attn_part, attn_rows, preferred_element_type=jnp.float32)
        partial_value = partial_value + jnp.dot(rec_part, rec_rows, preferred_element_type=jnp.float32)
        return running_sum + lax.optimization_barrier(partial_value.astype(jnp.bfloat16)).astype(jnp.float32)
    mixed_sum = lax.fori_loop(0, N_TP, add_group, jnp.zeros((TOKEN_COUNT, D), jnp.float32))
    return (mixed_sum.astype(jnp.bfloat16), log_sum.T)
```

```python
import jax
import jax.numpy as jnp
from jax import lax
from jax.experimental import pallas as pl
from jax.experimental.pallas import tpu as pltpu
from jax.sharding import PartitionSpec as P

F32 = jnp.float32
BF16 = jnp.bfloat16
MESH = pl.DeviceIdType.MESH
EPSILON = 1e-06
ROWS = 256
WIDTH = 2048
LANES = 128
HALF = 64
SHARDS = 16
RING = 4
CHUNKS = 4
CHUNK = WIDTH // CHUNKS
STATE_MSG = 144
KV_SENDS = 80
NEGATIVE = -1e30


def dot(a, b):
    return jnp.dot(a, b, preferred_element_type=F32)


def dot_nt(a, b):
    return lax.dot_general(a, b, (((1,), (1,)), ((), ())), preferred_element_type=F32)


def split2(v):
    hi = v.astype(BF16)
    return hi, (v - hi.astype(F32)).astype(BF16)


def split3(v):
    hi = v.astype(BF16)
    rest = v - hi.astype(F32)
    mid = rest.astype(BF16)
    return hi, mid, (rest - mid.astype(F32)).astype(BF16)


def iota(shape, dim):
    return lax.broadcasted_iota(jnp.int32, shape, dim)


def kernel(
    x_hbm, xg_hbm, wq_hbm, wk_hbm, wv_hbm, qg_hbm, kg_hbm, gate_hbm, ag_hbm,
    wrq_hbm, wf_hbm, wrv_hbm, wog_hbm, slack_hbm, extra_hbm, rg_hbm, woa_hbm, wor_hbm,
    mixed_ref, lse_ref,
    x_v, n_v, xg_v, qg_v, kg_v, ag_v, slack_v, extra_v, rg_v,
    wkv, wfr, wqq, wog, wo_own, wo_peer,
    gates, kv, q_v, m_v, acc_v,
    st_row, st_col, in_v, rec_v, visq_v, outgate_v,
    act, act_peer, part, xt, xd, xs, xsum,
    lsem, gsem, grecv, ssem, krecv, rsem, rrecv, csem, crecv, psem, precv, xsem, xrecv,
):
    sp = lax.axis_index("sp")
    tp = lax.axis_index("tp")
    z, y = sp // RING, sp % RING
    xc, core = tp // 2, tp % 2
    peer = 2 * xc + 1 - core

    loads = {}

    def load(name, src, dst):
        cp = pltpu.make_async_copy(src, dst, lsem.at[len(loads)])
        cp.start()
        loads[name] = cp

    load("x", x_hbm, x_v)
    load("xg", xg_hbm, xg_v)
    load("wk", wk_hbm, wkv.at[:, pl.ds(0, LANES)])
    load("wv", wv_hbm, wkv.at[:, pl.ds(LANES, LANES)])
    load("kg", kg_hbm, kg_v)
    load("gate", gate_hbm, gates.at[sp])
    load("wf", wf_hbm, wfr.at[:, pl.ds(0, LANES)])
    load("wrv", wrv_hbm, wfr.at[:, pl.ds(LANES, LANES)])
    load("slack", slack_hbm, slack_v)
    load("extra", extra_hbm, extra_v)
    load("wq", wq_hbm, wqq.at[:, pl.ds(0, LANES)])
    load("wrq", wrq_hbm, wqq.at[:, pl.ds(LANES, LANES)])
    load("qg", qg_hbm, qg_v)
    load("wog", wog_hbm, wog)
    load("ag", ag_hbm, ag_v)
    load("rg", rg_hbm, rg_v)
    load("woa", woa_hbm, wo_own.at[pl.ds(0, LANES)])
    load("wor", wor_hbm, wo_own.at[pl.ds(LANES, LANES)])

    barrier = pltpu.get_barrier_semaphore()
    for k in range(1, SHARDS):
        pl.semaphore_signal(barrier, inc=1, device_id=((sp + k) % SHARDS, tp), device_id_type=MESH)
    x_right = 2 * ((xc + 1) % RING) + core
    x_left = 2 * ((xc + 3) % RING) + core
    for other in (x_right, x_left, peer):
        pl.semaphore_signal(barrier, inc=1, device_id=(sp, other), device_id_type=MESH)

    pending = []

    def start(pred, cp):
        if pred is None:
            cp.start()
        else:
            pl.when(pred)(cp.start)
        pending.append((pred, cp))

    loads["x"].wait()
    loads["xg"].wait()
    step = 32
    for r in range(0, ROWS, step):
        xf = x_v[r : r + step, :].astype(F32)
        mean = jnp.sum(xf * xf, axis=-1, keepdims=True) * (1.0 / WIDTH)
        n_v[r : r + step, :] = (xf * lax.rsqrt(mean + EPSILON) * xg_v[...]).astype(BF16)

    lane = iota((ROWS, LANES), 1)
    low = lane < HALF
    same_half = (iota((LANES, LANES), 0) // HALF == iota((LANES, LANES), 1) // HALF)
    halves = jnp.where(same_half, 1.0, 0.0).astype(BF16)

    def half_rms(v, gain):
        hi, lo = split2(v * v)
        mean = (dot(hi, halves) + dot(lo, halves)) * (1.0 / HALF)
        return v * lax.rsqrt(mean + EPSILON) * gain

    loads["wk"].wait()
    loads["wv"].wait()
    loads["kg"].wait()
    kv_f = dot(n_v[...], wkv[...])
    keys = half_rms(kv_f[:, :LANES], kg_v[...])
    swapped = pltpu.roll(kv_f[:, LANES:], HALF, 1)
    kv[0, sp] = jnp.where(low, keys, swapped).astype(BF16)
    kv[1, sp] = jnp.where(low, swapped, keys).astype(BF16)

    loads["gate"].wait()
    pl.semaphore_wait(barrier, SHARDS - 1 + 3)

    y_up = z * RING + (y + 1) % RING
    y_down = z * RING + (y + 3) % RING
    count = [0]

    def send(pred, h, j, target):
        n = count[0]
        count[0] += 1
        start(
            pred,
            pltpu.make_async_remote_copy(
                src_ref=kv.at[h, j], dst_ref=kv.at[h, j], send_sem=ssem.at[n], recv_sem=krecv.at[h, j],
                device_id=(target, tp), device_id_type=MESH,
            ),
        )

    def arrive(pred, h, j):
        cp = pltpu.make_async_remote_copy(
            src_ref=kv.at[h, j], dst_ref=kv.at[h, j], send_sem=ssem.at[0], recv_sem=krecv.at[h, j],
            device_id=(sp, peer), device_id_type=MESH,
        )
        if pred is None:
            cp.wait_recv()
        else:
            pl.when(pred)(cp.wait_recv)

    def send_along_z(h, j):
        send(z < 3, h, j, (sp + RING) % SHARDS)
        send(z == 0, h, j, 3 * RING + y)
        send((z == 1) & (core == 1), h, j, y)

    def send_along_y(pred, h, j):
        send(pred, h, j, y_up)
        send(pred, h, j, y_down)

    send_along_y(None, 0, sp)
    send_along_z(1, sp)
    send_along_y(None, 1, sp)
    send_along_z(0, sp)

    def gate_copy(j, target):
        return pltpu.make_async_remote_copy(
            src_ref=gates.at[j], dst_ref=gates.at[j], send_sem=gsem.at[target], recv_sem=grecv.at[j],
            device_id=(target, tp), device_id_type=MESH,
        )

    for k in range(1, SHARDS):
        target = (sp + k) % SHARDS
        start(sp + k < SHARDS, gate_copy(sp, target))

    loads["wf"].wait()
    loads["wrv"].wait()
    loads["slack"].wait()
    loads["extra"].wait()
    fr = dot(n_v[...], wfr[...])
    forget = slack_v[...] * (1.0 / (1.0 + jnp.exp(fr[:, :LANES])))
    rec_value = fr[:, LANES:].astype(BF16)
    extra = jnp.broadcast_to(extra_v[...], (LANES, ROWS)).T
    row_at, col_at = iota((ROWS, ROWS), 0), iota((ROWS, ROWS), 1)
    causal = col_at <= row_at
    lower = jnp.where(causal, 1.0, 0.0).astype(BF16)
    sums = dot(lower, jnp.concatenate(split3(jnp.log1p(-forget)) + split3(extra), axis=1))
    share_sum = sums[:, :LANES] + sums[:, LANES : 2 * LANES] + sums[:, 2 * LANES : 3 * LANES]
    extra_sum = sums[:, 3 * LANES : 4 * LANES] + sums[:, 4 * LANES : 5 * LANES] + sums[:, 5 * LANES :]
    share_end = share_sum[ROWS - 1 :, :]
    extra_end = extra_sum[ROWS - 1 :, :]
    closing = (forget * jnp.exp((share_end - share_sum) + (extra_end - extra_sum))).astype(BF16)
    state_t = dot(fr[:, LANES:].T.astype(BF16), closing)

    def state_message(state, decay):
        hi, mid, lo = (part.astype(F32) for part in split3(decay))
        at = iota((16, LANES), 0)
        tail = jnp.where(at == 0, hi, jnp.where(at == 1, mid, jnp.where(at == 2, lo, 0.0)))
        return state.astype(BF16), tail.astype(BF16)

    body, tail = state_message(state_t, share_end + extra_end)
    st_row[y, :LANES] = body
    st_row[y, LANES:] = tail

    def row_copy(j, target, n):
        return pltpu.make_async_remote_copy(
            src_ref=st_row.at[j], dst_ref=st_row.at[j], send_sem=rsem.at[n], recv_sem=rrecv.at[j],
            device_id=(target, tp), device_id_type=MESH,
        )

    def col_copy(j, target, n):
        return pltpu.make_async_remote_copy(
            src_ref=st_col.at[j], dst_ref=st_col.at[j], send_sem=csem.at[n], recv_sem=crecv.at[j],
            device_id=(target, tp), device_id_type=MESH,
        )

    for n in range(1, RING):
        start(None, row_copy(y, z * RING + (y + n) % RING, n))

    loads["wq"].wait()
    loads["wrq"].wait()
    loads["qg"].wait()
    qq = dot(n_v[...], wqq[...])
    queries = (half_rms(qq[:, :LANES], qg_v[...]).astype(BF16).astype(F32)) * (HALF**-0.5)
    q_v[0] = jnp.where(low, queries, 0.0).astype(BF16)
    q_v[1] = jnp.where(low, 0.0, queries).astype(BF16)

    rq = qq[:, LANES:]
    rec_query = rq / (1.0 + jnp.exp(-rq))
    scores = dot_nt((rec_query * jnp.exp(share_sum)).astype(BF16), (forget * jnp.exp(-share_sum)).astype(BF16))
    differ = jnp.concatenate([extra_sum, extra_sum], axis=1) - extra_sum.T[:1, :]
    scores = scores * jnp.exp(jnp.where(causal, differ, NEGATIVE))
    rec_v[...] = dot(scores.astype(BF16), rec_value)
    visq_v[...] = (rec_query * jnp.exp(share_sum + extra_sum)).astype(BF16)

    loads["wog"].wait()
    og = dot(n_v[...], wog[...])
    outgate_v[...] = og / (1.0 + jnp.exp(-og))

    def attend(j, first):
        for h in range(2):
            block = kv[h, j]
            s = dot_nt(q_v[h], block) - gates[j, h : h + 1, :]
            if first:
                s = jnp.where(causal, s, NEGATIVE)
            top = jnp.max(s, axis=-1, keepdims=True)
            if not first:
                old = m_v[h]
                top = jnp.maximum(old[:, :1], top)
            weights = jnp.exp(s - top).astype(BF16)
            ones = jnp.ones_like(block)
            right = jnp.where(low, ones, block) if h == 0 else jnp.where(low, block, ones)
            summed = dot(weights, right)
            if not first:
                summed = summed + acc_v[h] * jnp.exp(old - top)
            acc_v[h] = summed
            m_v[h] = jnp.broadcast_to(top, (ROWS, LANES))

    attend(sp, True)

    loads["woa"].wait()
    loads["wor"].wait()
    wo_copy = pltpu.make_async_remote_copy(
        src_ref=wo_own, dst_ref=wo_peer, send_sem=psem.at[0], recv_sem=precv.at[0],
        device_id=(sp, peer), device_id_type=MESH,
    )
    start(None, wo_copy)

    def wait_gates():
        for k in range(1, SHARDS):
            j = (sp + SHARDS - k) % SHARDS
            pl.when(sp >= k)(gate_copy(j, j).wait_recv)

    wait_gates()

    hops = {0: 0, 1: 1, 3: 1, 2: 2}
    plan = sorted(
        ((back, up) for back in (0, 1, 3, 2) for up in (0, 1, 3, 2) if (back, up) != (0, 0)),
        key=lambda e: hops[e[0]] + hops[e[1]],
    )

    def shard_of(back, up):
        return ((z + RING - back) % RING) * RING + (y + up) % RING

    def relay_z(valid, h, j, back):
        if back == 1:
            send((z == 1) & (core == 0) | (z == 2) & (core == 0), h, j, (sp + RING) % SHARDS)
        if back == 3:
            send((z == 3) & (core == 1), h, j, 2 * RING + y)

    def handle(h, back, up):
        valid = None if back == 0 else z >= back
        j = shard_of(back, up)
        arrive(valid, h, j)
        if h == 0:
            if back == 0:
                if up == 3:
                    send(core == 0, h, j, y_up)
                if up == 1:
                    send(core == 1, h, j, y_down)
                send_along_z(h, j)
            else:
                relay_z(valid, h, j, back)
        else:
            if up == 0:
                relay_z(valid, h, j, back)
                send_along_y(valid, h, j)
            else:
                fine = core == (0 if up == 3 else 1)
                if up != 2:
                    send(fine if valid is None else fine & valid, h, j, y_up if up == 3 else y_down)
        if back == 1 and (h == 0 or up == 0):
            through = (z == 0) & (core == 1)
            jj = RING + (y + up) % RING
            arrive(through, h, jj)
            send(through, h, jj, 3 * RING + y)

    def compute(back, up):
        needed = (z >= back) if back else (y + up) % RING < y
        j = shard_of(back, up)

        @pl.when(needed)
        def _():
            attend(j, False)

    def read_state(ref, j):
        tail = ref[j, LANES:].astype(F32)
        return ref[j, :LANES].astype(F32), tail[0:1] + tail[1:2] + tail[2:3]

    def combine_row():
        for n in range(1, RING):
            row_copy((y + n) % RING, sp, n).wait_recv()
        before, decay = jnp.zeros((LANES, LANES), F32), jnp.zeros((1, LANES), F32)
        mine, mine_decay = before, decay
        for k in range(RING):
            state, log = read_state(st_row, k)
            before = jnp.exp(log) * before + state
            decay = decay + log
            mine = jnp.where(k < y, before, mine)
            mine_decay = jnp.where(k < y, decay, mine_decay)
        in_v[0] = mine
        in_v[1, 0:1] = mine_decay
        body, tail = state_message(before, decay)
        st_col[z, :LANES] = body
        st_col[z, LANES:] = tail
        for n in range(1, RING):
            start(z + n < RING, col_copy(z, ((z + n) % RING) * RING + y, n))

    def combine_col():
        for n in range(1, RING):
            pl.when(z >= n)(col_copy((z + RING - n) % RING, sp, n).wait_recv)
        in_v[2] = jnp.zeros((LANES, LANES), F32)
        for k in range(RING - 1):

            @pl.when(k < z)
            def _():
                state, log = read_state(st_col, k)
                in_v[2] = jnp.exp(log) * in_v[2] + state

        incoming = jnp.exp(in_v[1, 0:1]) * in_v[2] + in_v[0]
        recurrent = rec_v[...] + dot_nt(visq_v[...], incoming.astype(BF16))
        mean = jnp.mean(recurrent * recurrent, axis=-1, keepdims=True)
        return (recurrent * lax.rsqrt(mean + EPSILON) * rg_v[...] * outgate_v[...]).astype(BF16)

    last = None
    for i, (back, up) in enumerate(plan):
        handle(0, back, up)
        handle(1, back, up)
        if last is not None:
            compute(*last)
        last = (back, up)
        if i == 5:
            combine_row()
    loads["ag"].wait()
    loads["rg"].wait()
    rec_out = combine_col()
    compute(*last)

    a0, a1 = acc_v[0], acc_v[1]
    totals = jnp.where(low, a0, a1)
    attention = pltpu.roll(jnp.where(low, a1, a0), HALF, 1) / totals
    attn_out = half_rms(attention, ag_v[...]).astype(BF16)
    for b in range(8):
        rows = slice(32 * b, 32 * b + 32)
        at = slice(32 * (b // 2), 32 * (b // 2) + 32)
        act[b % 2, at, :LANES] = attn_out[rows]
        act[b % 2, at, LANES:] = rec_out[rows]
    act_copy = pltpu.make_async_remote_copy(
        src_ref=act.at[1 - core], dst_ref=act_peer, send_sem=psem.at[1], recv_sem=precv.at[1],
        device_id=(sp, peer), device_id_type=MESH,
    )
    start(None, act_copy)
    log_sum = (jnp.where(low, m_v[0], m_v[1]) + jnp.log(totals)).T
    lse_ref[0:1, :] = log_sum[0:1, :] + gates[sp, 0:1, :]
    lse_ref[1:2, :] = log_sum[HALF : HALF + 1, :] + gates[sp, 1:2, :]
    wo_copy.wait_recv()
    act_copy.wait_recv()

    e_next = (xc + 2 * core + 3) % RING
    e_prev = (xc + 5 - 2 * core) % RING
    far = (xc + 2) % RING
    to_next = 2 * e_next + core
    to_prev = 2 * e_prev + core

    def x_copy(kind, c, src, dst, target):
        return pltpu.make_async_remote_copy(
            src_ref=src, dst_ref=dst, send_sem=xsem.at[kind, c], recv_sem=xrecv.at[kind, c],
            device_id=(sp, target), device_id_type=MESH,
        )

    mine = act[core]
    theirs = act_peer[...]
    for c in range(CHUNKS):
        cols = slice(c * CHUNK, (c + 1) * CHUNK)
        product = dot(mine, wo_own[:, cols]) + dot(theirs, wo_peer[:, cols])
        for b in range(RING):
            part[c, b] = product[32 * b : 32 * b + 32].astype(BF16)
        start(None, x_copy(0, c, part.at[c, far], xt.at[c], to_next))
        start(None, x_copy(1, c, part.at[c, e_prev], xd.at[c], to_prev))
    for c in range(CHUNKS):
        x_copy(0, c, part.at[c, far], xt.at[c], to_next).wait_recv()
        xsum[c] = (xt[c].astype(F32) + part[c, e_next].astype(F32)).astype(BF16)
        start(None, x_copy(2, c, xsum.at[c], xs.at[c], to_next))
    for c in range(CHUNKS):
        x_copy(1, c, part.at[c, e_prev], xd.at[c], to_prev).wait_recv()
        x_copy(2, c, xsum.at[c], xs.at[c], to_next).wait_recv()
        total = part[c, xc].astype(F32) + xd[c].astype(F32) + xs[c].astype(F32)
        mixed_ref[:, c * CHUNK : (c + 1) * CHUNK] = total.astype(BF16)
    for pred, cp in pending:
        if pred is None:
            cp.wait_send()
        else:
            pl.when(pred)(cp.wait_send)


def body(*args):
    (
        layer_input_rows, input_norm_gain, query_weight, key_weight, value_weight, query_norm_gain,
        key_norm_gain, cumulative_gate, attention_norm_gain, recurrence_query_weight, forget_weight,
        recurrence_value_weight, output_gate_weight, gate_lower_slack, extra_log_decay,
        recurrence_norm_gain, attention_output_weight, recurrence_output_weight,
    ) = args
    twice = lambda gain: jnp.concatenate([gain, gain])[None]
    operands = (
        layer_input_rows, input_norm_gain[None], query_weight, key_weight, value_weight,
        twice(query_norm_gain), twice(key_norm_gain), cumulative_gate.T, attention_norm_gain[None],
        recurrence_query_weight, forget_weight, recurrence_value_weight, output_gate_weight,
        gate_lower_slack[None], extra_log_decay.T, recurrence_norm_gain[None],
        attention_output_weight, recurrence_output_weight,
    )
    dma = pltpu.SemaphoreType.DMA
    mixed, lse = pl.pallas_call(
        kernel,
        name="mixer",
        out_shape=(
            jax.ShapeDtypeStruct((ROWS // 8, WIDTH), BF16),
            jax.ShapeDtypeStruct((2, ROWS), F32),
        ),
        in_specs=[pl.BlockSpec(memory_space=pl.ANY)] * len(operands),
        out_specs=(pl.BlockSpec(memory_space=pltpu.VMEM), pl.BlockSpec(memory_space=pltpu.VMEM)),
        scratch_shapes=[
            pltpu.VMEM((ROWS, WIDTH), BF16),
            pltpu.VMEM((ROWS, WIDTH), BF16),
            pltpu.VMEM((1, WIDTH), F32),
            pltpu.VMEM((1, LANES), F32),
            pltpu.VMEM((1, LANES), F32),
            pltpu.VMEM((1, LANES), F32),
            pltpu.VMEM((1, LANES), F32),
            pltpu.VMEM((1, ROWS), F32),
            pltpu.VMEM((1, LANES), F32),
            pltpu.VMEM((WIDTH, 2 * LANES), BF16),
            pltpu.VMEM((WIDTH, 2 * LANES), BF16),
            pltpu.VMEM((WIDTH, 2 * LANES), BF16),
            pltpu.VMEM((WIDTH, LANES), BF16),
            pltpu.VMEM((2 * LANES, WIDTH), BF16),
            pltpu.VMEM((2 * LANES, WIDTH), BF16),
            pltpu.VMEM((SHARDS, 2, ROWS), F32),
            pltpu.VMEM((2, SHARDS, ROWS, LANES), BF16),
            pltpu.VMEM((2, ROWS, LANES), BF16),
            pltpu.VMEM((2, ROWS, LANES), F32),
            pltpu.VMEM((2, ROWS, LANES), F32),
            pltpu.VMEM((RING, STATE_MSG, LANES), BF16),
            pltpu.VMEM((RING, STATE_MSG, LANES), BF16),
            pltpu.VMEM((3, LANES, LANES), F32),
            pltpu.VMEM((ROWS, LANES), F32),
            pltpu.VMEM((ROWS, LANES), BF16),
            pltpu.VMEM((ROWS, LANES), F32),
            pltpu.VMEM((2, ROWS // 2, 2 * LANES), BF16),
            pltpu.VMEM((ROWS // 2, 2 * LANES), BF16),
            pltpu.VMEM((CHUNKS, RING, ROWS // 8, CHUNK), BF16),
            pltpu.VMEM((CHUNKS, ROWS // 8, CHUNK), BF16),
            pltpu.VMEM((CHUNKS, ROWS // 8, CHUNK), BF16),
            pltpu.VMEM((CHUNKS, ROWS // 8, CHUNK), BF16),
            pltpu.VMEM((CHUNKS, ROWS // 8, CHUNK), BF16),
            dma((18,)),
            dma((SHARDS,)),
            dma((SHARDS,)),
            dma((KV_SENDS,)),
            dma((2, SHARDS)),
            dma((RING,)),
            dma((RING,)),
            dma((RING,)),
            dma((RING,)),
            dma((2,)),
            dma((2,)),
            dma((3, CHUNKS)),
            dma((3, CHUNKS)),
        ],
        compiler_params=pltpu.CompilerParams(
            collective_id=0, has_side_effects=True, vmem_limit_bytes=60 * 1024 * 1024
        ),
    )(*operands)
    return mixed, lse.T


def solution(mesh):
    both = P("sp", "tp")
    placed = (
        P("sp", None), P(), P(None, "tp"), P(None, "tp"), P(None, "tp"), P(), P(), both, P("tp"),
        P(None, "tp"), P(None, "tp"), P(None, "tp"), P(None, "tp"), P("tp"), both, P("tp"),
        P("tp", None), P("tp", None),
    )
    return jax.shard_map(
        body, mesh=mesh, in_specs=placed, out_specs=(P(("sp", "tp"), None), both), check_vma=False
    )
```

```python
import jax
import jax.numpy as jnp
from jax import lax
from jax.experimental import pallas as pl
from jax.experimental.pallas import tpu as pltpu
from jax.sharding import PartitionSpec as P

F32 = jnp.float32
BF16 = jnp.bfloat16
MESH = pl.DeviceIdType.MESH
EPSILON = 1e-06
ROWS = 256
WIDTH = 2048
LANES = 128
HALF = 64
SHARDS = 16
RING = 4
CHUNKS = 4
CHUNK = WIDTH // CHUNKS
STATE_MSG = 144
KV_SENDS = 80
NEGATIVE = -1e30


def dot(a, b):
    return jnp.dot(a, b, preferred_element_type=F32)


def dot_nt(a, b):
    return lax.dot_general(a, b, (((1,), (1,)), ((), ())), preferred_element_type=F32)


def split2(v):
    hi = v.astype(BF16)
    return hi, (v - hi.astype(F32)).astype(BF16)


def split3(v):
    hi = v.astype(BF16)
    rest = v - hi.astype(F32)
    mid = rest.astype(BF16)
    return hi, mid, (rest - mid.astype(F32)).astype(BF16)


def iota(shape, dim):
    return lax.broadcasted_iota(jnp.int32, shape, dim)


def kernel(
    x_hbm, xg_hbm, wq_hbm, wk_hbm, wv_hbm, qg_hbm, kg_hbm, gate_hbm, ag_hbm,
    wrq_hbm, wf_hbm, wrv_hbm, wog_hbm, slack_hbm, extra_hbm, rg_hbm, woa_hbm, wor_hbm,
    mixed_ref, lse_ref,
    x_v, n_v, xg_v, qg_v, kg_v, ag_v, slack_v, extra_v, rg_v,
    wkv, wfr, wqq, wog, wo_own, wo_peer,
    gates, kv, q_v, m_v, acc_v,
    st_row, st_col, in_v, rec_v, visq_v, outgate_v,
    act, act_peer, part, xt, xd, xs, xsum,
    lsem, gsem, grecv, ssem, krecv, rsem, rrecv, csem, crecv, psem, precv, xsem, xrecv,
):
    sp = lax.axis_index("sp")
    tp = lax.axis_index("tp")
    z, y = sp // RING, sp % RING
    xc, core = tp // 2, tp % 2
    peer = 2 * xc + 1 - core

    loads = {}

    def load(name, src, dst):
        cp = pltpu.make_async_copy(src, dst, lsem.at[len(loads)])
        cp.start()
        loads[name] = cp

    load("x", x_hbm, x_v)
    load("xg", xg_hbm, xg_v)
    load("wk", wk_hbm, wkv.at[:, pl.ds(0, LANES)])
    load("wv", wv_hbm, wkv.at[:, pl.ds(LANES, LANES)])
    load("kg", kg_hbm, kg_v)
    load("gate", gate_hbm, gates.at[sp])
    load("wf", wf_hbm, wfr.at[:, pl.ds(0, LANES)])
    load("wrv", wrv_hbm, wfr.at[:, pl.ds(LANES, LANES)])
    load("slack", slack_hbm, slack_v)
    load("extra", extra_hbm, extra_v)
    load("wq", wq_hbm, wqq.at[:, pl.ds(0, LANES)])
    load("wrq", wrq_hbm, wqq.at[:, pl.ds(LANES, LANES)])
    load("qg", qg_hbm, qg_v)
    load("wog", wog_hbm, wog)
    load("ag", ag_hbm, ag_v)
    load("rg", rg_hbm, rg_v)
    load("woa", woa_hbm, wo_own.at[pl.ds(0, LANES)])
    load("wor", wor_hbm, wo_own.at[pl.ds(LANES, LANES)])

    barrier = pltpu.get_barrier_semaphore()
    for k in range(1, SHARDS):
        pl.semaphore_signal(barrier, inc=1, device_id=((sp + k) % SHARDS, tp), device_id_type=MESH)
    x_right = 2 * ((xc + 1) % RING) + core
    x_left = 2 * ((xc + 3) % RING) + core
    for other in (x_right, x_left, peer):
        pl.semaphore_signal(barrier, inc=1, device_id=(sp, other), device_id_type=MESH)

    pending = []

    def start(pred, cp):
        if pred is None:
            cp.start()
        else:
            pl.when(pred)(cp.start)
        pending.append((pred, cp))

    loads["x"].wait()
    loads["xg"].wait()
    step = 32
    for r in range(0, ROWS, step):
        xf = x_v[r : r + step, :].astype(F32)
        mean = jnp.sum(xf * xf, axis=-1, keepdims=True) * (1.0 / WIDTH)
        n_v[r : r + step, :] = (xf * lax.rsqrt(mean + EPSILON) * xg_v[...]).astype(BF16)

    lane = iota((ROWS, LANES), 1)
    low = lane < HALF
    same_half = (iota((LANES, LANES), 0) // HALF == iota((LANES, LANES), 1) // HALF)
    halves = jnp.where(same_half, 1.0, 0.0).astype(BF16)

    def twice(gain):
        return jnp.concatenate([gain, gain], axis=1)

    def half_rms(v, gain):
        hi, lo = split2(v * v)
        mean = (dot(hi, halves) + dot(lo, halves)) * (1.0 / HALF)
        return v * lax.rsqrt(mean + EPSILON) * gain

    loads["wk"].wait()
    loads["wv"].wait()
    loads["kg"].wait()
    kv_f = dot(n_v[...], wkv[...])
    keys = half_rms(kv_f[:, :LANES], twice(kg_v[...]))
    swapped = pltpu.roll(kv_f[:, LANES:], HALF, 1)
    kv[0, sp] = jnp.where(low, keys, swapped).astype(BF16)
    kv[1, sp] = jnp.where(low, swapped, keys).astype(BF16)

    loads["gate"].wait()
    pl.semaphore_wait(barrier, SHARDS - 1 + 3)

    y_up = z * RING + (y + 1) % RING
    y_down = z * RING + (y + 3) % RING
    count = [0]

    def send(pred, h, j, target):
        n = count[0]
        count[0] += 1
        start(
            pred,
            pltpu.make_async_remote_copy(
                src_ref=kv.at[h, j], dst_ref=kv.at[h, j], send_sem=ssem.at[n], recv_sem=krecv.at[h, j],
                device_id=(target, tp), device_id_type=MESH,
            ),
        )

    def arrive(pred, h, j):
        cp = pltpu.make_async_remote_copy(
            src_ref=kv.at[h, j], dst_ref=kv.at[h, j], send_sem=ssem.at[0], recv_sem=krecv.at[h, j],
            device_id=(sp, peer), device_id_type=MESH,
        )
        if pred is None:
            cp.wait_recv()
        else:
            pl.when(pred)(cp.wait_recv)

    def send_along_z(h, j):
        send(z < 3, h, j, (sp + RING) % SHARDS)
        send(z == 0, h, j, 3 * RING + y)
        send((z == 1) & (core == 1), h, j, y)

    def send_along_y(pred, h, j):
        send(pred, h, j, y_up)
        send(pred, h, j, y_down)

    def gate_copy(j, target):
        return pltpu.make_async_remote_copy(
            src_ref=gates.at[j], dst_ref=gates.at[j], send_sem=gsem.at[target], recv_sem=grecv.at[j],
            device_id=(target, tp), device_id_type=MESH,
        )

    for k in range(1, SHARDS):
        target = (sp + k) % SHARDS
        start(sp + k < SHARDS, gate_copy(sp, target))

    send_along_y(None, 0, sp)
    send_along_z(1, sp)
    send_along_y(None, 1, sp)
    send_along_z(0, sp)

    loads["wf"].wait()
    loads["wrv"].wait()
    loads["slack"].wait()
    loads["extra"].wait()
    fr = dot(n_v[...], wfr[...])
    forget = slack_v[...] * (1.0 / (1.0 + jnp.exp(fr[:, :LANES])))
    rec_value = fr[:, LANES:].astype(BF16)
    extra = jnp.broadcast_to(extra_v[...], (LANES, ROWS)).T
    row_at, col_at = iota((ROWS, ROWS), 0), iota((ROWS, ROWS), 1)
    causal = col_at <= row_at
    lower = jnp.where(causal, 1.0, 0.0).astype(BF16)
    sums = dot(lower, jnp.concatenate(split3(jnp.log1p(-forget)) + split3(extra), axis=1))
    share_sum = sums[:, :LANES] + sums[:, LANES : 2 * LANES] + sums[:, 2 * LANES : 3 * LANES]
    extra_sum = sums[:, 3 * LANES : 4 * LANES] + sums[:, 4 * LANES : 5 * LANES] + sums[:, 5 * LANES :]
    share_end = share_sum[ROWS - 1 :, :]
    extra_end = extra_sum[ROWS - 1 :, :]
    closing = (forget * jnp.exp((share_end - share_sum) + (extra_end - extra_sum))).astype(BF16)
    state_t = dot(fr[:, LANES:].T.astype(BF16), closing)

    def state_message(state, decay):
        hi, mid, lo = (part.astype(F32) for part in split3(decay))
        at = iota((16, LANES), 0)
        tail = jnp.where(at == 0, hi, jnp.where(at == 1, mid, jnp.where(at == 2, lo, 0.0)))
        return state.astype(BF16), tail.astype(BF16)

    body, tail = state_message(state_t, share_end + extra_end)
    st_row[y, :LANES] = body
    st_row[y, LANES:] = tail

    def row_copy(j, target, n):
        return pltpu.make_async_remote_copy(
            src_ref=st_row.at[j], dst_ref=st_row.at[j], send_sem=rsem.at[n], recv_sem=rrecv.at[j],
            device_id=(target, tp), device_id_type=MESH,
        )

    def col_copy(j, target, n):
        return pltpu.make_async_remote_copy(
            src_ref=st_col.at[j], dst_ref=st_col.at[j], send_sem=csem.at[n], recv_sem=crecv.at[j],
            device_id=(target, tp), device_id_type=MESH,
        )

    for n in range(1, RING):
        start(None, row_copy(y, z * RING + (y + n) % RING, n))

    loads["wq"].wait()
    loads["wrq"].wait()
    loads["qg"].wait()
    qq = dot(n_v[...], wqq[...])
    queries = (half_rms(qq[:, :LANES], twice(qg_v[...])).astype(BF16).astype(F32)) * (HALF**-0.5)
    q_v[0] = jnp.where(low, queries, 0.0).astype(BF16)
    q_v[1] = jnp.where(low, 0.0, queries).astype(BF16)

    rq = qq[:, LANES:]
    rec_query = rq / (1.0 + jnp.exp(-rq))
    scores = dot_nt((rec_query * jnp.exp(share_sum)).astype(BF16), (forget * jnp.exp(-share_sum)).astype(BF16))
    differ = jnp.concatenate([extra_sum, extra_sum], axis=1) - extra_sum.T[:1, :]
    scores = scores * jnp.exp(jnp.where(causal, differ, NEGATIVE))
    rec_v[...] = dot(scores.astype(BF16), rec_value)
    visq_v[...] = (rec_query * jnp.exp(share_sum + extra_sum)).astype(BF16)

    loads["wog"].wait()
    og = dot(n_v[...], wog[...])
    outgate_v[...] = og / (1.0 + jnp.exp(-og))

    def attend(blocks, first=False, shown=None):
        for h in range(2):
            parts = []
            for i, j in enumerate(blocks):
                gate = gates[j, h : h + 1, :]
                if shown is not None:
                    gate = jnp.where(shown[i], gate, -NEGATIVE)
                part = dot_nt(q_v[h], kv[h, j]) - gate
                parts.append(jnp.where(causal, part, NEGATIVE) if first else part)
            widest = parts[0]
            for part in parts[1:]:
                widest = jnp.maximum(widest, part)
            top = jnp.max(widest, axis=-1, keepdims=True)
            if not first:
                old = m_v[h]
                top = jnp.maximum(old[:, :1], top)
            summed = None if first else acc_v[h] * jnp.exp(old - top)
            for part, j in zip(parts, blocks):
                weights = jnp.exp(part - top).astype(BF16)
                block = kv[h, j]
                ones = jnp.ones_like(block)
                right = jnp.where(low, ones, block) if h == 0 else jnp.where(low, block, ones)
                term = dot(weights, right)
                summed = term if summed is None else summed + term
            acc_v[h] = summed
            m_v[h] = jnp.broadcast_to(top, (ROWS, LANES))

    attend([sp], first=True)

    loads["woa"].wait()
    loads["wor"].wait()
    wo_copy = pltpu.make_async_remote_copy(
        src_ref=wo_own, dst_ref=wo_peer, send_sem=psem.at[0], recv_sem=precv.at[0],
        device_id=(sp, peer), device_id_type=MESH,
    )
    start(None, wo_copy)

    def wait_gate(valid, j):
        pl.when(valid)(gate_copy(j, j).wait_recv)

    hops = {0: 0, 1: 1, 3: 1, 2: 2}
    plan = sorted(
        ((back, up) for back in (0, 1, 3, 2) for up in (0, 1, 3, 2) if (back, up) != (0, 0)),
        key=lambda e: hops[e[0]] + hops[e[1]],
    )

    def shard_of(back, up):
        return ((z + RING - back) % RING) * RING + (y + up) % RING

    def relay_z(valid, h, j, back):
        if back == 1:
            send((z == 1) & (core == 0) | (z == 2) & (core == 0), h, j, (sp + RING) % SHARDS)
        if back == 3:
            send((z == 3) & (core == 1), h, j, 2 * RING + y)

    def handle(h, back, up):
        valid = None if back == 0 else z >= back
        j = shard_of(back, up)
        arrive(valid, h, j)
        if h == 0:
            if back == 0:
                if up == 3:
                    send(core == 0, h, j, y_up)
                if up == 1:
                    send(core == 1, h, j, y_down)
                send_along_z(h, j)
            else:
                relay_z(valid, h, j, back)
        else:
            if up == 0:
                relay_z(valid, h, j, back)
                send_along_y(valid, h, j)
            else:
                fine = core == (0 if up == 3 else 1)
                if up != 2:
                    send(fine if valid is None else fine & valid, h, j, y_up if up == 3 else y_down)
        if back == 1 and (h == 0 or up == 0):
            through = (z == 0) & (core == 1)
            jj = RING + (y + up) % RING
            arrive(through, h, jj)
            send(through, h, jj, 3 * RING + y)

    def attend_own_row():
        blocks = [shard_of(0, up) for up in (1, 2, 3)]
        shown = [y + up >= RING for up in (1, 2, 3)]
        for valid, j in zip(shown, blocks):
            wait_gate(valid, j)

        @pl.when(y > 0)
        def _():
            attend(blocks, shown=shown)

    def attend_row(back, ups):
        @pl.when(z >= back)
        def _():
            blocks = [shard_of(back, up) for up in ups]
            for j in blocks:
                gate_copy(j, j).wait_recv()
            attend(blocks)

    def read_state(ref, j):
        tail = ref[j, LANES:].astype(F32)
        return ref[j, :LANES].astype(F32), tail[0:1] + tail[1:2] + tail[2:3]

    def combine_row():
        for n in range(1, RING):
            row_copy((y + n) % RING, sp, n).wait_recv()
        before, decay = jnp.zeros((LANES, LANES), F32), jnp.zeros((1, LANES), F32)
        mine, mine_decay = before, decay
        for k in range(RING):
            state, log = read_state(st_row, k)
            before = jnp.exp(log) * before + state
            decay = decay + log
            mine = jnp.where(k < y, before, mine)
            mine_decay = jnp.where(k < y, decay, mine_decay)
        in_v[0] = mine
        in_v[1, 0:1] = mine_decay
        body, tail = state_message(before, decay)
        st_col[z, :LANES] = body
        st_col[z, LANES:] = tail
        for n in range(1, RING):
            start(z + n < RING, col_copy(z, ((z + n) % RING) * RING + y, n))

    def combine_col():
        for n in range(1, RING):
            pl.when(z >= n)(col_copy((z + RING - n) % RING, sp, n).wait_recv)
        in_v[2] = jnp.zeros((LANES, LANES), F32)
        for k in range(RING - 1):

            @pl.when(k < z)
            def _():
                state, log = read_state(st_col, k)
                in_v[2] = jnp.exp(log) * in_v[2] + state

        incoming = jnp.exp(in_v[1, 0:1]) * in_v[2] + in_v[0]
        recurrent = rec_v[...] + dot_nt(visq_v[...], incoming.astype(BF16))
        mean = jnp.mean(recurrent * recurrent, axis=-1, keepdims=True)
        return (recurrent * lax.rsqrt(mean + EPSILON) * rg_v[...] * outgate_v[...]).astype(BF16)

    def handle_level(level):
        for back, up in plan:
            if hops[back] + hops[up] == level:
                handle(0, back, up)
                handle(1, back, up)

    handle_level(1)
    handle_level(2)
    combine_row()
    attend_own_row()
    handle_level(3)
    attend_row(1, (0, 1, 3, 2))
    attend_row(3, (0, 1, 3, 2))
    attend_row(2, (0, 1, 3))
    loads["ag"].wait()
    loads["rg"].wait()
    rec_out = combine_col()
    handle_level(4)
    attend_row(2, (2,))

    a0, a1 = acc_v[0], acc_v[1]
    totals = jnp.where(low, a0, a1)
    attention = pltpu.roll(jnp.where(low, a1, a0), HALF, 1) / totals
    attn_out = half_rms(attention, ag_v[...]).astype(BF16)
    for b in range(8):
        rows = slice(32 * b, 32 * b + 32)
        at = slice(32 * (b // 2), 32 * (b // 2) + 32)
        act[b % 2, at, :LANES] = attn_out[rows]
        act[b % 2, at, LANES:] = rec_out[rows]
    act_copy = pltpu.make_async_remote_copy(
        src_ref=act.at[1 - core], dst_ref=act_peer, send_sem=psem.at[1], recv_sem=precv.at[1],
        device_id=(sp, peer), device_id_type=MESH,
    )
    start(None, act_copy)
    log_sum = (jnp.where(low, m_v[0], m_v[1]) + jnp.log(totals)).T
    lse_ref[0:1, :] = log_sum[0:1, :] + gates[sp, 0:1, :]
    lse_ref[1:2, :] = log_sum[HALF : HALF + 1, :] + gates[sp, 1:2, :]
    wo_copy.wait_recv()
    act_copy.wait_recv()

    e_next = (xc + 2 * core + 3) % RING
    e_prev = (xc + 5 - 2 * core) % RING
    far = (xc + 2) % RING
    to_next = 2 * e_next + core
    to_prev = 2 * e_prev + core

    def x_copy(kind, c, src, dst, target):
        return pltpu.make_async_remote_copy(
            src_ref=src, dst_ref=dst, send_sem=xsem.at[kind, c], recv_sem=xrecv.at[kind, c],
            device_id=(sp, target), device_id_type=MESH,
        )

    mine = act[core]
    theirs = act_peer[...]
    for c in range(CHUNKS):
        cols = slice(c * CHUNK, (c + 1) * CHUNK)
        product = dot(mine, wo_own[:, cols]) + dot(theirs, wo_peer[:, cols])
        for b in range(RING):
            part[c, b] = product[32 * b : 32 * b + 32].astype(BF16)
        start(None, x_copy(0, c, part.at[c, far], xt.at[c], to_next))
    for c in range(CHUNKS):
        start(None, x_copy(1, c, part.at[c, e_prev], xd.at[c], to_prev))
    for c in range(CHUNKS):
        x_copy(0, c, part.at[c, far], xt.at[c], to_next).wait_recv()
        xsum[c] = (xt[c].astype(F32) + part[c, e_next].astype(F32)).astype(BF16)
        start(None, x_copy(2, c, xsum.at[c], xs.at[c], to_next))
    for c in range(CHUNKS):
        x_copy(1, c, part.at[c, e_prev], xd.at[c], to_prev).wait_recv()
        x_copy(2, c, xsum.at[c], xs.at[c], to_next).wait_recv()
        total = part[c, xc].astype(F32) + xd[c].astype(F32) + xs[c].astype(F32)
        mixed_ref[:, c * CHUNK : (c + 1) * CHUNK] = total.astype(BF16)
    for pred, cp in pending:
        if pred is None:
            cp.wait_send()
        else:
            pl.when(pred)(cp.wait_send)


def body(*args):
    (
        layer_input_rows, input_norm_gain, query_weight, key_weight, value_weight, query_norm_gain,
        key_norm_gain, cumulative_gate, attention_norm_gain, recurrence_query_weight, forget_weight,
        recurrence_value_weight, output_gate_weight, gate_lower_slack, extra_log_decay,
        recurrence_norm_gain, attention_output_weight, recurrence_output_weight,
    ) = args
    operands = (
        layer_input_rows, input_norm_gain[None], query_weight, key_weight, value_weight,
        query_norm_gain[None], key_norm_gain[None], cumulative_gate.T, attention_norm_gain[None],
        recurrence_query_weight, forget_weight, recurrence_value_weight, output_gate_weight,
        gate_lower_slack[None], extra_log_decay.T, recurrence_norm_gain[None],
        attention_output_weight, recurrence_output_weight,
    )
    dma = pltpu.SemaphoreType.DMA
    mixed, lse = pl.pallas_call(
        kernel,
        name="mixer",
        out_shape=(
            jax.ShapeDtypeStruct((ROWS // 8, WIDTH), BF16),
            jax.ShapeDtypeStruct((2, ROWS), F32),
        ),
        in_specs=[pl.BlockSpec(memory_space=pltpu.HBM)] * len(operands),
        out_specs=(pl.BlockSpec(memory_space=pltpu.VMEM), pl.BlockSpec(memory_space=pltpu.VMEM)),
        scratch_shapes=[
            pltpu.VMEM((ROWS, WIDTH), BF16),
            pltpu.VMEM((ROWS, WIDTH), BF16),
            pltpu.VMEM((1, WIDTH), F32),
            pltpu.VMEM((1, HALF), F32),
            pltpu.VMEM((1, HALF), F32),
            pltpu.VMEM((1, LANES), F32),
            pltpu.VMEM((1, LANES), F32),
            pltpu.VMEM((1, ROWS), F32),
            pltpu.VMEM((1, LANES), F32),
            pltpu.VMEM((WIDTH, 2 * LANES), BF16),
            pltpu.VMEM((WIDTH, 2 * LANES), BF16),
            pltpu.VMEM((WIDTH, 2 * LANES), BF16),
            pltpu.VMEM((WIDTH, LANES), BF16),
            pltpu.VMEM((2 * LANES, WIDTH), BF16),
            pltpu.VMEM((2 * LANES, WIDTH), BF16),
            pltpu.VMEM((SHARDS, 2, ROWS), F32),
            pltpu.VMEM((2, SHARDS, ROWS, LANES), BF16),
            pltpu.VMEM((2, ROWS, LANES), BF16),
            pltpu.VMEM((2, ROWS, LANES), F32),
            pltpu.VMEM((2, ROWS, LANES), F32),
            pltpu.VMEM((RING, STATE_MSG, LANES), BF16),
            pltpu.VMEM((RING, STATE_MSG, LANES), BF16),
            pltpu.VMEM((3, LANES, LANES), F32),
            pltpu.VMEM((ROWS, LANES), F32),
            pltpu.VMEM((ROWS, LANES), BF16),
            pltpu.VMEM((ROWS, LANES), F32),
            pltpu.VMEM((2, ROWS // 2, 2 * LANES), BF16),
            pltpu.VMEM((ROWS // 2, 2 * LANES), BF16),
            pltpu.VMEM((CHUNKS, RING, ROWS // 8, CHUNK), BF16),
            pltpu.VMEM((CHUNKS, ROWS // 8, CHUNK), BF16),
            pltpu.VMEM((CHUNKS, ROWS // 8, CHUNK), BF16),
            pltpu.VMEM((CHUNKS, ROWS // 8, CHUNK), BF16),
            pltpu.VMEM((CHUNKS, ROWS // 8, CHUNK), BF16),
            dma((18,)),
            dma((SHARDS,)),
            dma((SHARDS,)),
            dma((KV_SENDS,)),
            dma((2, SHARDS)),
            dma((RING,)),
            dma((RING,)),
            dma((RING,)),
            dma((RING,)),
            dma((2,)),
            dma((2,)),
            dma((3, CHUNKS)),
            dma((3, CHUNKS)),
        ],
        compiler_params=pltpu.CompilerParams(
            collective_id=0, has_side_effects=True, vmem_limit_bytes=60 * 1024 * 1024
        ),
    )(*operands)
    return mixed, lse.T


def solution(mesh):
    both = P("sp", "tp")
    placed = (
        P("sp", None), P(), P(None, "tp"), P(None, "tp"), P(None, "tp"), P(), P(), both, P("tp"),
        P(None, "tp"), P(None, "tp"), P(None, "tp"), P(None, "tp"), P("tp"), both, P("tp"),
        P("tp", None), P("tp", None),
    )
    return jax.shard_map(
        body, mesh=mesh, in_specs=placed, out_specs=(P(("sp", "tp"), None), both), check_vma=False
    )
```

```python
import jax
import jax.numpy as jnp
from jax import lax
from jax.experimental import pallas as pl
from jax.experimental.pallas import tpu as pltpu
from jax.sharding import PartitionSpec as P

F32 = jnp.float32
BF16 = jnp.bfloat16
MESH = pl.DeviceIdType.MESH
EPSILON = 1e-06
ROWS = 256
WIDTH = 2048
LANES = 128
HALF = 64
SHARDS = 16
RING = 4
CHUNKS = 4
CHUNK = WIDTH // CHUNKS
STATE_MSG = 144
KV_SENDS = 80
NEGATIVE = -1e30


def dot(a, b):
    return jnp.dot(a, b, preferred_element_type=F32)


def dot_nt(a, b):
    return lax.dot_general(a, b, (((1,), (1,)), ((), ())), preferred_element_type=F32)


def split2(v):
    hi = v.astype(BF16)
    return hi, (v - hi.astype(F32)).astype(BF16)


def split3(v):
    hi = v.astype(BF16)
    rest = v - hi.astype(F32)
    mid = rest.astype(BF16)
    return hi, mid, (rest - mid.astype(F32)).astype(BF16)


def iota(shape, dim):
    return lax.broadcasted_iota(jnp.int32, shape, dim)


def kernel(
    x_hbm, xg_hbm, wq_hbm, wk_hbm, wv_hbm, qg_hbm, kg_hbm, gate_hbm, ag_hbm,
    wrq_hbm, wf_hbm, wrv_hbm, wog_hbm, slack_hbm, extra_hbm, rg_hbm, woa_hbm, wor_hbm,
    own_ref, direct_ref, summed_ref, lse_ref,
    x_v, n_v, xg_v, qg_v, kg_v, ag_v, slack_v, extra_v, rg_v,
    wkv, wfr, wqq, wog, woa, wor, product_v,
    gates, kv, q_v, m_v, acc_v,
    st_row, st_col, in_v, rec_v, visq_v, outgate_v,
    act_r, act_a, peer_r, peer_a, part, xt, xsum,
    lsem, gsem, grecv, ssem, krecv, rsem, rrecv, csem, crecv, psem, precv, xsem, xrecv,
):
    sp = lax.axis_index("sp")
    tp = lax.axis_index("tp")
    z, y = sp // RING, sp % RING
    xc, core = tp // 2, tp % 2
    peer = 2 * xc + 1 - core

    loads = {}

    def load(name, src, dst):
        cp = pltpu.make_async_copy(src, dst, lsem.at[len(loads)])
        cp.start()
        loads[name] = cp

    for r in range(0, ROWS, HALF):
        load(("x", r), x_hbm.at[pl.ds(r, HALF)], x_v.at[pl.ds(r, HALF)])
    load("xg", xg_hbm, xg_v)
    load("wk", wk_hbm, wkv.at[:, pl.ds(0, LANES)])
    load("wv", wv_hbm, wkv.at[:, pl.ds(LANES, LANES)])
    load("kg", kg_hbm, kg_v)
    load("gate", gate_hbm, gates.at[sp])

    barrier = pltpu.get_barrier_semaphore()
    for k in range(1, SHARDS):
        pl.semaphore_signal(barrier, inc=1, device_id=((sp + k) % SHARDS, tp), device_id_type=MESH)
    x_right = 2 * ((xc + 1) % RING) + core
    x_left = 2 * ((xc + 3) % RING) + core
    for other in (x_right, x_left, peer):
        pl.semaphore_signal(barrier, inc=1, device_id=(sp, other), device_id_type=MESH)

    pending = []

    def start(pred, cp):
        if pred is None:
            cp.start()
        else:
            pl.when(pred)(cp.start)
        pending.append((pred, cp))

    loads["xg"].wait()
    step = 32
    for r in range(0, ROWS, step):
        if r % HALF == 0:
            loads["x", r].wait()
        if r == HALF:
            load("wf", wf_hbm, wfr.at[:, pl.ds(0, LANES)])
            load("wrv", wrv_hbm, wfr.at[:, pl.ds(LANES, LANES)])
            load("slack", slack_hbm, slack_v)
            load("extra", extra_hbm, extra_v)
            load("wq", wq_hbm, wqq.at[:, pl.ds(0, LANES)])
            load("wrq", wrq_hbm, wqq.at[:, pl.ds(LANES, LANES)])
            load("qg", qg_hbm, qg_v)
            load("wog", wog_hbm, wog)
            load("ag", ag_hbm, ag_v)
            load("rg", rg_hbm, rg_v)
            load("woa", woa_hbm, woa.at[pl.ds(0, LANES)])
            load("wor", wor_hbm, wor.at[pl.ds(0, LANES)])
        xf = x_v[r : r + step, :].astype(F32)
        mean = jnp.sum(xf * xf, axis=-1, keepdims=True) * (1.0 / WIDTH)
        n_v[r : r + step, :] = (xf * lax.rsqrt(mean + EPSILON) * xg_v[...]).astype(BF16)

    lane = iota((ROWS, LANES), 1)
    low = lane < HALF
    same_half = (iota((LANES, LANES), 0) // HALF == iota((LANES, LANES), 1) // HALF)
    halves = jnp.where(same_half, 1.0, 0.0).astype(BF16)

    def twice(gain):
        return jnp.concatenate([gain, gain], axis=1)

    def half_rms(v, gain):
        hi, lo = split2(v * v)
        mean = (dot(hi, halves) + dot(lo, halves)) * (1.0 / HALF)
        return v * lax.rsqrt(mean + EPSILON) * gain

    loads["wk"].wait()
    loads["wv"].wait()
    loads["kg"].wait()
    kv_f = dot(n_v[...], wkv[...])
    keys = half_rms(kv_f[:, :LANES], twice(kg_v[...]))
    swapped = pltpu.roll(kv_f[:, LANES:], HALF, 1)
    kv[0, sp] = jnp.where(low, keys, swapped).astype(BF16)
    kv[1, sp] = jnp.where(low, swapped, keys).astype(BF16)

    loads["gate"].wait()
    pl.semaphore_wait(barrier, SHARDS - 1 + 3)

    y_up = z * RING + (y + 1) % RING
    y_down = z * RING + (y + 3) % RING
    count = [0]

    def send(pred, h, j, target):
        n = count[0]
        count[0] += 1
        start(
            pred,
            pltpu.make_async_remote_copy(
                src_ref=kv.at[h, j], dst_ref=kv.at[h, j], send_sem=ssem.at[n], recv_sem=krecv.at[h, j],
                device_id=(target, tp), device_id_type=MESH,
            ),
        )

    def arrive(pred, h, j):
        cp = pltpu.make_async_remote_copy(
            src_ref=kv.at[h, j], dst_ref=kv.at[h, j], send_sem=ssem.at[0], recv_sem=krecv.at[h, j],
            device_id=(sp, peer), device_id_type=MESH,
        )
        if pred is None:
            cp.wait_recv()
        else:
            pl.when(pred)(cp.wait_recv)

    def send_along_z(h, j):
        send(z < 3, h, j, (sp + RING) % SHARDS)
        send(z == 0, h, j, 3 * RING + y)
        send((z == 1) & (core == 1), h, j, y)

    def send_along_y(pred, h, j):
        send(pred, h, j, y_up)
        send(pred, h, j, y_down)

    def gate_copy(j, target):
        return pltpu.make_async_remote_copy(
            src_ref=gates.at[j], dst_ref=gates.at[j], send_sem=gsem.at[target], recv_sem=grecv.at[j],
            device_id=(target, tp), device_id_type=MESH,
        )

    for k in range(1, SHARDS):
        target = (sp + k) % SHARDS
        start(sp + k < SHARDS, gate_copy(sp, target))

    send_along_y(None, 0, sp)
    send_along_z(1, sp)
    send_along_y(None, 1, sp)
    send_along_z(0, sp)

    loads["wf"].wait()
    loads["wrv"].wait()
    loads["slack"].wait()
    loads["extra"].wait()
    fr = dot(n_v[...], wfr[...])
    forget = slack_v[...] * (1.0 / (1.0 + jnp.exp(fr[:, :LANES])))
    rec_value = fr[:, LANES:].astype(BF16)
    extra = jnp.broadcast_to(extra_v[...], (LANES, ROWS)).T
    row_at, col_at = iota((ROWS, ROWS), 0), iota((ROWS, ROWS), 1)
    causal = col_at <= row_at
    lower = jnp.where(causal, 1.0, 0.0).astype(BF16)
    sums = dot(lower, jnp.concatenate(split3(jnp.log1p(-forget)) + split3(extra), axis=1))
    share_sum = sums[:, :LANES] + sums[:, LANES : 2 * LANES] + sums[:, 2 * LANES : 3 * LANES]
    extra_sum = sums[:, 3 * LANES : 4 * LANES] + sums[:, 4 * LANES : 5 * LANES] + sums[:, 5 * LANES :]
    share_end = share_sum[ROWS - 1 :, :]
    extra_end = extra_sum[ROWS - 1 :, :]
    closing = (forget * jnp.exp((share_end - share_sum) + (extra_end - extra_sum))).astype(BF16)
    state_t = dot(fr[:, LANES:].T.astype(BF16), closing)

    def state_message(state, decay):
        hi, mid, lo = (part.astype(F32) for part in split3(decay))
        at = iota((16, LANES), 0)
        tail = jnp.where(at == 0, hi, jnp.where(at == 1, mid, jnp.where(at == 2, lo, 0.0)))
        return state.astype(BF16), tail.astype(BF16)

    body, tail = state_message(state_t, share_end + extra_end)
    st_row[y, :LANES] = body
    st_row[y, LANES:] = tail

    def row_copy(j, target, n):
        return pltpu.make_async_remote_copy(
            src_ref=st_row.at[j], dst_ref=st_row.at[j], send_sem=rsem.at[n], recv_sem=rrecv.at[j],
            device_id=(target, tp), device_id_type=MESH,
        )

    def col_copy(j, target, n):
        return pltpu.make_async_remote_copy(
            src_ref=st_col.at[j], dst_ref=st_col.at[j], send_sem=csem.at[n], recv_sem=crecv.at[j],
            device_id=(target, tp), device_id_type=MESH,
        )

    for n in range(1, RING):
        start(None, row_copy(y, z * RING + (y + n) % RING, n))

    loads["wq"].wait()
    loads["wrq"].wait()
    loads["qg"].wait()
    qq = dot(n_v[...], wqq[...])
    queries = (half_rms(qq[:, :LANES], twice(qg_v[...])).astype(BF16).astype(F32)) * (HALF**-0.5)
    q_v[0] = jnp.where(low, queries, 0.0).astype(BF16)
    q_v[1] = jnp.where(low, 0.0, queries).astype(BF16)

    rq = qq[:, LANES:]
    rec_query = rq / (1.0 + jnp.exp(-rq))
    scores = dot_nt((rec_query * jnp.exp(share_sum)).astype(BF16), (forget * jnp.exp(-share_sum)).astype(BF16))
    differ = jnp.concatenate([extra_sum, extra_sum], axis=1) - extra_sum.T[:1, :]
    scores = scores * jnp.exp(jnp.where(causal, differ, NEGATIVE))
    rec_v[...] = dot(scores.astype(BF16), rec_value)
    visq_v[...] = (rec_query * jnp.exp(share_sum + extra_sum)).astype(BF16)

    loads["wog"].wait()
    og = dot(n_v[...], wog[...])
    outgate_v[...] = og / (1.0 + jnp.exp(-og))

    def attend(blocks, first=False, shown=None):
        for h in range(2):
            parts = []
            for i, j in enumerate(blocks):
                gate = gates[j, h : h + 1, :]
                if shown is not None:
                    gate = jnp.where(shown[i], gate, -NEGATIVE)
                part = dot_nt(q_v[h], kv[h, j]) - gate
                parts.append(jnp.where(causal, part, NEGATIVE) if first else part)
            widest = parts[0]
            for part in parts[1:]:
                widest = jnp.maximum(widest, part)
            top = jnp.max(widest, axis=-1, keepdims=True)
            if not first:
                old = m_v[h]
                top = jnp.maximum(old[:, :1], top)
            summed = None if first else acc_v[h] * jnp.exp(old - top)
            for part, j in zip(parts, blocks):
                weights = jnp.exp(part - top).astype(BF16)
                block = kv[h, j]
                ones = jnp.ones_like(block)
                right = jnp.where(low, ones, block) if h == 0 else jnp.where(low, block, ones)
                term = dot(weights, right)
                summed = term if summed is None else summed + term
            acc_v[h] = summed
            m_v[h] = jnp.broadcast_to(top, (ROWS, LANES))

    attend([sp], first=True)

    def to_peer(n, src, dst):
        return pltpu.make_async_remote_copy(
            src_ref=src, dst_ref=dst, send_sem=psem.at[n], recv_sem=precv.at[n],
            device_id=(sp, peer), device_id_type=MESH,
        )

    loads["woa"].wait()
    loads["wor"].wait()
    wor_copy = to_peer(0, wor.at[pl.ds(0, LANES)], wor.at[pl.ds(LANES, LANES)])
    woa_copy = to_peer(1, woa.at[pl.ds(0, LANES)], woa.at[pl.ds(LANES, LANES)])
    start(None, wor_copy)
    start(None, woa_copy)

    def wait_gate(valid, j):
        pl.when(valid)(gate_copy(j, j).wait_recv)

    hops = {0: 0, 1: 1, 3: 1, 2: 2}
    plan = sorted(
        ((back, up) for back in (0, 1, 3, 2) for up in (0, 1, 3, 2) if (back, up) != (0, 0)),
        key=lambda e: hops[e[0]] + hops[e[1]],
    )

    def shard_of(back, up):
        return ((z + RING - back) % RING) * RING + (y + up) % RING

    def relay_z(valid, h, j, back):
        if back == 1:
            send((z == 1) & (core == 0) | (z == 2) & (core == 0), h, j, (sp + RING) % SHARDS)
        if back == 3:
            send((z == 3) & (core == 1), h, j, 2 * RING + y)

    def handle(h, back, up):
        valid = None if back == 0 else z >= back
        j = shard_of(back, up)
        arrive(valid, h, j)
        if h == 0:
            if back == 0:
                if up == 3:
                    send(core == 0, h, j, y_up)
                if up == 1:
                    send(core == 1, h, j, y_down)
                send_along_z(h, j)
            else:
                relay_z(valid, h, j, back)
        else:
            if up == 0:
                relay_z(valid, h, j, back)
                send_along_y(valid, h, j)
            else:
                fine = core == (0 if up == 3 else 1)
                if up != 2:
                    send(fine if valid is None else fine & valid, h, j, y_up if up == 3 else y_down)
        if back == 1 and (h == 0 or up == 0):
            through = (z == 0) & (core == 1)
            jj = RING + (y + up) % RING
            arrive(through, h, jj)
            send(through, h, jj, 3 * RING + y)

    def attend_own_row():
        blocks = [shard_of(0, up) for up in (1, 2, 3)]
        shown = [y + up >= RING for up in (1, 2, 3)]
        for valid, j in zip(shown, blocks):
            wait_gate(valid, j)

        @pl.when(y > 0)
        def _():
            attend(blocks, shown=shown)

    def attend_row(back, ups):
        @pl.when(z >= back)
        def _():
            blocks = [shard_of(back, up) for up in ups]
            for j in blocks:
                gate_copy(j, j).wait_recv()
            attend(blocks)

    def read_state(ref, j):
        tail = ref[j, LANES:].astype(F32)
        return ref[j, :LANES].astype(F32), tail[0:1] + tail[1:2] + tail[2:3]

    def combine_row():
        for n in range(1, RING):
            row_copy((y + n) % RING, sp, n).wait_recv()
        before, decay = jnp.zeros((LANES, LANES), F32), jnp.zeros((1, LANES), F32)
        mine, mine_decay = before, decay
        for k in range(RING):
            state, log = read_state(st_row, k)
            before = jnp.exp(log) * before + state
            decay = decay + log
            mine = jnp.where(k < y, before, mine)
            mine_decay = jnp.where(k < y, decay, mine_decay)
        in_v[0] = mine
        in_v[1, 0:1] = mine_decay
        body, tail = state_message(before, decay)
        st_col[z, :LANES] = body
        st_col[z, LANES:] = tail
        for n in range(1, RING):
            start(z + n < RING, col_copy(z, ((z + n) % RING) * RING + y, n))

    def combine_col():
        for n in range(1, RING):
            pl.when(z >= n)(col_copy((z + RING - n) % RING, sp, n).wait_recv)
        in_v[2] = jnp.zeros((LANES, LANES), F32)
        for k in range(RING - 1):

            @pl.when(k < z)
            def _():
                state, log = read_state(st_col, k)
                in_v[2] = jnp.exp(log) * in_v[2] + state

        incoming = jnp.exp(in_v[1, 0:1]) * in_v[2] + in_v[0]
        recurrent = rec_v[...] + dot_nt(visq_v[...], incoming.astype(BF16))
        mean = jnp.mean(recurrent * recurrent, axis=-1, keepdims=True)
        return (recurrent * lax.rsqrt(mean + EPSILON) * rg_v[...] * outgate_v[...]).astype(BF16)

    def by_owner(ref, rows):
        for b in range(8):
            ref[b % 2, 32 * (b // 2) : 32 * (b // 2) + 32, :] = rows[32 * b : 32 * b + 32]

    def share_recurrence():
        loads["rg"].wait()
        by_owner(act_r, combine_col())
        start(None, to_peer(2, act_r.at[1 - core], peer_r))

    def project_recurrence():
        wor_copy.wait_recv()
        to_peer(2, act_r.at[1 - core], peer_r).wait_recv()
        both = jnp.concatenate([act_r[core], peer_r[...]], axis=1)
        for c in range(CHUNKS):
            cols = slice(c * CHUNK, (c + 1) * CHUNK)
            product_v[:, cols] = dot(both, wor[:, cols])

    def handle_all(events):
        for h, back, up in events:
            handle(h, back, up)

    handle_all((
        (1, 3, 0), (1, 1, 0), (0, 0, 3), (0, 0, 1), (1, 0, 1), (1, 0, 3), (0, 3, 0), (0, 3, 3), (0, 1, 0),
        (1, 3, 1), (1, 2, 0), (1, 3, 3), (1, 1, 3), (1, 1, 1), (1, 0, 2), (0, 3, 1), (0, 0, 2), (0, 1, 1),
    ))
    attend_own_row()
    handle_all(((0, 2, 0), (1, 2, 3), (0, 1, 3)))
    combine_row()
    handle_all(((0, 3, 2), (1, 2, 1), (1, 3, 2)))
    attend_row(3, (0, 1, 3, 2))
    handle_all(((0, 1, 2), (1, 1, 2), (0, 2, 1)))
    attend_row(1, (0, 1, 3, 2))
    share_recurrence()
    handle_all(((0, 2, 3),))
    project_recurrence()
    handle_all(((0, 2, 2), (1, 2, 2)))
    attend_row(2, (0, 1, 3, 2))

    a0, a1 = acc_v[0], acc_v[1]
    totals = jnp.where(low, a0, a1)
    loads["ag"].wait()
    attention = pltpu.roll(jnp.where(low, a1, a0), HALF, 1) / totals
    attn_out = half_rms(attention, ag_v[...]).astype(BF16)
    by_owner(act_a, attn_out)
    act_copy = to_peer(3, act_a.at[1 - core], peer_a)
    start(None, act_copy)
    log_sum = (jnp.where(low, m_v[0], m_v[1]) + jnp.log(totals)).T
    lse_ref[0:1, :] = log_sum[0:1, :] + gates[sp, 0:1, :]
    lse_ref[1:2, :] = log_sum[HALF : HALF + 1, :] + gates[sp, 1:2, :]
    woa_copy.wait_recv()
    act_copy.wait_recv()

    e_next = (xc + 2 * core + 3) % RING
    e_prev = (xc + 5 - 2 * core) % RING
    far = (xc + 2) % RING
    to_next = 2 * e_next + core
    to_prev = 2 * e_prev + core

    def x_copy(kind, c, src, dst, target):
        return pltpu.make_async_remote_copy(
            src_ref=src, dst_ref=dst, send_sem=xsem.at[kind, c], recv_sem=xrecv.at[kind, c],
            device_id=(sp, target), device_id_type=MESH,
        )

    both = jnp.concatenate([act_a[core], peer_a[...]], axis=1)
    for c in range(CHUNKS):
        cols = slice(c * CHUNK, (c + 1) * CHUNK)
        product = product_v[:, cols] + dot(both, woa[:, cols])
        for b in range(RING):
            part[c, b] = product[32 * b : 32 * b + 32].astype(BF16)
        start(None, x_copy(0, c, part.at[c, far], xt.at[c], to_next))
    for c in range(CHUNKS):
        start(None, x_copy(1, c, part.at[c, e_prev], direct_ref.at[c], to_prev))
    own_copies = [
        pltpu.make_async_copy(part.at[c, xc], own_ref.at[c], xsem.at[3, c]) for c in range(CHUNKS)
    ]
    for cp in own_copies:
        cp.start()
    for c in range(CHUNKS):
        x_copy(0, c, part.at[c, far], xt.at[c], to_next).wait_recv()
        xsum[c] = (xt[c].astype(F32) + part[c, e_next].astype(F32)).astype(BF16)
        start(None, x_copy(2, c, xsum.at[c], summed_ref.at[c], to_next))
    for cp in own_copies:
        cp.wait()
    for c in range(CHUNKS):
        x_copy(1, c, part.at[c, e_prev], direct_ref.at[c], to_prev).wait_recv()
        x_copy(2, c, xsum.at[c], summed_ref.at[c], to_next).wait_recv()
    for pred, cp in pending:
        if pred is None:
            cp.wait_send()
        else:
            pl.when(pred)(cp.wait_send)


def finish(own_ref, direct_ref, summed_ref, lse_in, mixed_ref, lse_ref):
    for c in range(CHUNKS):
        total = own_ref[c].astype(F32) + direct_ref[c].astype(F32) + summed_ref[c].astype(F32)
        mixed_ref[:, c * CHUNK : (c + 1) * CHUNK] = total.astype(BF16)
    lse_ref[...] = lse_in[...]


def body(*args):
    (
        layer_input_rows, input_norm_gain, query_weight, key_weight, value_weight, query_norm_gain,
        key_norm_gain, cumulative_gate, attention_norm_gain, recurrence_query_weight, forget_weight,
        recurrence_value_weight, output_gate_weight, gate_lower_slack, extra_log_decay,
        recurrence_norm_gain, attention_output_weight, recurrence_output_weight,
    ) = args
    operands = (
        layer_input_rows, input_norm_gain[None], query_weight, key_weight, value_weight,
        query_norm_gain[None], key_norm_gain[None], cumulative_gate.T, attention_norm_gain[None],
        recurrence_query_weight, forget_weight, recurrence_value_weight, output_gate_weight,
        gate_lower_slack[None], extra_log_decay.T, recurrence_norm_gain[None],
        attention_output_weight, recurrence_output_weight,
    )
    dma = pltpu.SemaphoreType.DMA
    own, direct, summed, lse = pl.pallas_call(
        kernel,
        name="mixer",
        out_shape=(
            jax.ShapeDtypeStruct((CHUNKS, ROWS // 8, CHUNK), BF16),
            jax.ShapeDtypeStruct((CHUNKS, ROWS // 8, CHUNK), BF16),
            jax.ShapeDtypeStruct((CHUNKS, ROWS // 8, CHUNK), BF16),
            jax.ShapeDtypeStruct((2, ROWS), F32),
        ),
        in_specs=[pl.BlockSpec(memory_space=pltpu.HBM)] * len(operands),
        out_specs=(pl.BlockSpec(memory_space=pltpu.HBM),) * 3 + (pl.BlockSpec(memory_space=pltpu.VMEM),),
        scratch_shapes=[
            pltpu.VMEM((ROWS, WIDTH), BF16),
            pltpu.VMEM((ROWS, WIDTH), BF16),
            pltpu.VMEM((1, WIDTH), F32),
            pltpu.VMEM((1, HALF), F32),
            pltpu.VMEM((1, HALF), F32),
            pltpu.VMEM((1, LANES), F32),
            pltpu.VMEM((1, LANES), F32),
            pltpu.VMEM((1, ROWS), F32),
            pltpu.VMEM((1, LANES), F32),
            pltpu.VMEM((WIDTH, 2 * LANES), BF16),
            pltpu.VMEM((WIDTH, 2 * LANES), BF16),
            pltpu.VMEM((WIDTH, 2 * LANES), BF16),
            pltpu.VMEM((WIDTH, LANES), BF16),
            pltpu.VMEM((2 * LANES, WIDTH), BF16),
            pltpu.VMEM((2 * LANES, WIDTH), BF16),
            pltpu.VMEM((ROWS // 2, WIDTH), F32),
            pltpu.VMEM((SHARDS, 2, ROWS), F32),
            pltpu.VMEM((2, SHARDS, ROWS, LANES), BF16),
            pltpu.VMEM((2, ROWS, LANES), BF16),
            pltpu.VMEM((2, ROWS, LANES), F32),
            pltpu.VMEM((2, ROWS, LANES), F32),
            pltpu.VMEM((RING, STATE_MSG, LANES), BF16),
            pltpu.VMEM((RING, STATE_MSG, LANES), BF16),
            pltpu.VMEM((3, LANES, LANES), F32),
            pltpu.VMEM((ROWS, LANES), F32),
            pltpu.VMEM((ROWS, LANES), BF16),
            pltpu.VMEM((ROWS, LANES), F32),
            pltpu.VMEM((2, ROWS // 2, LANES), BF16),
            pltpu.VMEM((2, ROWS // 2, LANES), BF16),
            pltpu.VMEM((ROWS // 2, LANES), BF16),
            pltpu.VMEM((ROWS // 2, LANES), BF16),
            pltpu.VMEM((CHUNKS, RING, ROWS // 8, CHUNK), BF16),
            pltpu.VMEM((CHUNKS, ROWS // 8, CHUNK), BF16),
            pltpu.VMEM((CHUNKS, ROWS // 8, CHUNK), BF16),
            dma((21,)),
            dma((SHARDS,)),
            dma((SHARDS,)),
            dma((KV_SENDS,)),
            dma((2, SHARDS)),
            dma((RING,)),
            dma((RING,)),
            dma((RING,)),
            dma((RING,)),
            dma((4,)),
            dma((4,)),
            dma((4, CHUNKS)),
            dma((3, CHUNKS)),
        ],
        compiler_params=pltpu.CompilerParams(
            collective_id=0, has_side_effects=True, vmem_limit_bytes=60 * 1024 * 1024
        ),
    )(*operands)
    mixed, lse = pl.pallas_call(
        finish,
        name="finish",
        out_shape=(
            jax.ShapeDtypeStruct((ROWS // 8, WIDTH), BF16),
            jax.ShapeDtypeStruct((2, ROWS), F32),
        ),
    )(own, direct, summed, lse)
    return mixed, lse.T


def solution(mesh):
    both = P("sp", "tp")
    placed = (
        P("sp", None), P(), P(None, "tp"), P(None, "tp"), P(None, "tp"), P(), P(), both, P("tp"),
        P(None, "tp"), P(None, "tp"), P(None, "tp"), P(None, "tp"), P("tp"), both, P("tp"),
        P("tp", None), P("tp", None),
    )
    return jax.shard_map(
        body, mesh=mesh, in_specs=placed, out_specs=(P(("sp", "tp"), None), both), check_vma=False
    )
```

```python
import functools

import jax
import jax.numpy as jnp
from jax import lax
from jax.experimental import pallas as pl
from jax.experimental.pallas import tpu as pltpu
from jax.sharding import PartitionSpec as P

F32 = jnp.float32
BF16 = jnp.bfloat16
MESH = pl.DeviceIdType.MESH
EPSILON = 1e-06
ROWS = 256
WIDTH = 2048
LANES = 128
HALF = 64
SHARDS = 16
RING = 4
CHUNKS = 4
CHUNK = WIDTH // CHUNKS
STATE_MSG = 144
KV_SENDS = 80
NEGATIVE = -1e30


def dot(a, b):
    return jnp.dot(a, b, preferred_element_type=F32)


def dot_nt(a, b):
    return lax.dot_general(a, b, (((1,), (1,)), ((), ())), preferred_element_type=F32)


def split2(v):
    hi = v.astype(BF16)
    return hi, (v - hi.astype(F32)).astype(BF16)


def split3(v):
    hi = v.astype(BF16)
    rest = v - hi.astype(F32)
    mid = rest.astype(BF16)
    return hi, mid, (rest - mid.astype(F32)).astype(BF16)


def iota(shape, dim):
    return lax.broadcasted_iota(jnp.int32, shape, dim)


def kernel(
    x_hbm, xg_hbm, wq_hbm, wk_hbm, wv_hbm, qg_hbm, kg_hbm, gate_hbm, ag_hbm,
    wrq_hbm, wf_hbm, wrv_hbm, wog_hbm, slack_hbm, extra_hbm, rg_hbm, woa_hbm, wor_hbm,
    own_ref, direct_ref, summed_ref, lse_ref,
    x_v, n_v, xg_v, qg_v, kg_v, ag_v, slack_v, extra_v, rg_v,
    wkv, wfr, wqq, wog, woa, wor, product_v,
    gates, kv, q_v, m_v, acc_v,
    st_row, st_col, in_v, rec_v, visq_v, outgate_v,
    act_r, act_a, peer_r, peer_a, part, xt, xsum,
    entered, lsem, gsem, grecv, ssem, krecv, rsem, rrecv, csem, crecv, psem, precv, xsem, xrecv,
):
    sp = lax.axis_index("sp")
    tp = lax.axis_index("tp")
    z, y = sp // RING, sp % RING
    xc, core = tp // 2, tp % 2
    peer = 2 * xc + 1 - core

    loads = {}

    def load(name, src, dst):
        cp = pltpu.make_async_copy(src, dst, lsem.at[len(loads)])
        cp.start()
        loads[name] = cp

    for r in range(0, ROWS, HALF):
        load(("x", r), x_hbm.at[pl.ds(r, HALF)], x_v.at[pl.ds(r, HALF)])
    load("xg", xg_hbm, xg_v)
    load("wk", wk_hbm, wkv.at[:, pl.ds(0, LANES)])
    load("wv", wv_hbm, wkv.at[:, pl.ds(LANES, LANES)])
    load("kg", kg_hbm, kg_v)
    load("gate", gate_hbm, gates.at[sp])

    barrier = pltpu.get_barrier_semaphore()
    x_right = 2 * ((xc + 1) % RING) + core
    x_left = 2 * ((xc + 3) % RING) + core
    for other in (x_right, x_left, peer):
        pl.semaphore_signal(barrier, inc=1, device_id=(sp, other), device_id_type=MESH)

    def greet(k):
        pl.semaphore_signal(barrier, inc=1, device_id=((sp + k) % SHARDS, tp), device_id_type=MESH)

    def answer(k):
        pl.semaphore_signal(entered.at[sp], inc=1, device_id=((sp + SHARDS - k) % SHARDS, tp), device_id_type=MESH)

    for k in range(1, SHARDS):
        pl.when(sp + k < SHARDS)(functools.partial(greet, k))
    pl.semaphore_wait(barrier, sp + 3)
    for k in (1, 4, 3, 2, 12, 5, 6, 7, 8, 9, 10, 11, 13, 14, 15):
        pl.when(sp >= k)(functools.partial(answer, k))

    def await_entry(pred, k):
        @pl.when(pred)
        def _():
            pl.semaphore_wait(entered.at[(sp + k) % SHARDS], 1)

    pending = []

    def start(pred, cp):
        if pred is None:
            cp.start()
        else:
            pl.when(pred)(cp.start)
        pending.append((pred, cp))

    loads["xg"].wait()
    step = 32
    for r in range(0, ROWS, step):
        if r % HALF == 0:
            loads["x", r].wait()
        if r == HALF:
            load("wf", wf_hbm, wfr.at[:, pl.ds(0, LANES)])
            load("wrv", wrv_hbm, wfr.at[:, pl.ds(LANES, LANES)])
            load("slack", slack_hbm, slack_v)
            load("extra", extra_hbm, extra_v)
            load("wq", wq_hbm, wqq.at[:, pl.ds(0, LANES)])
            load("wrq", wrq_hbm, wqq.at[:, pl.ds(LANES, LANES)])
            load("qg", qg_hbm, qg_v)
            load("wog", wog_hbm, wog)
            load("ag", ag_hbm, ag_v)
            load("rg", rg_hbm, rg_v)
            load("woa", woa_hbm, woa.at[pl.ds(0, LANES)])
            load("wor", wor_hbm, wor.at[pl.ds(0, LANES)])
        xf = x_v[r : r + step, :].astype(F32)
        mean = jnp.sum(xf * xf, axis=-1, keepdims=True) * (1.0 / WIDTH)
        n_v[r : r + step, :] = (xf * lax.rsqrt(mean + EPSILON) * xg_v[...]).astype(BF16)

    lane = iota((ROWS, LANES), 1)
    low = lane < HALF
    same_half = (iota((LANES, LANES), 0) // HALF == iota((LANES, LANES), 1) // HALF)
    halves = jnp.where(same_half, 1.0, 0.0).astype(BF16)

    def twice(gain):
        return jnp.concatenate([gain, gain], axis=1)

    def half_rms(v, gain):
        hi, lo = split2(v * v)
        mean = (dot(hi, halves) + dot(lo, halves)) * (1.0 / HALF)
        return v * lax.rsqrt(mean + EPSILON) * gain

    loads["wk"].wait()
    loads["wv"].wait()
    loads["kg"].wait()
    kv_f = dot(n_v[...], wkv[...])
    keys = half_rms(kv_f[:, :LANES], twice(kg_v[...]))
    swapped = pltpu.roll(kv_f[:, LANES:], HALF, 1)
    kv[0, sp] = jnp.where(low, keys, swapped).astype(BF16)
    kv[1, sp] = jnp.where(low, swapped, keys).astype(BF16)

    loads["gate"].wait()

    y_up = z * RING + (y + 1) % RING
    y_down = z * RING + (y + 3) % RING
    count = [0]

    def send(pred, h, j, target):
        n = count[0]
        count[0] += 1
        start(
            pred,
            pltpu.make_async_remote_copy(
                src_ref=kv.at[h, j], dst_ref=kv.at[h, j], send_sem=ssem.at[n], recv_sem=krecv.at[h, j],
                device_id=(target, tp), device_id_type=MESH,
            ),
        )

    def arrive(pred, h, j):
        cp = pltpu.make_async_remote_copy(
            src_ref=kv.at[h, j], dst_ref=kv.at[h, j], send_sem=ssem.at[0], recv_sem=krecv.at[h, j],
            device_id=(sp, peer), device_id_type=MESH,
        )
        if pred is None:
            cp.wait_recv()
        else:
            pl.when(pred)(cp.wait_recv)

    def send_along_z(h, j):
        send(z < 3, h, j, (sp + RING) % SHARDS)
        send(z == 0, h, j, 3 * RING + y)
        send((z == 1) & (core == 1), h, j, y)

    def send_along_y(pred, h, j):
        send(pred, h, j, y_up)
        send(pred, h, j, y_down)

    def gate_copy(j, target):
        return pltpu.make_async_remote_copy(
            src_ref=gates.at[j], dst_ref=gates.at[j], send_sem=gsem.at[target], recv_sem=grecv.at[j],
            device_id=(target, tp), device_id_type=MESH,
        )

    await_entry(y < 3, 1)
    send(None, 0, sp, y_up)
    send(y > 0, 0, sp, y_down)
    send(None, 1, sp, y_up)
    send(y > 0, 1, sp, y_down)
    await_entry(z < 3, RING)
    for h in (1, 0):
        send(z < 3, h, sp, (sp + RING) % SHARDS)
        send((z == 1) & (core == 1), h, sp, y)

    loads["wf"].wait()
    loads["wrv"].wait()
    loads["slack"].wait()
    loads["extra"].wait()
    fr = dot(n_v[...], wfr[...])
    forget = slack_v[...] * (1.0 / (1.0 + jnp.exp(fr[:, :LANES])))
    rec_value = fr[:, LANES:].astype(BF16)
    extra = jnp.broadcast_to(extra_v[...], (LANES, ROWS)).T
    row_at, col_at = iota((ROWS, ROWS), 0), iota((ROWS, ROWS), 1)
    causal = col_at <= row_at
    lower = jnp.where(causal, 1.0, 0.0).astype(BF16)
    sums = dot(lower, jnp.concatenate(split3(jnp.log1p(-forget)) + split3(extra), axis=1))
    share_sum = sums[:, :LANES] + sums[:, LANES : 2 * LANES] + sums[:, 2 * LANES : 3 * LANES]
    extra_sum = sums[:, 3 * LANES : 4 * LANES] + sums[:, 4 * LANES : 5 * LANES] + sums[:, 5 * LANES :]
    share_end = share_sum[ROWS - 1 :, :]
    extra_end = extra_sum[ROWS - 1 :, :]
    closing = (forget * jnp.exp((share_end - share_sum) + (extra_end - extra_sum))).astype(BF16)
    state_t = dot(fr[:, LANES:].T.astype(BF16), closing)

    def state_message(state, decay):
        hi, mid, lo = (part.astype(F32) for part in split3(decay))
        at = iota((16, LANES), 0)
        tail = jnp.where(at == 0, hi, jnp.where(at == 1, mid, jnp.where(at == 2, lo, 0.0)))
        return state.astype(BF16), tail.astype(BF16)

    body, tail = state_message(state_t, share_end + extra_end)
    st_row[y, :LANES] = body
    st_row[y, LANES:] = tail

    def row_copy(j, target, n):
        return pltpu.make_async_remote_copy(
            src_ref=st_row.at[j], dst_ref=st_row.at[j], send_sem=rsem.at[n], recv_sem=rrecv.at[j],
            device_id=(target, tp), device_id_type=MESH,
        )

    def col_copy(j, target, n):
        return pltpu.make_async_remote_copy(
            src_ref=st_col.at[j], dst_ref=st_col.at[j], send_sem=csem.at[n], recv_sem=crecv.at[j],
            device_id=(target, tp), device_id_type=MESH,
        )

    await_entry(y == 0, 3)
    send(y == 0, 0, sp, y_down)
    send(y == 0, 1, sp, y_down)

    loads["wq"].wait()
    loads["wrq"].wait()
    loads["qg"].wait()
    qq = dot(n_v[...], wqq[...])
    queries = (half_rms(qq[:, :LANES], twice(qg_v[...])).astype(BF16).astype(F32)) * (HALF**-0.5)
    q_v[0] = jnp.where(low, queries, 0.0).astype(BF16)
    q_v[1] = jnp.where(low, 0.0, queries).astype(BF16)

    rq = qq[:, LANES:]
    rec_query = rq / (1.0 + jnp.exp(-rq))
    scores = dot_nt((rec_query * jnp.exp(share_sum)).astype(BF16), (forget * jnp.exp(-share_sum)).astype(BF16))
    differ = jnp.concatenate([extra_sum, extra_sum], axis=1) - extra_sum.T[:1, :]
    scores = scores * jnp.exp(jnp.where(causal, differ, NEGATIVE))
    rec_v[...] = dot(scores.astype(BF16), rec_value)
    visq_v[...] = (rec_query * jnp.exp(share_sum + extra_sum)).astype(BF16)

    loads["wog"].wait()
    og = dot(n_v[...], wog[...])
    outgate_v[...] = og / (1.0 + jnp.exp(-og))

    def attend(blocks, first=False, shown=None):
        for h in range(2):
            parts = []
            for i, j in enumerate(blocks):
                gate = gates[j, h : h + 1, :]
                if shown is not None:
                    gate = jnp.where(shown[i], gate, -NEGATIVE)
                part = dot_nt(q_v[h], kv[h, j]) - gate
                parts.append(jnp.where(causal, part, NEGATIVE) if first else part)
            widest = parts[0]
            for part in parts[1:]:
                widest = jnp.maximum(widest, part)
            top = jnp.max(widest, axis=-1, keepdims=True)
            if not first:
                old = m_v[h]
                top = jnp.maximum(old[:, :1], top)
            summed = None if first else acc_v[h] * jnp.exp(old - top)
            for part, j in zip(parts, blocks):
                weights = jnp.exp(part - top).astype(BF16)
                block = kv[h, j]
                ones = jnp.ones_like(block)
                right = jnp.where(low, ones, block) if h == 0 else jnp.where(low, block, ones)
                term = dot(weights, right)
                summed = term if summed is None else summed + term
            acc_v[h] = summed
            m_v[h] = jnp.broadcast_to(top, (ROWS, LANES))

    attend([sp], first=True)

    await_entry(z == 0, 12)
    send(z == 0, 1, sp, 3 * RING + y)
    send(z == 0, 0, sp, 3 * RING + y)
    await_entry(y <= 1, 2)
    for n in range(1, RING):
        start(None, row_copy(y, z * RING + (y + n) % RING, n))

    def to_peer(n, src, dst):
        return pltpu.make_async_remote_copy(
            src_ref=src, dst_ref=dst, send_sem=psem.at[n], recv_sem=precv.at[n],
            device_id=(sp, peer), device_id_type=MESH,
        )

    loads["woa"].wait()
    loads["wor"].wait()
    wor_copy = to_peer(0, wor.at[pl.ds(0, LANES)], wor.at[pl.ds(LANES, LANES)])
    woa_copy = to_peer(1, woa.at[pl.ds(0, LANES)], woa.at[pl.ds(LANES, LANES)])
    start(None, wor_copy)
    start(None, woa_copy)

    def wait_gate(valid, j):
        pl.when(valid)(gate_copy(j, j).wait_recv)

    hops = {0: 0, 1: 1, 3: 1, 2: 2}
    plan = sorted(
        ((back, up) for back in (0, 1, 3, 2) for up in (0, 1, 3, 2) if (back, up) != (0, 0)),
        key=lambda e: hops[e[0]] + hops[e[1]],
    )

    def shard_of(back, up):
        return ((z + RING - back) % RING) * RING + (y + up) % RING

    def relay_z(valid, h, j, back):
        if back == 1:
            send((z == 1) & (core == 0) | (z == 2) & (core == 0), h, j, (sp + RING) % SHARDS)
        if back == 3:
            send((z == 3) & (core == 1), h, j, 2 * RING + y)

    def handle(h, back, up):
        valid = None if back == 0 else z >= back
        j = shard_of(back, up)
        arrive(valid, h, j)
        if h == 0:
            if back == 0:
                if up == 3:
                    send(core == 0, h, j, y_up)
                if up == 1:
                    send(core == 1, h, j, y_down)
                send_along_z(h, j)
            else:
                relay_z(valid, h, j, back)
        else:
            if up == 0:
                relay_z(valid, h, j, back)
                send_along_y(valid, h, j)
            else:
                fine = core == (0 if up == 3 else 1)
                if up != 2:
                    send(fine if valid is None else fine & valid, h, j, y_up if up == 3 else y_down)
        if back == 1 and (h == 0 or up == 0):
            through = (z == 0) & (core == 1)
            jj = RING + (y + up) % RING
            arrive(through, h, jj)
            send(through, h, jj, 3 * RING + y)

    def attend_own_row():
        blocks = [shard_of(0, up) for up in (1, 2, 3)]
        shown = [y + up >= RING for up in (1, 2, 3)]
        for valid, j in zip(shown, blocks):
            wait_gate(valid, j)

        @pl.when(y > 0)
        def _():
            attend(blocks, shown=shown)

    def attend_row(back, ups):
        @pl.when(z >= back)
        def _():
            blocks = [shard_of(back, up) for up in ups]
            for j in blocks:
                gate_copy(j, j).wait_recv()
            attend(blocks)

    def read_state(ref, j):
        tail = ref[j, LANES:].astype(F32)
        return ref[j, :LANES].astype(F32), tail[0:1] + tail[1:2] + tail[2:3]

    def combine_row():
        for n in range(1, RING):
            row_copy((y + n) % RING, sp, n).wait_recv()
        before, decay = jnp.zeros((LANES, LANES), F32), jnp.zeros((1, LANES), F32)
        mine, mine_decay = before, decay
        for k in range(RING):
            state, log = read_state(st_row, k)
            before = jnp.exp(log) * before + state
            decay = decay + log
            mine = jnp.where(k < y, before, mine)
            mine_decay = jnp.where(k < y, decay, mine_decay)
        in_v[0] = mine
        in_v[1, 0:1] = mine_decay
        body, tail = state_message(before, decay)
        st_col[z, :LANES] = body
        st_col[z, LANES:] = tail
        for n in range(1, RING):
            start(z + n < RING, col_copy(z, ((z + n) % RING) * RING + y, n))

    def combine_col():
        for n in range(1, RING):
            pl.when(z >= n)(col_copy((z + RING - n) % RING, sp, n).wait_recv)
        in_v[2] = jnp.zeros((LANES, LANES), F32)
        for k in range(RING - 1):

            @pl.when(k < z)
            def _():
                state, log = read_state(st_col, k)
                in_v[2] = jnp.exp(log) * in_v[2] + state

        incoming = jnp.exp(in_v[1, 0:1]) * in_v[2] + in_v[0]
        recurrent = rec_v[...] + dot_nt(visq_v[...], incoming.astype(BF16))
        mean = jnp.mean(recurrent * recurrent, axis=-1, keepdims=True)
        return (recurrent * lax.rsqrt(mean + EPSILON) * rg_v[...] * outgate_v[...]).astype(BF16)

    def by_owner(ref, rows):
        for b in range(8):
            ref[b % 2, 32 * (b // 2) : 32 * (b // 2) + 32, :] = rows[32 * b : 32 * b + 32]

    def share_recurrence():
        loads["rg"].wait()
        by_owner(act_r, combine_col())
        start(None, to_peer(2, act_r.at[1 - core], peer_r))

    def project_recurrence():
        wor_copy.wait_recv()
        to_peer(2, act_r.at[1 - core], peer_r).wait_recv()
        both = jnp.concatenate([act_r[core], peer_r[...]], axis=1)
        for c in range(CHUNKS):
            cols = slice(c * CHUNK, (c + 1) * CHUNK)
            product_v[:, cols] = dot(both, wor[:, cols])

    def handle_all(events):
        for h, back, up in events:
            handle(h, back, up)

    def share_gates():
        later = {1: y == 3, 2: y >= 2, 3: y >= 1}
        for k in range(1, SHARDS):
            if k not in (RING, 12):
                await_entry((sp + k < SHARDS) & later.get(k, True), k)
            start(sp + k < SHARDS, gate_copy(sp, (sp + k) % SHARDS))

    handle_all((
        (1, 3, 0), (1, 1, 0), (0, 0, 3), (0, 0, 1), (1, 0, 1), (1, 0, 3), (0, 3, 0), (0, 3, 3), (0, 1, 0),
    ))
    share_gates()
    handle_all((
        (1, 3, 1), (1, 2, 0), (1, 3, 3), (1, 1, 3), (1, 1, 1), (1, 0, 2), (0, 3, 1), (0, 0, 2), (0, 1, 1),
    ))
    attend_own_row()
    handle_all(((0, 2, 0), (1, 2, 3), (0, 1, 3)))
    combine_row()
    handle_all(((0, 3, 2), (1, 2, 1), (1, 3, 2)))
    attend_row(3, (0, 1, 3, 2))
    handle_all(((0, 1, 2), (1, 1, 2), (0, 2, 1)))
    attend_row(1, (0, 1, 3, 2))
    share_recurrence()
    handle_all(((0, 2, 3), (0, 2, 2), (1, 2, 2)))
    attend_row(2, (0, 1, 3, 2))
    a0, a1 = acc_v[0], acc_v[1]
    totals = jnp.where(low, a0, a1)
    loads["ag"].wait()
    attention = pltpu.roll(jnp.where(low, a1, a0), HALF, 1) / totals
    attn_out = half_rms(attention, ag_v[...]).astype(BF16)
    by_owner(act_a, attn_out)
    act_copy = to_peer(3, act_a.at[1 - core], peer_a)
    start(None, act_copy)
    log_sum = (jnp.where(low, m_v[0], m_v[1]) + jnp.log(totals)).T
    lse_ref[0:1, :] = log_sum[0:1, :] + gates[sp, 0:1, :]
    lse_ref[1:2, :] = log_sum[HALF : HALF + 1, :] + gates[sp, 1:2, :]
    project_recurrence()
    woa_copy.wait_recv()
    act_copy.wait_recv()

    far = (xc + 2) % RING
    sides = ((xc + 3) % RING, (xc + 1) % RING)

    def x_copy(kind, c, src, dst, target):
        return pltpu.make_async_remote_copy(
            src_ref=src, dst_ref=dst, send_sem=xsem.at[kind, c], recv_sem=xrecv.at[kind, c],
            device_id=(sp, target), device_id_type=MESH,
        )

    def transit(c):
        return x_copy(0, c, part.at[c, far], xt.at[c], 2 * sides[c % 2] + core)

    def direct(c):
        return x_copy(1, c, part.at[c, sides[1 - c % 2]], direct_ref.at[c], 2 * sides[1 - c % 2] + core)

    def summed(c):
        return x_copy(2, c, xsum.at[c], summed_ref.at[c], 2 * sides[c % 2] + core)

    both = jnp.concatenate([act_a[core], peer_a[...]], axis=1)
    for c in range(CHUNKS):
        cols = slice(c * CHUNK, (c + 1) * CHUNK)
        product = product_v[:, cols] + dot(both, woa[:, cols])
        for b in range(RING):
            part[c, b] = product[32 * b : 32 * b + 32].astype(BF16)
        start(None, transit(c))
    for c in range(CHUNKS):
        start(None, direct(c))
    own_copies = [
        pltpu.make_async_copy(part.at[c, xc], own_ref.at[c], xsem.at[3, c]) for c in range(CHUNKS)
    ]
    for cp in own_copies:
        cp.start()
    for c in range(CHUNKS):
        transit(c).wait_recv()
        xsum[c] = (xt[c].astype(F32) + part[c, sides[c % 2]].astype(F32)).astype(BF16)
        start(None, summed(c))
    for cp in own_copies:
        cp.wait()
    for c in range(CHUNKS):
        direct(c).wait_recv()
        summed(c).wait_recv()
    for pred, cp in pending:
        if pred is None:
            cp.wait_send()
        else:
            pl.when(pred)(cp.wait_send)


def finish(own_ref, direct_ref, summed_ref, lse_in, mixed_ref, lse_ref):
    for c in range(CHUNKS):
        total = own_ref[c].astype(F32) + direct_ref[c].astype(F32) + summed_ref[c].astype(F32)
        mixed_ref[:, c * CHUNK : (c + 1) * CHUNK] = total.astype(BF16)
    lse_ref[...] = lse_in[...]


def body(*args):
    (
        layer_input_rows, input_norm_gain, query_weight, key_weight, value_weight, query_norm_gain,
        key_norm_gain, cumulative_gate, attention_norm_gain, recurrence_query_weight, forget_weight,
        recurrence_value_weight, output_gate_weight, gate_lower_slack, extra_log_decay,
        recurrence_norm_gain, attention_output_weight, recurrence_output_weight,
    ) = args
    operands = (
        layer_input_rows, input_norm_gain[None], query_weight, key_weight, value_weight,
        query_norm_gain[None], key_norm_gain[None], cumulative_gate.T, attention_norm_gain[None],
        recurrence_query_weight, forget_weight, recurrence_value_weight, output_gate_weight,
        gate_lower_slack[None], extra_log_decay.T, recurrence_norm_gain[None],
        attention_output_weight, recurrence_output_weight,
    )
    dma = pltpu.SemaphoreType.DMA
    own, direct, summed, lse = pl.pallas_call(
        kernel,
        name="mixer",
        out_shape=(
            jax.ShapeDtypeStruct((CHUNKS, ROWS // 8, CHUNK), BF16),
            jax.ShapeDtypeStruct((CHUNKS, ROWS // 8, CHUNK), BF16),
            jax.ShapeDtypeStruct((CHUNKS, ROWS // 8, CHUNK), BF16),
            jax.ShapeDtypeStruct((2, ROWS), F32),
        ),
        in_specs=[pl.BlockSpec(memory_space=pltpu.HBM)] * len(operands),
        out_specs=(pl.BlockSpec(memory_space=pltpu.HBM),) * 3 + (pl.BlockSpec(memory_space=pltpu.VMEM),),
        scratch_shapes=[
            pltpu.VMEM((ROWS, WIDTH), BF16),
            pltpu.VMEM((ROWS, WIDTH), BF16),
            pltpu.VMEM((1, WIDTH), F32),
            pltpu.VMEM((1, HALF), F32),
            pltpu.VMEM((1, HALF), F32),
            pltpu.VMEM((1, LANES), F32),
            pltpu.VMEM((1, LANES), F32),
            pltpu.VMEM((1, ROWS), F32),
            pltpu.VMEM((1, LANES), F32),
            pltpu.VMEM((WIDTH, 2 * LANES), BF16),
            pltpu.VMEM((WIDTH, 2 * LANES), BF16),
            pltpu.VMEM((WIDTH, 2 * LANES), BF16),
            pltpu.VMEM((WIDTH, LANES), BF16),
            pltpu.VMEM((2 * LANES, WIDTH), BF16),
            pltpu.VMEM((2 * LANES, WIDTH), BF16),
            pltpu.VMEM((ROWS // 2, WIDTH), F32),
            pltpu.VMEM((SHARDS, 2, ROWS), F32),
            pltpu.VMEM((2, SHARDS, ROWS, LANES), BF16),
            pltpu.VMEM((2, ROWS, LANES), BF16),
            pltpu.VMEM((2, ROWS, LANES), F32),
            pltpu.VMEM((2, ROWS, LANES), F32),
            pltpu.VMEM((RING, STATE_MSG, LANES), BF16),
            pltpu.VMEM((RING, STATE_MSG, LANES), BF16),
            pltpu.VMEM((3, LANES, LANES), F32),
            pltpu.VMEM((ROWS, LANES), F32),
            pltpu.VMEM((ROWS, LANES), BF16),
            pltpu.VMEM((ROWS, LANES), F32),
            pltpu.VMEM((2, ROWS // 2, LANES), BF16),
            pltpu.VMEM((2, ROWS // 2, LANES), BF16),
            pltpu.VMEM((ROWS // 2, LANES), BF16),
            pltpu.VMEM((ROWS // 2, LANES), BF16),
            pltpu.VMEM((CHUNKS, RING, ROWS // 8, CHUNK), BF16),
            pltpu.VMEM((CHUNKS, ROWS // 8, CHUNK), BF16),
            pltpu.VMEM((CHUNKS, ROWS // 8, CHUNK), BF16),
            pltpu.SemaphoreType.REGULAR((SHARDS,)),
            dma((21,)),
            dma((SHARDS,)),
            dma((SHARDS,)),
            dma((KV_SENDS,)),
            dma((2, SHARDS)),
            dma((RING,)),
            dma((RING,)),
            dma((RING,)),
            dma((RING,)),
            dma((4,)),
            dma((4,)),
            dma((4, CHUNKS)),
            dma((3, CHUNKS)),
        ],
        compiler_params=pltpu.CompilerParams(
            collective_id=0, has_side_effects=True, vmem_limit_bytes=60 * 1024 * 1024
        ),
    )(*operands)
    mixed, lse = pl.pallas_call(
        finish,
        name="finish",
        out_shape=(
            jax.ShapeDtypeStruct((ROWS // 8, WIDTH), BF16),
            jax.ShapeDtypeStruct((2, ROWS), F32),
        ),
    )(own, direct, summed, lse)
    return mixed, lse.T


def solution(mesh):
    both = P("sp", "tp")
    placed = (
        P("sp", None), P(), P(None, "tp"), P(None, "tp"), P(None, "tp"), P(), P(), both, P("tp"),
        P(None, "tp"), P(None, "tp"), P(None, "tp"), P(None, "tp"), P("tp"), both, P("tp"),
        P("tp", None), P("tp", None),
    )
    return jax.shard_map(
        body, mesh=mesh, in_specs=placed, out_specs=(P(("sp", "tp"), None), both), check_vma=False
    )
```

```python
import functools

import jax
import jax.numpy as jnp
from jax import lax
from jax.experimental import pallas as pl
from jax.experimental.pallas import tpu as pltpu
from jax.sharding import PartitionSpec as P

F32 = jnp.float32
BF16 = jnp.bfloat16
MESH = pl.DeviceIdType.MESH
EPSILON = 1e-06
ROWS = 256
WIDTH = 2048
LANES = 128
HALF = 64
SHARDS = 16
RING = 4
CHUNKS = 4
CHUNK = WIDTH // CHUNKS
STATE_MSG = 144
KV_SENDS = 80
NEGATIVE = -1e30


def dot(a, b):
    return jnp.dot(a, b, preferred_element_type=F32)


def dot_nt(a, b):
    return lax.dot_general(a, b, (((1,), (1,)), ((), ())), preferred_element_type=F32)


def split2(v):
    hi = v.astype(BF16)
    return hi, (v - hi.astype(F32)).astype(BF16)


def split3(v):
    hi = v.astype(BF16)
    rest = v - hi.astype(F32)
    mid = rest.astype(BF16)
    return hi, mid, (rest - mid.astype(F32)).astype(BF16)


def iota(shape, dim):
    return lax.broadcasted_iota(jnp.int32, shape, dim)


def kernel(
    x_hbm, xg_hbm, wq_hbm, wk_hbm, wv_hbm, qg_hbm, kg_hbm, gate_hbm, ag_hbm,
    wrq_hbm, wf_hbm, wrv_hbm, wog_hbm, slack_hbm, extra_hbm, rg_hbm, woa_hbm, wor_hbm,
    mixed_ref, lse_ref,
    x_v, n_v, xg_v, qg_v, kg_v, ag_v, slack_v, extra_v, rg_v,
    wkv, wfr, wqq, wog, woa, wor, product_v,
    gates, kv, q_v, m_v, acc_v,
    st_row, st_col, in_v, rec_v, visq_v, outgate_v,
    act_r, act_a, peer_r, peer_a, part, xt, near, relayed, xsum,
    entered, lsem, gsem, grecv, ssem, krecv, rsem, rrecv, csem, crecv, psem, precv, xsem, xrecv,
):
    sp = lax.axis_index("sp")
    tp = lax.axis_index("tp")
    z, y = sp // RING, sp % RING
    xc, core = tp // 2, tp % 2
    peer = 2 * xc + 1 - core

    loads = {}

    def load(name, src, dst):
        cp = pltpu.make_async_copy(src, dst, lsem.at[len(loads)])
        cp.start()
        loads[name] = cp

    for r in range(0, ROWS, HALF):
        load(("x", r), x_hbm.at[pl.ds(r, HALF)], x_v.at[pl.ds(r, HALF)])
    load("xg", xg_hbm, xg_v)
    load("wk", wk_hbm, wkv.at[:, pl.ds(0, LANES)])
    load("wv", wv_hbm, wkv.at[:, pl.ds(LANES, LANES)])
    load("kg", kg_hbm, kg_v)
    load("gate", gate_hbm, gates.at[sp])

    barrier = pltpu.get_barrier_semaphore()

    def along_y(k):
        return (z * RING + (y + k) % RING, tp)

    def along_z(k):
        return ((sp + RING * k) % SHARDS, tp)

    def along_x(k):
        return (sp, 2 * ((xc + k) % RING) + core)

    def greet(pred, device):
        @pl.when(pred)
        def _():
            pl.semaphore_signal(barrier, inc=1, device_id=device, device_id_type=MESH)

    def answer(pred, kind, k, device):
        @pl.when(pred)
        def _():
            pl.semaphore_signal(entered.at[kind, k], inc=1, device_id=device, device_id_type=MESH)

    def await_entry(pred, kind, k):
        @pl.when(pred)
        def _():
            pl.semaphore_wait(entered.at[kind, k], 1)

    for k in range(1, RING):
        greet(y + k < RING, along_y(k))
        greet(z + k < RING, along_z(k))
    greet(xc < 3, along_x(1))
    greet(xc == 0, along_x(3))
    greet(core == 0, (sp, peer))
    earlier = y + z + (xc + 3) // 4 + xc // 3 + core

    @pl.when(earlier > 0)
    def _():
        pl.semaphore_wait(barrier, earlier)

    for k in range(1, RING):
        answer(y >= k, 0, k, along_y(RING - k))
        answer(z >= k, 1, k, along_z(RING - k))
    answer(core == 1, 2, 0, (sp, peer))
    answer(xc > 0, 2, 1, along_x(3))
    answer(xc == 3, 2, 3, along_x(1))

    pending = []

    def start(pred, cp):
        if pred is None:
            cp.start()
        else:
            pl.when(pred)(cp.start)
        pending.append((pred, cp))

    loads["xg"].wait()
    step = 32
    for r in range(0, ROWS, step):
        if r % HALF == 0:
            loads["x", r].wait()
        if r == HALF:
            load("wf", wf_hbm, wfr.at[:, pl.ds(0, LANES)])
            load("wrv", wrv_hbm, wfr.at[:, pl.ds(LANES, LANES)])
            load("slack", slack_hbm, slack_v)
            load("extra", extra_hbm, extra_v)
            load("wq", wq_hbm, wqq.at[:, pl.ds(0, LANES)])
            load("wrq", wrq_hbm, wqq.at[:, pl.ds(LANES, LANES)])
            load("qg", qg_hbm, qg_v)
            load("wog", wog_hbm, wog)
            load("ag", ag_hbm, ag_v)
            load("rg", rg_hbm, rg_v)
            load("woa", woa_hbm, woa.at[pl.ds(0, LANES)])
            load("wor", wor_hbm, wor.at[pl.ds(0, LANES)])
        xf = x_v[r : r + step, :].astype(F32)
        mean = jnp.sum(xf * xf, axis=-1, keepdims=True) * (1.0 / WIDTH)
        n_v[r : r + step, :] = (xf * lax.rsqrt(mean + EPSILON) * xg_v[...]).astype(BF16)

    lane = iota((ROWS, LANES), 1)
    low = lane < HALF
    same_half = (iota((LANES, LANES), 0) // HALF == iota((LANES, LANES), 1) // HALF)
    halves = jnp.where(same_half, 1.0, 0.0).astype(BF16)

    def twice(gain):
        return jnp.concatenate([gain, gain], axis=1)

    def half_rms(v, gain):
        hi, lo = split2(v * v)
        mean = (dot(hi, halves) + dot(lo, halves)) * (1.0 / HALF)
        return v * lax.rsqrt(mean + EPSILON) * gain

    loads["wk"].wait()
    loads["wv"].wait()
    loads["kg"].wait()
    kv_f = dot(n_v[...], wkv[...])
    keys = half_rms(kv_f[:, :LANES], twice(kg_v[...]))
    swapped = pltpu.roll(kv_f[:, LANES:], HALF, 1)
    kv[0, sp] = jnp.where(low, keys, swapped).astype(BF16)
    kv[1, sp] = jnp.where(low, swapped, keys).astype(BF16)

    loads["gate"].wait()

    y_up = z * RING + (y + 1) % RING
    y_down = z * RING + (y + 3) % RING
    count = [0]

    def send(pred, h, j, target):
        n = count[0]
        count[0] += 1
        start(
            pred,
            pltpu.make_async_remote_copy(
                src_ref=kv.at[h, j], dst_ref=kv.at[h, j], send_sem=ssem.at[n], recv_sem=krecv.at[h, j],
                device_id=(target, tp), device_id_type=MESH,
            ),
        )

    def arrive(pred, h, j):
        cp = pltpu.make_async_remote_copy(
            src_ref=kv.at[h, j], dst_ref=kv.at[h, j], send_sem=ssem.at[0], recv_sem=krecv.at[h, j],
            device_id=(sp, peer), device_id_type=MESH,
        )
        if pred is None:
            cp.wait_recv()
        else:
            pl.when(pred)(cp.wait_recv)

    def send_along_z(h, j):
        send(z < 3, h, j, (sp + RING) % SHARDS)
        send(z == 0, h, j, 3 * RING + y)
        send((z == 1) & (core == 1), h, j, y)

    def send_along_y(pred, h, j):
        send(pred, h, j, y_up)
        send(pred, h, j, y_down)

    def gate_copy(j, k):
        return pltpu.make_async_remote_copy(
            src_ref=gates.at[j], dst_ref=gates.at[j], send_sem=gsem.at[0, k], recv_sem=grecv.at[0, j % RING],
            device_id=along_y(k), device_id_type=MESH,
        )

    def gate_rows(row, k):
        four = gates.at[pl.ds(row * RING, RING)]
        return pltpu.make_async_remote_copy(
            src_ref=four, dst_ref=four, send_sem=gsem.at[1, k], recv_sem=grecv.at[1, row],
            device_id=along_z(k), device_id_type=MESH,
        )

    row_at, col_at = iota((ROWS, ROWS), 0), iota((ROWS, ROWS), 1)
    causal = col_at <= row_at

    def state_message(state, decay):
        hi, mid, lo = (part.astype(F32) for part in split3(decay))
        at = iota((16, LANES), 0)
        tail = jnp.where(at == 0, hi, jnp.where(at == 1, mid, jnp.where(at == 2, lo, 0.0)))
        return state.astype(BF16), tail.astype(BF16)

    def row_copy(j, target, n):
        return pltpu.make_async_remote_copy(
            src_ref=st_row.at[j], dst_ref=st_row.at[j], send_sem=rsem.at[n], recv_sem=rrecv.at[j],
            device_id=(target, tp), device_id_type=MESH,
        )

    def col_copy(j, target, n):
        return pltpu.make_async_remote_copy(
            src_ref=st_col.at[j], dst_ref=st_col.at[j], send_sem=csem.at[n], recv_sem=crecv.at[j],
            device_id=(target, tp), device_id_type=MESH,
        )

    def first_y():
        await_entry(y < 3, 0, 1)
        send((y < 3) | (z < 3), 0, sp, y_up)
        send((y > 0) & (z < 3), 0, sp, y_down)
        send(y < 3, 1, sp, y_up)
        send((y == 1) & (core == 1), 1, sp, y_down)
        send((y == 1) & (core == 1) & (z == 3), 0, sp, y_down)

    def first_z():
        await_entry(z < 3, 1, 1)
        for h in (1, 0):
            send(z < 3, h, sp, (sp + RING) % SHARDS)
            send((z == 1) & (core == 1), h, sp, y)

    def last_y():
        await_entry(y == 0, 0, 3)
        send(y == 0, 0, sp, y_down)
        send(y == 0, 1, sp, y_down)

    def last_z():
        await_entry(z == 0, 1, 3)
        for h in (1, 0):
            send(z == 0, h, sp, 3 * RING + y)

    def share_row_gates():
        await_entry(y <= 1, 0, 2)
        for k in range(1, RING):
            start(None, gate_copy(sp, k))

    def share_states():
        for n in range(1, RING):
            start(None, row_copy(y, z * RING + (y + n) % RING, n))

    def recurrence():
        loads["wf"].wait()
        loads["wrv"].wait()
        loads["slack"].wait()
        loads["extra"].wait()
        fr = dot(n_v[...], wfr[...])
        forget = slack_v[...] * (1.0 / (1.0 + jnp.exp(fr[:, :LANES])))
        rec_value = fr[:, LANES:].astype(BF16)
        extra = jnp.broadcast_to(extra_v[...], (LANES, ROWS)).T
        lower_tri = jnp.where(causal, 1.0, 0.0).astype(BF16)
        sums = dot(lower_tri, jnp.concatenate(split3(jnp.log1p(-forget)) + split3(extra), axis=1))
        share_sum = sums[:, :LANES] + sums[:, LANES : 2 * LANES] + sums[:, 2 * LANES : 3 * LANES]
        extra_sum = sums[:, 3 * LANES : 4 * LANES] + sums[:, 4 * LANES : 5 * LANES] + sums[:, 5 * LANES :]
        share_end = share_sum[ROWS - 1 :, :]
        extra_end = extra_sum[ROWS - 1 :, :]
        closing = (forget * jnp.exp((share_end - share_sum) + (extra_end - extra_sum))).astype(BF16)
        state_t = dot(fr[:, LANES:].T.astype(BF16), closing)

        body, tail = state_message(state_t, share_end + extra_end)
        st_row[y, :LANES] = body
        st_row[y, LANES:] = tail
        return forget, rec_value, share_sum, extra_sum

    def query_side(forget, rec_value, share_sum, extra_sum):
        loads["wq"].wait()
        loads["wrq"].wait()
        loads["qg"].wait()
        qq = dot(n_v[...], wqq[...])
        queries = (half_rms(qq[:, :LANES], twice(qg_v[...])).astype(BF16).astype(F32)) * (HALF**-0.5)
        q_v[0] = jnp.where(low, queries, 0.0).astype(BF16)
        q_v[1] = jnp.where(low, 0.0, queries).astype(BF16)

        rq = qq[:, LANES:]
        rec_query = rq / (1.0 + jnp.exp(-rq))
        scores = dot_nt((rec_query * jnp.exp(share_sum)).astype(BF16), (forget * jnp.exp(-share_sum)).astype(BF16))
        differ = jnp.concatenate([extra_sum, extra_sum], axis=1) - extra_sum.T[:1, :]
        scores = scores * jnp.exp(jnp.where(causal, differ, NEGATIVE))
        rec_v[...] = dot(scores.astype(BF16), rec_value)
        visq_v[...] = (rec_query * jnp.exp(share_sum + extra_sum)).astype(BF16)

        loads["wog"].wait()
        og = dot(n_v[...], wog[...])
        outgate_v[...] = og / (1.0 + jnp.exp(-og))

    def attend(blocks, first=False, shown=None):
        def keys_of(h, i, j):
            block = kv[h, j]
            return block if shown is None or shown[i] is None else jnp.where(shown[i], block, jnp.zeros_like(block))

        for h in range(2):
            parts = []
            for i, j in enumerate(blocks):
                gate = gates[j, h : h + 1, :]
                if shown is not None and shown[i] is not None:
                    gate = jnp.where(shown[i], gate, -NEGATIVE)
                part = dot_nt(q_v[h], keys_of(h, i, j)) - gate
                parts.append(jnp.where(causal, part, NEGATIVE) if first else part)
            widest = parts[0]
            for part in parts[1:]:
                widest = jnp.maximum(widest, part)
            top = jnp.max(widest, axis=-1, keepdims=True)
            if not first:
                old = m_v[h]
                top = jnp.maximum(old[:, :1], top)
            summed = None if first else acc_v[h] * jnp.exp(old - top)
            for i, (part, j) in enumerate(zip(parts, blocks)):
                weights = jnp.exp(part - top).astype(BF16)
                block = keys_of(h, i, j)
                ones = jnp.ones_like(block)
                right = jnp.where(low, ones, block) if h == 0 else jnp.where(low, block, ones)
                term = dot(weights, right)
                summed = term if summed is None else summed + term
            acc_v[h] = summed
            m_v[h] = jnp.broadcast_to(top, (ROWS, LANES))

    def to_peer(n, src, dst):
        return pltpu.make_async_remote_copy(
            src_ref=src, dst_ref=dst, send_sem=psem.at[n], recv_sem=precv.at[n],
            device_id=(sp, peer), device_id_type=MESH,
        )

    wor_copy = to_peer(0, wor.at[pl.ds(0, LANES)], wor.at[pl.ds(LANES, LANES)])
    woa_copy = to_peer(1, woa.at[pl.ds(0, LANES)], woa.at[pl.ds(LANES, LANES)])
    def share_weights():
        loads["woa"].wait()
        loads["wor"].wait()
        await_entry(core == 0, 2, 0)
        start(None, wor_copy)
        start(None, woa_copy)

    def shard_of(back, up):
        return ((z + RING - back) % RING) * RING + (y + up) % RING

    def relay_z(valid, h, j, back):
        if back == 1:
            send((z == 1) & (core == 0) | (z == 2) & (core == 0), h, j, (sp + RING) % SHARDS)
        if back == 3:
            send((z == 3) & (core == 1), h, j, 2 * RING + y)

    def handle(h, back, up):
        j = shard_of(back, up)
        if back == 0:
            wanted = y + up >= RING
            if up == 1:
                wanted = wanted | (y == 0) & (core == 1)
            arrive(wanted if h else wanted | (z < 3), h, j)
            if up == 3:
                onward = (core == 0) & ((y == 1) | (y == 2))
                send(onward if h else onward | (core == 0) & (z < 3), h, j, y_up)
            if up == 1:
                onward = (core == 1) & ((y == 3) | (y == 0))
                send(onward if h else onward | (core == 1) & (z < 3), h, j, y_down)
            if h == 0:
                send_along_z(h, j)
            return
        valid = z >= back
        arrive(valid, h, j)
        if h == 0:
            relay_z(valid, h, j, back)
        elif up == 0:
            relay_z(valid, h, j, back)
            send_along_y(valid, h, j)
        elif up == 3:
            send((core == 0) & valid, h, j, y_up)
        elif up == 1:
            send((core == 1) & valid, h, j, y_down)
        if back == 1 and (h == 0 or up == 0):
            through = (z == 0) & (core == 1)
            jj = RING + (y + up) % RING
            arrive(through, h, jj)
            send(through, h, jj, 3 * RING + y)

    def attend_rows(backs):
        for at in range(RING):
            rows = [b for b in backs if b <= at]

            @pl.when((z == at) & (y > 0) if rows == [0] else z == at)
            def _():
                blocks, shown = [], []
                for b in rows:
                    for up in (1, 2, 3) if b == 0 else (0, 1, 3, 2):
                        blocks.append(shard_of(b, up))
                        shown.append(y + up >= RING if b == 0 else None)
                    if b > 0:
                        gate_rows((z + RING - b) % RING, b).wait_recv()
                if blocks:
                    attend(blocks, shown=shown)

    def read_state(ref, j):
        tail = ref[j, LANES:].astype(F32)
        return ref[j, :LANES].astype(F32), tail[0:1] + tail[1:2] + tail[2:3]

    def combine_row():
        for n in range(1, RING):
            row_copy((y + n) % RING, sp, n).wait_recv()
        before, decay = jnp.zeros((LANES, LANES), F32), jnp.zeros((1, LANES), F32)
        mine, mine_decay = before, decay
        for k in range(RING):
            state, log = read_state(st_row, k)
            before = jnp.exp(log) * before + state
            decay = decay + log
            mine = jnp.where(k < y, before, mine)
            mine_decay = jnp.where(k < y, decay, mine_decay)
        in_v[0] = mine
        in_v[1, 0:1] = mine_decay
        body, tail = state_message(before, decay)
        st_col[z, :LANES] = body
        st_col[z, LANES:] = tail
        for n in range(1, RING):
            start(z + n < RING, col_copy(z, ((z + n) % RING) * RING + y, n))

    def combine_col():
        for n in range(1, RING):
            pl.when(z >= n)(col_copy((z + RING - n) % RING, sp, n).wait_recv)
        in_v[2] = jnp.zeros((LANES, LANES), F32)
        for k in range(RING - 1):

            @pl.when(k < z)
            def _():
                state, log = read_state(st_col, k)
                in_v[2] = jnp.exp(log) * in_v[2] + state

        incoming = jnp.exp(in_v[1, 0:1]) * in_v[2] + in_v[0]
        recurrent = rec_v[...] + dot_nt(visq_v[...], incoming.astype(BF16))
        mean = jnp.mean(recurrent * recurrent, axis=-1, keepdims=True)
        return (recurrent * lax.rsqrt(mean + EPSILON) * rg_v[...] * outgate_v[...]).astype(BF16)

    def by_owner(ref, rows):
        for b in range(8):
            ref[b % 2, 32 * (b // 2) : 32 * (b // 2) + 32, :] = rows[32 * b : 32 * b + 32]

    def share_recurrence():
        loads["rg"].wait()
        by_owner(act_r, combine_col())
        start(None, to_peer(2, act_r.at[1 - core], peer_r))

    def project_recurrence():
        wor_copy.wait_recv()
        to_peer(2, act_r.at[1 - core], peer_r).wait_recv()
        both = jnp.concatenate([act_r[core], peer_r[...]], axis=1)
        for c in range(CHUNKS):
            cols = slice(c * CHUNK, (c + 1) * CHUNK)
            product_v[:, cols] = dot(both, wor[:, cols])

    def handle_all(events):
        for h, back, up in events:
            handle(h, back, up)

    def share_gates():
        await_entry(z <= 1, 1, 2)
        for k in range(1, RING):
            gate_copy(z * RING + (y + k) % RING, k).wait_recv()
        for k in range(1, RING):
            start(z + k < RING, gate_rows(z, k))

    first_y()
    last_y()
    share_row_gates()
    first_z()
    local = recurrence()
    share_states()
    last_z()
    handle_all((
        (1, 3, 0), (1, 1, 0), (0, 0, 3), (0, 0, 1),
    ))
    query_side(*local)
    handle_all((
        (0, 3, 0), (1, 2, 0), (1, 0, 1), (0, 1, 0),
    ))
    share_weights()
    handle_all((
        (0, 3, 3), (1, 3, 3),
    ))
    attend([sp], first=True)
    handle_all((
        (0, 1, 3),
    ))
    share_gates()
    handle_all((
        (0, 3, 1), (1, 0, 3), (1, 1, 3), (0, 0, 2),
    ))
    combine_row()
    handle_all((
        (1, 3, 1), (1, 1, 1), (0, 2, 0), (1, 2, 3), (1, 2, 1), (0, 1, 2), (1, 0, 2),
    ))
    attend_rows((0,))
    handle_all((
        (0, 1, 1), (0, 3, 2), (1, 3, 2),
    ))
    attend_rows((3,))
    handle_all((
        (1, 1, 2),
    ))
    attend_rows((1,))
    share_recurrence()
    handle_all((
        (1, 2, 2), (0, 2, 3), (0, 2, 1), (0, 2, 2),
    ))
    attend_rows((2,))

    a0, a1 = acc_v[0], acc_v[1]
    totals = jnp.where(low, a0, a1)
    loads["ag"].wait()
    attention = pltpu.roll(jnp.where(low, a1, a0), HALF, 1) / totals
    attn_out = half_rms(attention, ag_v[...]).astype(BF16)
    by_owner(act_a, attn_out)
    act_copy = to_peer(3, act_a.at[1 - core], peer_a)
    start(None, act_copy)
    log_sum = (jnp.where(low, m_v[0], m_v[1]) + jnp.log(totals)).T
    lse_ref[0:1, :] = log_sum[0:1, :] + gates[sp, 0:1, :]
    lse_ref[1:2, :] = log_sum[HALF : HALF + 1, :] + gates[sp, 1:2, :]
    await_entry(xc < 3, 2, 1)
    await_entry(xc == 0, 2, 3)
    project_recurrence()
    woa_copy.wait_recv()
    act_copy.wait_recv()

    far = (xc + 2) % RING
    sides = ((xc + 3) % RING, (xc + 1) % RING)

    def x_copy(kind, c, src, dst, target):
        return pltpu.make_async_remote_copy(
            src_ref=src, dst_ref=dst, send_sem=xsem.at[kind, c], recv_sem=xrecv.at[kind, c],
            device_id=(sp, target), device_id_type=MESH,
        )

    def transit(c):
        return x_copy(0, c, part.at[c, far], xt.at[c], 2 * sides[c % 2] + core)

    def direct(c):
        return x_copy(1, c, part.at[c, sides[1 - c % 2]], near.at[c], 2 * sides[1 - c % 2] + core)

    def summed(c):
        return x_copy(2, c, xsum.at[c], relayed.at[c], 2 * sides[c % 2] + core)

    both = jnp.concatenate([act_a[core], peer_a[...]], axis=1)
    for c in range(CHUNKS):
        cols = slice(c * CHUNK, (c + 1) * CHUNK)
        product = product_v[:, cols] + dot(both, woa[:, cols])
        for b in range(RING):
            part[c, b] = product[32 * b : 32 * b + 32].astype(BF16)
        start(None, transit(c))
    for c in range(CHUNKS):
        start(None, direct(c))
    for c in range(CHUNKS):
        transit(c).wait_recv()
        xsum[c] = (xt[c].astype(F32) + part[c, sides[c % 2]].astype(F32)).astype(BF16)
        start(None, summed(c))
    for c in range(CHUNKS):
        direct(c).wait_recv()
        summed(c).wait_recv()
        total = part[c, xc].astype(F32) + near[c].astype(F32) + relayed[c].astype(F32)
        mixed_ref[:, c * CHUNK : (c + 1) * CHUNK] = total.astype(BF16)
    for pred, cp in pending:
        if pred is None:
            cp.wait_send()
        else:
            pl.when(pred)(cp.wait_send)


def finish(mixed_v, lse_v, mixed_hbm, lse_hbm, sem):
    copies = [
        pltpu.make_async_copy(mixed_v, mixed_hbm, sem.at[0]),
        pltpu.make_async_copy(lse_v, lse_hbm, sem.at[1]),
    ]
    for cp in copies:
        cp.start()
    for cp in copies:
        cp.wait()


def body(*args):
    (
        layer_input_rows, input_norm_gain, query_weight, key_weight, value_weight, query_norm_gain,
        key_norm_gain, cumulative_gate, attention_norm_gain, recurrence_query_weight, forget_weight,
        recurrence_value_weight, output_gate_weight, gate_lower_slack, extra_log_decay,
        recurrence_norm_gain, attention_output_weight, recurrence_output_weight,
    ) = args
    operands = (
        layer_input_rows, input_norm_gain[None], query_weight, key_weight, value_weight,
        query_norm_gain[None], key_norm_gain[None], cumulative_gate.T, attention_norm_gain[None],
        recurrence_query_weight, forget_weight, recurrence_value_weight, output_gate_weight,
        gate_lower_slack[None], extra_log_decay.T, recurrence_norm_gain[None],
        attention_output_weight, recurrence_output_weight,
    )
    operands = [pltpu.with_memory_space_constraint(a, pltpu.HBM) for a in operands]
    dma = pltpu.SemaphoreType.DMA
    mixed, lse = pl.pallas_call(
        kernel,
        name="mixer",
        out_shape=(
            pltpu.VMEM((ROWS // 8, WIDTH), BF16),
            pltpu.VMEM((2, ROWS), F32),
        ),
        in_specs=[pl.BlockSpec(memory_space=pltpu.HBM)] * len(operands),
        out_specs=(pl.BlockSpec(memory_space=pltpu.VMEM),) * 2,
        scratch_shapes=[
            pltpu.VMEM((ROWS, WIDTH), BF16),
            pltpu.VMEM((ROWS, WIDTH), BF16),
            pltpu.VMEM((1, WIDTH), F32),
            pltpu.VMEM((1, HALF), F32),
            pltpu.VMEM((1, HALF), F32),
            pltpu.VMEM((1, LANES), F32),
            pltpu.VMEM((1, LANES), F32),
            pltpu.VMEM((1, ROWS), F32),
            pltpu.VMEM((1, LANES), F32),
            pltpu.VMEM((WIDTH, 2 * LANES), BF16),
            pltpu.VMEM((WIDTH, 2 * LANES), BF16),
            pltpu.VMEM((WIDTH, 2 * LANES), BF16),
            pltpu.VMEM((WIDTH, LANES), BF16),
            pltpu.VMEM((2 * LANES, WIDTH), BF16),
            pltpu.VMEM((2 * LANES, WIDTH), BF16),
            pltpu.VMEM((ROWS // 2, WIDTH), F32),
            pltpu.VMEM((SHARDS, 2, ROWS), F32),
            pltpu.VMEM((2, SHARDS, ROWS, LANES), BF16),
            pltpu.VMEM((2, ROWS, LANES), BF16),
            pltpu.VMEM((2, ROWS, LANES), F32),
            pltpu.VMEM((2, ROWS, LANES), F32),
            pltpu.VMEM((RING, STATE_MSG, LANES), BF16),
            pltpu.VMEM((RING, STATE_MSG, LANES), BF16),
            pltpu.VMEM((3, LANES, LANES), F32),
            pltpu.VMEM((ROWS, LANES), F32),
            pltpu.VMEM((ROWS, LANES), BF16),
            pltpu.VMEM((ROWS, LANES), F32),
            pltpu.VMEM((2, ROWS // 2, LANES), BF16),
            pltpu.VMEM((2, ROWS // 2, LANES), BF16),
            pltpu.VMEM((ROWS // 2, LANES), BF16),
            pltpu.VMEM((ROWS // 2, LANES), BF16),
            pltpu.VMEM((CHUNKS, RING, ROWS // 8, CHUNK), BF16),
            pltpu.VMEM((CHUNKS, ROWS // 8, CHUNK), BF16),
            pltpu.VMEM((CHUNKS, ROWS // 8, CHUNK), BF16),
            pltpu.VMEM((CHUNKS, ROWS // 8, CHUNK), BF16),
            pltpu.VMEM((CHUNKS, ROWS // 8, CHUNK), BF16),
            pltpu.SemaphoreType.REGULAR((3, RING)),
            dma((21,)),
            dma((2, RING)),
            dma((2, RING)),
            dma((KV_SENDS,)),
            dma((2, SHARDS)),
            dma((RING,)),
            dma((RING,)),
            dma((RING,)),
            dma((RING,)),
            dma((4,)),
            dma((4,)),
            dma((3, CHUNKS)),
            dma((3, CHUNKS)),
        ],
        compiler_params=pltpu.CompilerParams(
            collective_id=0, has_side_effects=True, vmem_limit_bytes=40 * 1024 * 1024
        ),
    )(*operands)
    mixed, lse = pl.pallas_call(
        finish,
        name="finish",
        out_shape=(
            jax.ShapeDtypeStruct((ROWS // 8, WIDTH), BF16),
            jax.ShapeDtypeStruct((2, ROWS), F32),
        ),
        in_specs=[pl.BlockSpec(memory_space=pltpu.VMEM)] * 2,
        out_specs=(pl.BlockSpec(memory_space=pltpu.HBM),) * 2,
        scratch_shapes=[pltpu.SemaphoreType.DMA((2,))],
    )(pltpu.with_memory_space_constraint(mixed, pltpu.VMEM), pltpu.with_memory_space_constraint(lse, pltpu.VMEM))
    return mixed, lse.T


def solution(mesh):
    both = P("sp", "tp")
    placed = (
        P("sp", None), P(), P(None, "tp"), P(None, "tp"), P(None, "tp"), P(), P(), both, P("tp"),
        P(None, "tp"), P(None, "tp"), P(None, "tp"), P(None, "tp"), P("tp"), both, P("tp"),
        P("tp", None), P("tp", None),
    )
    return jax.shard_map(
        body, mesh=mesh, in_specs=placed, out_specs=(P(("sp", "tp"), None), both), check_vma=False
    )
```

```python
import functools

import jax
import jax.numpy as jnp
from jax import lax
from jax.experimental import pallas as pl
from jax.experimental.pallas import tpu as pltpu
from jax.sharding import PartitionSpec as P

F32 = jnp.float32
BF16 = jnp.bfloat16
MESH = pl.DeviceIdType.MESH
EPSILON = 1e-06
ROWS = 256
WIDTH = 2048
LANES = 128
HALF = 64
SHARDS = 16
RING = 4
CHUNKS = 4
CHUNK = WIDTH // CHUNKS
STATE_MSG = 144
KV_SENDS = 80
NEGATIVE = -1e30


def dot(a, b):
    return jnp.dot(a, b, preferred_element_type=F32)


def dot_nt(a, b):
    return lax.dot_general(a, b, (((1,), (1,)), ((), ())), preferred_element_type=F32)


def split2(v):
    hi = v.astype(BF16)
    return hi, (v - hi.astype(F32)).astype(BF16)


def split3(v):
    hi = v.astype(BF16)
    rest = v - hi.astype(F32)
    mid = rest.astype(BF16)
    return hi, mid, (rest - mid.astype(F32)).astype(BF16)


def iota(shape, dim):
    return lax.broadcasted_iota(jnp.int32, shape, dim)


def kernel(
    x_hbm, xg_hbm, wq_hbm, wk_hbm, wv_hbm, qg_hbm, kg_hbm, gate_hbm, ag_hbm,
    wrq_hbm, wf_hbm, wrv_hbm, wog_hbm, slack_hbm, extra_hbm, rg_hbm, woa_hbm, wor_hbm,
    mixed_ref, lse_ref,
    x_v, n_v, xg_v, qg_v, kg_v, ag_v, slack_v, extra_v, rg_v,
    wkv, wfr, wqq, wog, woa, wor, product_v,
    gates, kv, q_v, m_v, acc_v,
    st_row, st_col, in_v, rec_v, visq_v, outgate_v,
    act_r, act_a, peer_r, peer_a, part, xt, near, relayed, xsum,
    entered, lsem, gsem, grecv, ssem, krecv, rsem, rrecv, csem, crecv, psem, precv, xsem, xrecv,
):
    sp = lax.axis_index("sp")
    tp = lax.axis_index("tp")
    z, y = sp // RING, sp % RING
    xc, core = tp // 2, tp % 2
    peer = 2 * xc + 1 - core

    loads = {}

    def load(name, src, dst):
        cp = pltpu.make_async_copy(src, dst, lsem.at[len(loads)])
        cp.start()
        loads[name] = cp

    for r in range(0, ROWS, HALF):
        load(("x", r), x_hbm.at[pl.ds(r, HALF)], x_v.at[pl.ds(r, HALF)])
    load("xg", xg_hbm, xg_v)
    load("wk", wk_hbm, wkv.at[:, pl.ds(0, LANES)])
    load("wv", wv_hbm, wkv.at[:, pl.ds(LANES, LANES)])
    load("kg", kg_hbm, kg_v)
    load("gate", gate_hbm, gates.at[sp])

    barrier = pltpu.get_barrier_semaphore()

    def along_y(k):
        return (z * RING + (y + k) % RING, tp)

    def along_z(k):
        return ((sp + RING * k) % SHARDS, tp)

    def along_x(k):
        return (sp, 2 * ((xc + k) % RING) + core)

    def greet(pred, device):
        @pl.when(pred)
        def _():
            pl.semaphore_signal(barrier, inc=1, device_id=device, device_id_type=MESH)

    def answer(pred, kind, k, device):
        @pl.when(pred)
        def _():
            pl.semaphore_signal(entered.at[kind, k], inc=1, device_id=device, device_id_type=MESH)

    def await_entry(pred, kind, k):
        @pl.when(pred)
        def _():
            pl.semaphore_wait(entered.at[kind, k], 1)

    for k in range(1, RING):
        greet(y + k < RING, along_y(k))
        greet(z + k < RING, along_z(k))
    greet(xc < 3, along_x(1))
    greet(xc == 0, along_x(3))
    greet(core == 0, (sp, peer))
    earlier = y + z + (xc + 3) // 4 + xc // 3 + core

    @pl.when(earlier > 0)
    def _():
        pl.semaphore_wait(barrier, earlier)

    for k in range(1, RING):
        answer(y >= k, 0, k, along_y(RING - k))
        answer(z >= k, 1, k, along_z(RING - k))
    answer(core == 1, 2, 0, (sp, peer))
    answer(xc > 0, 2, 1, along_x(3))
    answer(xc == 3, 2, 3, along_x(1))

    pending = []

    def start(pred, cp):
        if pred is None:
            cp.start()
        else:
            pl.when(pred)(cp.start)
        pending.append((pred, cp))

    loads["xg"].wait()
    step = 32
    for r in range(0, ROWS, step):
        if r % HALF == 0:
            loads["x", r].wait()
        if r == HALF:
            load("wf", wf_hbm, wfr.at[:, pl.ds(0, LANES)])
            load("wrv", wrv_hbm, wfr.at[:, pl.ds(LANES, LANES)])
            load("slack", slack_hbm, slack_v)
            load("extra", extra_hbm, extra_v)
            load("wq", wq_hbm, wqq.at[:, pl.ds(0, LANES)])
            load("wrq", wrq_hbm, wqq.at[:, pl.ds(LANES, LANES)])
            load("qg", qg_hbm, qg_v)
            load("wog", wog_hbm, wog)
            load("ag", ag_hbm, ag_v)
            load("rg", rg_hbm, rg_v)
            load("woa", woa_hbm, woa.at[pl.ds(0, LANES)])
            load("wor", wor_hbm, wor.at[pl.ds(0, LANES)])
        xf = x_v[r : r + step, :].astype(F32)
        mean = jnp.sum(xf * xf, axis=-1, keepdims=True) * (1.0 / WIDTH)
        n_v[r : r + step, :] = (xf * lax.rsqrt(mean + EPSILON) * xg_v[...]).astype(BF16)

    lane = iota((ROWS, LANES), 1)
    low = lane < HALF
    same_half = (iota((LANES, LANES), 0) // HALF == iota((LANES, LANES), 1) // HALF)
    halves = jnp.where(same_half, 1.0, 0.0).astype(BF16)

    def twice(gain):
        return jnp.concatenate([gain, gain], axis=1)

    def half_rms(v, gain):
        hi, lo = split2(v * v)
        mean = (dot(hi, halves) + dot(lo, halves)) * (1.0 / HALF)
        return v * lax.rsqrt(mean + EPSILON) * gain

    loads["wk"].wait()
    loads["wv"].wait()
    loads["kg"].wait()
    kv_f = dot(n_v[...], wkv[...])
    keys = half_rms(kv_f[:, :LANES], twice(kg_v[...]))
    swapped = pltpu.roll(kv_f[:, LANES:], HALF, 1)
    kv[0, sp] = jnp.where(low, keys, swapped).astype(BF16)
    kv[1, sp] = jnp.where(low, swapped, keys).astype(BF16)

    loads["gate"].wait()

    y_up = z * RING + (y + 1) % RING
    y_down = z * RING + (y + 3) % RING
    count = [0]

    def send(pred, h, j, target):
        n = count[0]
        count[0] += 1
        start(
            pred,
            pltpu.make_async_remote_copy(
                src_ref=kv.at[h, j], dst_ref=kv.at[h, j], send_sem=ssem.at[n], recv_sem=krecv.at[h, j],
                device_id=(target, tp), device_id_type=MESH,
            ),
        )

    def arrive(pred, h, j):
        cp = pltpu.make_async_remote_copy(
            src_ref=kv.at[h, j], dst_ref=kv.at[h, j], send_sem=ssem.at[0], recv_sem=krecv.at[h, j],
            device_id=(sp, peer), device_id_type=MESH,
        )
        if pred is None:
            cp.wait_recv()
        else:
            pl.when(pred)(cp.wait_recv)

    def send_along_z(h, j):
        send(z < 3, h, j, (sp + RING) % SHARDS)
        send(z == 0, h, j, 3 * RING + y)
        send((z == 1) & (core == 1), h, j, y)

    def send_along_y(pred, h, j):
        send(pred, h, j, y_up)
        send(pred, h, j, y_down)

    def gate_copy(j, k):
        return pltpu.make_async_remote_copy(
            src_ref=gates.at[j], dst_ref=gates.at[j], send_sem=gsem.at[0, k], recv_sem=grecv.at[0, j % RING],
            device_id=along_y(k), device_id_type=MESH,
        )

    def gate_rows(row, k):
        four = gates.at[pl.ds(row * RING, RING)]
        return pltpu.make_async_remote_copy(
            src_ref=four, dst_ref=four, send_sem=gsem.at[1, k], recv_sem=grecv.at[1, row],
            device_id=along_z(k), device_id_type=MESH,
        )

    row_at, col_at = iota((ROWS, ROWS), 0), iota((ROWS, ROWS), 1)
    causal = col_at <= row_at

    def state_message(state, decay):
        hi, mid, lo = (part.astype(F32) for part in split3(decay))
        at = iota((16, LANES), 0)
        tail = jnp.where(at == 0, hi, jnp.where(at == 1, mid, jnp.where(at == 2, lo, 0.0)))
        return state.astype(BF16), tail.astype(BF16)

    def row_copy(j, target, n):
        return pltpu.make_async_remote_copy(
            src_ref=st_row.at[j], dst_ref=st_row.at[j], send_sem=rsem.at[n], recv_sem=rrecv.at[j],
            device_id=(target, tp), device_id_type=MESH,
        )

    def col_copy(j, target, n):
        return pltpu.make_async_remote_copy(
            src_ref=st_col.at[j], dst_ref=st_col.at[j], send_sem=csem.at[n], recv_sem=crecv.at[j],
            device_id=(target, tp), device_id_type=MESH,
        )

    def first_y():
        await_entry(y < 3, 0, 1)
        send((y < 3) | (z < 3), 0, sp, y_up)
        send((y > 0) & (z < 3), 0, sp, y_down)
        send(y < 3, 1, sp, y_up)
        send((y == 1) & (core == 1), 1, sp, y_down)
        send((y == 1) & (core == 1) & (z == 3), 0, sp, y_down)

    def first_z():
        await_entry(z < 3, 1, 1)
        for h in (1, 0):
            send(z < 3, h, sp, (sp + RING) % SHARDS)
            send((z == 1) & (core == 1), h, sp, y)

    def last_y():
        await_entry(y == 0, 0, 3)
        send(y == 0, 0, sp, y_down)
        send(y == 0, 1, sp, y_down)

    def last_z():
        await_entry(z == 0, 1, 3)
        for h in (1, 0):
            send(z == 0, h, sp, 3 * RING + y)

    def share_row_gates():
        await_entry(y <= 1, 0, 2)
        for k in range(1, RING):
            start(None, gate_copy(sp, k))

    def share_states():
        for n in range(1, RING):
            start(None, row_copy(y, z * RING + (y + n) % RING, n))

    def recurrence():
        loads["wf"].wait()
        loads["wrv"].wait()
        loads["slack"].wait()
        loads["extra"].wait()
        fr = dot(n_v[...], wfr[...])
        forget = slack_v[...] * (1.0 / (1.0 + jnp.exp(fr[:, :LANES])))
        rec_value = fr[:, LANES:].astype(BF16)
        extra = jnp.broadcast_to(extra_v[...], (LANES, ROWS)).T
        lower_tri = jnp.where(causal, 1.0, 0.0).astype(BF16)
        sums = dot(lower_tri, jnp.concatenate(split3(jnp.log1p(-forget)) + split3(extra), axis=1))
        share_sum = sums[:, :LANES] + sums[:, LANES : 2 * LANES] + sums[:, 2 * LANES : 3 * LANES]
        extra_sum = sums[:, 3 * LANES : 4 * LANES] + sums[:, 4 * LANES : 5 * LANES] + sums[:, 5 * LANES :]
        share_end = share_sum[ROWS - 1 :, :]
        extra_end = extra_sum[ROWS - 1 :, :]
        closing = (forget * jnp.exp((share_end - share_sum) + (extra_end - extra_sum))).astype(BF16)
        state_t = dot(fr[:, LANES:].T.astype(BF16), closing)

        body, tail = state_message(state_t, share_end + extra_end)
        st_row[y, :LANES] = body
        st_row[y, LANES:] = tail
        return forget, rec_value, share_sum, extra_sum

    def query_side(forget, rec_value, share_sum, extra_sum):
        loads["wq"].wait()
        loads["wrq"].wait()
        loads["qg"].wait()
        qq = dot(n_v[...], wqq[...])
        queries = (half_rms(qq[:, :LANES], twice(qg_v[...])).astype(BF16).astype(F32)) * (HALF**-0.5)
        q_v[0] = jnp.where(low, queries, 0.0).astype(BF16)
        q_v[1] = jnp.where(low, 0.0, queries).astype(BF16)

        rq = qq[:, LANES:]
        rec_query = rq / (1.0 + jnp.exp(-rq))
        scores = dot_nt((rec_query * jnp.exp(share_sum)).astype(BF16), (forget * jnp.exp(-share_sum)).astype(BF16))
        differ = jnp.concatenate([extra_sum, extra_sum], axis=1) - extra_sum.T[:1, :]
        scores = scores * jnp.exp(jnp.where(causal, differ, NEGATIVE))
        rec_v[...] = dot(scores.astype(BF16), rec_value)
        visq_v[...] = (rec_query * jnp.exp(share_sum + extra_sum)).astype(BF16)

        loads["wog"].wait()
        og = dot(n_v[...], wog[...])
        outgate_v[...] = og / (1.0 + jnp.exp(-og))

    def attend(blocks, first=False, shown=None):
        def keys_of(h, i, j):
            block = kv[h, j]
            return block if shown is None or shown[i] is None else jnp.where(shown[i], block, jnp.zeros_like(block))

        for h in range(2):
            parts = []
            for i, j in enumerate(blocks):
                gate = gates[j, h : h + 1, :]
                if shown is not None and shown[i] is not None:
                    gate = jnp.where(shown[i], gate, -NEGATIVE)
                part = dot_nt(q_v[h], keys_of(h, i, j)) - gate
                parts.append(jnp.where(causal, part, NEGATIVE) if first else part)
            widest = parts[0]
            for part in parts[1:]:
                widest = jnp.maximum(widest, part)
            top = jnp.max(widest, axis=-1, keepdims=True)
            if not first:
                old = m_v[h]
                top = jnp.maximum(old[:, :1], top)
            summed = None if first else acc_v[h] * jnp.exp(old - top)
            for i, (part, j) in enumerate(zip(parts, blocks)):
                weights = jnp.exp(part - top).astype(BF16)
                block = keys_of(h, i, j)
                ones = jnp.ones_like(block)
                right = jnp.where(low, ones, block) if h == 0 else jnp.where(low, block, ones)
                term = dot(weights, right)
                summed = term if summed is None else summed + term
            acc_v[h] = summed
            m_v[h] = jnp.broadcast_to(top, (ROWS, LANES))

    def to_peer(n, src, dst):
        return pltpu.make_async_remote_copy(
            src_ref=src, dst_ref=dst, send_sem=psem.at[n], recv_sem=precv.at[n],
            device_id=(sp, peer), device_id_type=MESH,
        )

    wor_copy = to_peer(0, wor.at[pl.ds(0, LANES)], wor.at[pl.ds(LANES, LANES)])
    woa_copy = to_peer(1, woa.at[pl.ds(0, LANES)], woa.at[pl.ds(LANES, LANES)])
    def share_weights():
        loads["woa"].wait()
        loads["wor"].wait()
        await_entry(core == 0, 2, 0)
        start(None, wor_copy)
        start(None, woa_copy)

    def shard_of(back, up):
        return ((z + RING - back) % RING) * RING + (y + up) % RING

    def relay_z(valid, h, j, back):
        if back == 1:
            send((z == 1) & (core == 0) | (z == 2) & (core == 0), h, j, (sp + RING) % SHARDS)
        if back == 3:
            send((z == 3) & (core == 1), h, j, 2 * RING + y)

    def handle(h, back, up):
        j = shard_of(back, up)
        if back == 0:
            wanted = y + up >= RING
            if up == 1:
                wanted = wanted | (y == 0) & (core == 1)
            arrive(wanted if h else wanted | (z < 3), h, j)
            if up == 3:
                onward = (core == 0) & ((y == 1) | (y == 2))
                send(onward if h else onward | (core == 0) & (z < 3), h, j, y_up)
            if up == 1:
                onward = (core == 1) & ((y == 3) | (y == 0))
                send(onward if h else onward | (core == 1) & (z < 3), h, j, y_down)
            if h == 0:
                send_along_z(h, j)
            return
        valid = z >= back
        arrive(valid, h, j)
        if h == 0:
            relay_z(valid, h, j, back)
        elif up == 0:
            relay_z(valid, h, j, back)
            send_along_y(valid, h, j)
        elif up == 3:
            send((core == 0) & valid, h, j, y_up)
        elif up == 1:
            send((core == 1) & valid, h, j, y_down)
        if back == 1 and (h == 0 or up == 0):
            through = (z == 0) & (core == 1)
            jj = RING + (y + up) % RING
            arrive(through, h, jj)
            send(through, h, jj, 3 * RING + y)

    def attend_group(places):
        for at in range(RING):
            here = [p for p in places if p[0] <= at]

            @pl.when((z == at) & (y > 0) if all(b == 0 for b, _ in here) else z == at)
            def _():
                for back in dict.fromkeys(b for b, _ in here):
                    if back and back not in gated[at]:
                        gated[at].add(back)
                        gate_rows((z + RING - back) % RING, back).wait_recv()
                if here:
                    shown = [y + up >= RING if back == 0 else None for back, up in here]
                    attend([shard_of(*p) for p in here], shown=shown)

    gated = [set() for _ in range(RING)]

    def read_state(ref, j):
        tail = ref[j, LANES:].astype(F32)
        return ref[j, :LANES].astype(F32), tail[0:1] + tail[1:2] + tail[2:3]

    def combine_row():
        for n in range(1, RING):
            row_copy((y + n) % RING, sp, n).wait_recv()
        before, decay = jnp.zeros((LANES, LANES), F32), jnp.zeros((1, LANES), F32)
        mine, mine_decay = before, decay
        for k in range(RING):
            state, log = read_state(st_row, k)
            before = jnp.exp(log) * before + state
            decay = decay + log
            mine = jnp.where(k < y, before, mine)
            mine_decay = jnp.where(k < y, decay, mine_decay)
        in_v[0] = mine
        in_v[1, 0:1] = mine_decay
        body, tail = state_message(before, decay)
        st_col[z, :LANES] = body
        st_col[z, LANES:] = tail
        for n in range(1, RING):
            start(z + n < RING, col_copy(z, ((z + n) % RING) * RING + y, n))

    def combine_col():
        for n in range(1, RING):
            pl.when(z >= n)(col_copy((z + RING - n) % RING, sp, n).wait_recv)
        in_v[2] = jnp.zeros((LANES, LANES), F32)
        for k in range(RING - 1):

            @pl.when(k < z)
            def _():
                state, log = read_state(st_col, k)
                in_v[2] = jnp.exp(log) * in_v[2] + state

        incoming = jnp.exp(in_v[1, 0:1]) * in_v[2] + in_v[0]
        recurrent = rec_v[...] + dot_nt(visq_v[...], incoming.astype(BF16))
        mean = jnp.mean(recurrent * recurrent, axis=-1, keepdims=True)
        return (recurrent * lax.rsqrt(mean + EPSILON) * rg_v[...] * outgate_v[...]).astype(BF16)

    def by_owner(ref, rows):
        for b in range(8):
            ref[b % 2, 32 * (b // 2) : 32 * (b // 2) + 32, :] = rows[32 * b : 32 * b + 32]

    def share_recurrence():
        loads["rg"].wait()
        by_owner(act_r, combine_col())
        start(None, to_peer(2, act_r.at[1 - core], peer_r))

    def project_recurrence():
        wor_copy.wait_recv()
        to_peer(2, act_r.at[1 - core], peer_r).wait_recv()
        both = jnp.concatenate([act_r[core], peer_r[...]], axis=1)
        for c in range(CHUNKS):
            cols = slice(c * CHUNK, (c + 1) * CHUNK)
            product_v[:, cols] = dot(both, wor[:, cols]) + dot(act_a[core], woa[:LANES, cols])

    def handle_all(events):
        for h, back, up in events:
            handle(h, back, up)

    def share_gates():
        await_entry(z <= 1, 1, 2)
        for k in range(1, RING):
            gate_copy(z * RING + (y + k) % RING, k).wait_recv()
        for k in range(1, RING):
            start(z + k < RING, gate_rows(z, k))

    first_y()
    first_z()
    local = recurrence()
    last_y()
    share_row_gates()
    share_states()
    last_z()
    query_side(*local)
    handle_all((
        (1, 3, 0), (1, 1, 0), (0, 0, 3), (0, 0, 1), (0, 3, 0), (1, 2, 0), (1, 0, 1), (0, 1, 0),
    ))
    share_weights()
    handle_all((
        (0, 3, 3), (1, 3, 3),
    ))
    attend([sp], first=True)
    handle_all((
        (0, 1, 3),
    ))
    share_gates()
    handle_all((
        (0, 3, 1), (1, 0, 3), (1, 1, 3), (0, 0, 2),
    ))
    combine_row()
    handle_all((
        (1, 3, 1), (1, 1, 1), (0, 2, 0), (1, 2, 3), (1, 2, 1), (0, 1, 2), (1, 0, 2),
    ))
    attend_group(((0, 1), (0, 2), (0, 3)))
    handle_all((
        (0, 1, 1), (0, 3, 2), (1, 3, 2),
    ))
    attend_group(((3, 0), (3, 1), (3, 3), (3, 2)))
    handle_all((
        (1, 1, 2),
    ))
    attend_group(((1, 0), (1, 1), (1, 3), (1, 2)))
    share_recurrence()
    handle_all((
        (1, 2, 2), (0, 2, 3), (0, 2, 1), (0, 2, 2),
    ))
    attend_group(((2, 0), (2, 1), (2, 3), (2, 2)))

    a0, a1 = acc_v[0], acc_v[1]
    totals = jnp.where(low, a0, a1)
    loads["ag"].wait()
    attention = pltpu.roll(jnp.where(low, a1, a0), HALF, 1) / totals
    attn_out = half_rms(attention, ag_v[...]).astype(BF16)
    by_owner(act_a, attn_out)
    act_copy = to_peer(3, act_a.at[1 - core], peer_a)
    start(None, act_copy)
    await_entry(xc < 3, 2, 1)
    await_entry(xc == 0, 2, 3)
    project_recurrence()
    woa_copy.wait_recv()
    act_copy.wait_recv()

    far = (xc + 2) % RING
    sides = ((xc + 3) % RING, (xc + 1) % RING)

    def x_copy(kind, c, src, dst, target):
        return pltpu.make_async_remote_copy(
            src_ref=src, dst_ref=dst, send_sem=xsem.at[kind, c], recv_sem=xrecv.at[kind, c],
            device_id=(sp, target), device_id_type=MESH,
        )

    def transit(c):
        return x_copy(0, c, part.at[c, far], xt.at[c], 2 * sides[c % 2] + core)

    def direct(c):
        return x_copy(1, c, part.at[c, sides[1 - c % 2]], near.at[c], 2 * sides[1 - c % 2] + core)

    def summed(c):
        return x_copy(2, c, xsum.at[c], relayed.at[c], 2 * sides[c % 2] + core)

    theirs = peer_a[...]
    for c in range(CHUNKS):
        cols = slice(c * CHUNK, (c + 1) * CHUNK)
        product = product_v[:, cols] + dot(theirs, woa[LANES:, cols])
        for b in range(RING):
            part[c, b] = product[32 * b : 32 * b + 32].astype(BF16)
        start(None, transit(c))
    for c in range(CHUNKS):
        start(None, direct(c))
    log_sum = (jnp.where(low, m_v[0], m_v[1]) + jnp.log(totals)).T
    lse_ref[0:1, :] = log_sum[0:1, :] + gates[sp, 0:1, :]
    lse_ref[1:2, :] = log_sum[HALF : HALF + 1, :] + gates[sp, 1:2, :]
    for c in range(CHUNKS):
        transit(c).wait_recv()
        xsum[c] = (xt[c].astype(F32) + part[c, sides[c % 2]].astype(F32)).astype(BF16)
        start(None, summed(c))
    for c in range(CHUNKS):
        direct(c).wait_recv()
        summed(c).wait_recv()
        total = part[c, xc].astype(F32) + near[c].astype(F32) + relayed[c].astype(F32)
        mixed_ref[:, c * CHUNK : (c + 1) * CHUNK] = total.astype(BF16)
    for pred, cp in pending:
        if pred is None:
            cp.wait_send()
        else:
            pl.when(pred)(cp.wait_send)


def finish(mixed_v, lse_v, mixed_hbm, lse_hbm, sem):
    copies = [
        pltpu.make_async_copy(mixed_v, mixed_hbm, sem.at[0]),
        pltpu.make_async_copy(lse_v, lse_hbm, sem.at[1]),
    ]
    for cp in copies:
        cp.start()
    for cp in copies:
        cp.wait()


def body(*args):
    (
        layer_input_rows, input_norm_gain, query_weight, key_weight, value_weight, query_norm_gain,
        key_norm_gain, cumulative_gate, attention_norm_gain, recurrence_query_weight, forget_weight,
        recurrence_value_weight, output_gate_weight, gate_lower_slack, extra_log_decay,
        recurrence_norm_gain, attention_output_weight, recurrence_output_weight,
    ) = args
    operands = (
        layer_input_rows, input_norm_gain[None], query_weight, key_weight, value_weight,
        query_norm_gain[None], key_norm_gain[None], cumulative_gate.T, attention_norm_gain[None],
        recurrence_query_weight, forget_weight, recurrence_value_weight, output_gate_weight,
        gate_lower_slack[None], extra_log_decay.T, recurrence_norm_gain[None],
        attention_output_weight, recurrence_output_weight,
    )
    operands = [pltpu.with_memory_space_constraint(a, pltpu.HBM) for a in operands]
    dma = pltpu.SemaphoreType.DMA
    mixed, lse = pl.pallas_call(
        kernel,
        name="mixer",
        out_shape=(
            pltpu.VMEM((ROWS // 8, WIDTH), BF16),
            pltpu.VMEM((2, ROWS), F32),
        ),
        in_specs=[pl.BlockSpec(memory_space=pltpu.HBM)] * len(operands),
        out_specs=(pl.BlockSpec(memory_space=pltpu.VMEM),) * 2,
        scratch_shapes=[
            pltpu.VMEM((ROWS, WIDTH), BF16),
            pltpu.VMEM((ROWS, WIDTH), BF16),
            pltpu.VMEM((1, WIDTH), F32),
            pltpu.VMEM((1, HALF), F32),
            pltpu.VMEM((1, HALF), F32),
            pltpu.VMEM((1, LANES), F32),
            pltpu.VMEM((1, LANES), F32),
            pltpu.VMEM((1, ROWS), F32),
            pltpu.VMEM((1, LANES), F32),
            pltpu.VMEM((WIDTH, 2 * LANES), BF16),
            pltpu.VMEM((WIDTH, 2 * LANES), BF16),
            pltpu.VMEM((WIDTH, 2 * LANES), BF16),
            pltpu.VMEM((WIDTH, LANES), BF16),
            pltpu.VMEM((2 * LANES, WIDTH), BF16),
            pltpu.VMEM((2 * LANES, WIDTH), BF16),
            pltpu.VMEM((ROWS // 2, WIDTH), F32),
            pltpu.VMEM((SHARDS, 2, ROWS), F32),
            pltpu.VMEM((2, SHARDS, ROWS, LANES), BF16),
            pltpu.VMEM((2, ROWS, LANES), BF16),
            pltpu.VMEM((2, ROWS, LANES), F32),
            pltpu.VMEM((2, ROWS, LANES), F32),
            pltpu.VMEM((RING, STATE_MSG, LANES), BF16),
            pltpu.VMEM((RING, STATE_MSG, LANES), BF16),
            pltpu.VMEM((3, LANES, LANES), F32),
            pltpu.VMEM((ROWS, LANES), F32),
            pltpu.VMEM((ROWS, LANES), BF16),
            pltpu.VMEM((ROWS, LANES), F32),
            pltpu.VMEM((2, ROWS // 2, LANES), BF16),
            pltpu.VMEM((2, ROWS // 2, LANES), BF16),
            pltpu.VMEM((ROWS // 2, LANES), BF16),
            pltpu.VMEM((ROWS // 2, LANES), BF16),
            pltpu.VMEM((CHUNKS, RING, ROWS // 8, CHUNK), BF16),
            pltpu.VMEM((CHUNKS, ROWS // 8, CHUNK), BF16),
            pltpu.VMEM((CHUNKS, ROWS // 8, CHUNK), BF16),
            pltpu.VMEM((CHUNKS, ROWS // 8, CHUNK), BF16),
            pltpu.VMEM((CHUNKS, ROWS // 8, CHUNK), BF16),
            pltpu.SemaphoreType.REGULAR((3, RING)),
            dma((21,)),
            dma((2, RING)),
            dma((2, RING)),
            dma((KV_SENDS,)),
            dma((2, SHARDS)),
            dma((RING,)),
            dma((RING,)),
            dma((RING,)),
            dma((RING,)),
            dma((4,)),
            dma((4,)),
            dma((3, CHUNKS)),
            dma((3, CHUNKS)),
        ],
        compiler_params=pltpu.CompilerParams(
            collective_id=0, has_side_effects=True, vmem_limit_bytes=40 * 1024 * 1024
        ),
    )(*operands)
    mixed, lse = pl.pallas_call(
        finish,
        name="finish",
        out_shape=(
            jax.ShapeDtypeStruct((ROWS // 8, WIDTH), BF16),
            jax.ShapeDtypeStruct((2, ROWS), F32),
        ),
        in_specs=[pl.BlockSpec(memory_space=pltpu.VMEM)] * 2,
        out_specs=(pl.BlockSpec(memory_space=pltpu.HBM),) * 2,
        scratch_shapes=[pltpu.SemaphoreType.DMA((2,))],
    )(pltpu.with_memory_space_constraint(mixed, pltpu.VMEM), pltpu.with_memory_space_constraint(lse, pltpu.VMEM))
    return mixed, lse.T


def solution(mesh):
    both = P("sp", "tp")
    placed = (
        P("sp", None), P(), P(None, "tp"), P(None, "tp"), P(None, "tp"), P(), P(), both, P("tp"),
        P(None, "tp"), P(None, "tp"), P(None, "tp"), P(None, "tp"), P("tp"), both, P("tp"),
        P("tp", None), P("tp", None),
    )
    return jax.shard_map(
        body, mesh=mesh, in_specs=placed, out_specs=(P(("sp", "tp"), None), both), check_vma=False
    )
```

```python
import functools

import jax
import jax.numpy as jnp
from jax import lax
from jax.experimental import pallas as pl
from jax.experimental.pallas import tpu as pltpu
from jax.sharding import PartitionSpec as P

F32 = jnp.float32
BF16 = jnp.bfloat16
MESH = pl.DeviceIdType.MESH
EPSILON = 1e-06
ROWS = 256
WIDTH = 2048
LANES = 128
HALF = 64
SHARDS = 16
RING = 4
CHUNKS = 4
CHUNK = WIDTH // CHUNKS
STATE_MSG = 144
KV_SENDS = 80
NEGATIVE = -1e30


def dot(a, b):
    return jnp.dot(a, b, preferred_element_type=F32)


def dot_nt(a, b):
    return lax.dot_general(a, b, (((1,), (1,)), ((), ())), preferred_element_type=F32)


def split2(v):
    hi = v.astype(BF16)
    return hi, (v - hi.astype(F32)).astype(BF16)


def split3(v):
    hi = v.astype(BF16)
    rest = v - hi.astype(F32)
    mid = rest.astype(BF16)
    return hi, mid, (rest - mid.astype(F32)).astype(BF16)


def iota(shape, dim):
    return lax.broadcasted_iota(jnp.int32, shape, dim)


def kernel(
    x_hbm, xg_hbm, wq_hbm, wk_hbm, wv_hbm, qg_hbm, kg_hbm, gate_hbm, ag_hbm,
    wrq_hbm, wf_hbm, wrv_hbm, wog_hbm, slack_hbm, extra_hbm, rg_hbm, woa_hbm, wor_hbm,
    mixed_ref, lse_ref,
    x_v, n_v, xg_v, qg_v, kg_v, ag_v, slack_v, extra_v, rg_v,
    wkv, wfr, wqq, wog, woa, wor, product_v,
    gates, kv, q_v, m_v, acc_v,
    st_row, st_col, in_v, rec_v, visq_v, outgate_v,
    act_r, act_a, peer_r, peer_a, part, xt, near, relayed, xsum,
    entered, lsem, gsem, grecv, ssem, krecv, rsem, rrecv, csem, crecv, psem, precv, xsem, xrecv,
):
    sp = lax.axis_index("sp")
    tp = lax.axis_index("tp")
    z, y = sp // RING, sp % RING
    xc, core = tp // 2, tp % 2
    peer = 2 * xc + 1 - core

    loads = {}

    def load(name, src, dst):
        cp = pltpu.make_async_copy(src, dst, lsem.at[len(loads)])
        cp.start()
        loads[name] = cp

    for r in range(0, ROWS, HALF):
        load(("x", r), x_hbm.at[pl.ds(r, HALF)], x_v.at[pl.ds(r, HALF)])
    load("xg", xg_hbm, xg_v)
    load("wk", wk_hbm, wkv.at[:, pl.ds(0, LANES)])
    load("wv", wv_hbm, wkv.at[:, pl.ds(LANES, LANES)])
    load("kg", kg_hbm, kg_v)
    load("gate", gate_hbm, gates.at[sp])

    barrier = pltpu.get_barrier_semaphore()

    def along_y(k):
        return (z * RING + (y + k) % RING, tp)

    def along_z(k):
        return ((sp + RING * k) % SHARDS, tp)

    def along_x(k):
        return (sp, 2 * ((xc + k) % RING) + core)

    def greet(pred, device):
        @pl.when(pred)
        def _():
            pl.semaphore_signal(barrier, inc=1, device_id=device, device_id_type=MESH)

    def answer(pred, kind, k, device):
        @pl.when(pred)
        def _():
            pl.semaphore_signal(entered.at[kind, k], inc=1, device_id=device, device_id_type=MESH)

    def await_entry(pred, kind, k):
        @pl.when(pred)
        def _():
            pl.semaphore_wait(entered.at[kind, k], 1)

    for k in range(1, RING):
        greet(y + k < RING, along_y(k))
        greet(z + k < RING, along_z(k))
    greet(xc < 3, along_x(1))
    greet(xc == 0, along_x(3))
    greet(core == 0, (sp, peer))
    earlier = y + z + (xc + 3) // 4 + xc // 3 + core

    @pl.when(earlier > 0)
    def _():
        pl.semaphore_wait(barrier, earlier)

    for k in range(1, RING):
        answer(y >= k, 0, k, along_y(RING - k))
        answer(z >= k, 1, k, along_z(RING - k))
    answer(core == 1, 2, 0, (sp, peer))
    answer(xc > 0, 2, 1, along_x(3))
    answer(xc == 3, 2, 3, along_x(1))

    pending = []

    def start(pred, cp):
        if pred is None:
            cp.start()
        else:
            pl.when(pred)(cp.start)
        pending.append((pred, cp))

    loads["xg"].wait()
    step = 32
    for r in range(0, ROWS, step):
        if r % HALF == 0:
            loads["x", r].wait()
        if r == HALF:
            load("wf", wf_hbm, wfr.at[:, pl.ds(0, LANES)])
            load("wrv", wrv_hbm, wfr.at[:, pl.ds(LANES, LANES)])
            load("slack", slack_hbm, slack_v)
            load("extra", extra_hbm, extra_v)
            load("wq", wq_hbm, wqq.at[:, pl.ds(0, LANES)])
            load("wrq", wrq_hbm, wqq.at[:, pl.ds(LANES, LANES)])
            load("qg", qg_hbm, qg_v)
            load("wog", wog_hbm, wog)
            load("ag", ag_hbm, ag_v)
            load("rg", rg_hbm, rg_v)
            load("woa", woa_hbm, woa.at[pl.ds(0, LANES)])
            load("wor", wor_hbm, wor.at[pl.ds(0, LANES)])
        xf = x_v[r : r + step, :].astype(F32)
        mean = jnp.sum(xf * xf, axis=-1, keepdims=True) * (1.0 / WIDTH)
        n_v[r : r + step, :] = (xf * lax.rsqrt(mean + EPSILON) * xg_v[...]).astype(BF16)

    lane = iota((ROWS, LANES), 1)
    low = lane < HALF
    same_half = (iota((LANES, LANES), 0) // HALF == iota((LANES, LANES), 1) // HALF)
    halves = jnp.where(same_half, 1.0, 0.0).astype(BF16)

    def twice(gain):
        return jnp.concatenate([gain, gain], axis=1)

    def half_rms(v, gain):
        hi, lo = split2(v * v)
        mean = (dot(hi, halves) + dot(lo, halves)) * (1.0 / HALF)
        return v * lax.rsqrt(mean + EPSILON) * gain

    loads["wk"].wait()
    loads["wv"].wait()
    loads["kg"].wait()
    kv_f = dot(n_v[...], wkv[...])
    keys = half_rms(kv_f[:, :LANES], twice(kg_v[...]))
    swapped = pltpu.roll(kv_f[:, LANES:], HALF, 1)
    kv[0, sp] = jnp.where(low, keys, swapped).astype(BF16)
    kv[1, sp] = jnp.where(low, swapped, keys).astype(BF16)

    loads["gate"].wait()

    y_up = z * RING + (y + 1) % RING
    y_down = z * RING + (y + 3) % RING
    count = [0]

    def send(pred, h, j, target):
        n = count[0]
        count[0] += 1
        start(
            pred,
            pltpu.make_async_remote_copy(
                src_ref=kv.at[h, j], dst_ref=kv.at[h, j], send_sem=ssem.at[n], recv_sem=krecv.at[h, j],
                device_id=(target, tp), device_id_type=MESH,
            ),
        )

    def arrive(pred, h, j):
        cp = pltpu.make_async_remote_copy(
            src_ref=kv.at[h, j], dst_ref=kv.at[h, j], send_sem=ssem.at[0], recv_sem=krecv.at[h, j],
            device_id=(sp, peer), device_id_type=MESH,
        )
        if pred is None:
            cp.wait_recv()
        else:
            pl.when(pred)(cp.wait_recv)

    def send_along_z(h, j):
        send(z < 3, h, j, (sp + RING) % SHARDS)
        send(z == 0, h, j, 3 * RING + y)
        send((z == 1) & (core == 1), h, j, y)

    def send_along_y(pred, h, j):
        send(pred, h, j, y_up)
        send(pred, h, j, y_down)

    def gate_copy(j, k):
        return pltpu.make_async_remote_copy(
            src_ref=gates.at[j], dst_ref=gates.at[j], send_sem=gsem.at[0, k], recv_sem=grecv.at[0, j % RING],
            device_id=along_y(k), device_id_type=MESH,
        )

    def gate_rows(row, k):
        four = gates.at[pl.ds(row * RING, RING)]
        return pltpu.make_async_remote_copy(
            src_ref=four, dst_ref=four, send_sem=gsem.at[1, k], recv_sem=grecv.at[1, row],
            device_id=along_z(k), device_id_type=MESH,
        )

    row_at, col_at = iota((ROWS, ROWS), 0), iota((ROWS, ROWS), 1)
    causal = col_at <= row_at

    def state_message(state, decay):
        hi, mid, lo = (part.astype(F32) for part in split3(decay))
        at = iota((16, LANES), 0)
        tail = jnp.where(at == 0, hi, jnp.where(at == 1, mid, jnp.where(at == 2, lo, 0.0)))
        return state.astype(BF16), tail.astype(BF16)

    def row_copy(j, target, n):
        return pltpu.make_async_remote_copy(
            src_ref=st_row.at[j], dst_ref=st_row.at[j], send_sem=rsem.at[n], recv_sem=rrecv.at[j],
            device_id=(target, tp), device_id_type=MESH,
        )

    def col_copy(j, target, n):
        return pltpu.make_async_remote_copy(
            src_ref=st_col.at[j], dst_ref=st_col.at[j], send_sem=csem.at[n], recv_sem=crecv.at[j],
            device_id=(target, tp), device_id_type=MESH,
        )

    def first_y():
        await_entry(y < 3, 0, 1)
        send((y < 3) | (z < 3), 0, sp, y_up)
        send((y > 0) & (z < 3), 0, sp, y_down)
        send(y < 3, 1, sp, y_up)
        send((y == 1) & (core == 1), 1, sp, y_down)
        send((y == 1) & (core == 1) & (z == 3), 0, sp, y_down)

    def first_z():
        await_entry(z < 3, 1, 1)
        for h in (1, 0):
            send(z < 3, h, sp, (sp + RING) % SHARDS)
            send((z == 1) & (core == 1), h, sp, y)

    def last_y():
        await_entry(y == 0, 0, 3)
        send(y == 0, 0, sp, y_down)
        send(y == 0, 1, sp, y_down)

    def last_z():
        await_entry(z == 0, 1, 3)
        for h in (1, 0):
            send(z == 0, h, sp, 3 * RING + y)

    def share_row_gates():
        await_entry(y <= 1, 0, 2)
        for k in range(1, RING):
            start(None, gate_copy(sp, k))

    def share_states():
        for n in range(1, RING):
            start(None, row_copy(y, z * RING + (y + n) % RING, n))

    def recurrence():
        loads["wf"].wait()
        loads["wrv"].wait()
        loads["slack"].wait()
        loads["extra"].wait()
        fr = dot(n_v[...], wfr[...])
        forget = slack_v[...] * (1.0 / (1.0 + jnp.exp(fr[:, :LANES])))
        rec_value = fr[:, LANES:].astype(BF16)
        extra = jnp.broadcast_to(extra_v[...], (LANES, ROWS)).T
        lower_tri = jnp.where(causal, 1.0, 0.0).astype(BF16)
        sums = dot(lower_tri, jnp.concatenate(split3(jnp.log1p(-forget)) + split3(extra), axis=1))
        share_sum = sums[:, :LANES] + sums[:, LANES : 2 * LANES] + sums[:, 2 * LANES : 3 * LANES]
        extra_sum = sums[:, 3 * LANES : 4 * LANES] + sums[:, 4 * LANES : 5 * LANES] + sums[:, 5 * LANES :]
        share_end = share_sum[ROWS - 1 :, :]
        extra_end = extra_sum[ROWS - 1 :, :]
        closing = (forget * jnp.exp((share_end - share_sum) + (extra_end - extra_sum))).astype(BF16)
        state_t = dot(fr[:, LANES:].T.astype(BF16), closing)

        body, tail = state_message(state_t, share_end + extra_end)
        st_row[y, :LANES] = body
        st_row[y, LANES:] = tail
        return forget, rec_value, share_sum, extra_sum

    def query_side(forget, rec_value, share_sum, extra_sum):
        loads["wq"].wait()
        loads["wrq"].wait()
        loads["qg"].wait()
        qq = dot(n_v[...], wqq[...])
        queries = (half_rms(qq[:, :LANES], twice(qg_v[...])).astype(BF16).astype(F32)) * (HALF**-0.5)
        q_v[0] = jnp.where(low, queries, 0.0).astype(BF16)
        q_v[1] = jnp.where(low, 0.0, queries).astype(BF16)

        rq = qq[:, LANES:]
        rec_query = rq / (1.0 + jnp.exp(-rq))
        scores = dot_nt((rec_query * jnp.exp(share_sum)).astype(BF16), (forget * jnp.exp(-share_sum)).astype(BF16))
        differ = jnp.concatenate([extra_sum, extra_sum], axis=1) - extra_sum.T[:1, :]
        scores = scores * jnp.exp(jnp.where(causal, differ, NEGATIVE))
        rec_v[...] = dot(scores.astype(BF16), rec_value)
        visq_v[...] = (rec_query * jnp.exp(share_sum + extra_sum)).astype(BF16)

        loads["wog"].wait()
        og = dot(n_v[...], wog[...])
        outgate_v[...] = og / (1.0 + jnp.exp(-og))

    def attend(blocks, first=False, shown=None):
        def keys_of(h, i, j):
            block = kv[h, j]
            return block if shown is None or shown[i] is None else jnp.where(shown[i], block, jnp.zeros_like(block))

        for h in range(2):
            parts = []
            for i, j in enumerate(blocks):
                gate = gates[j, h : h + 1, :]
                if shown is not None and shown[i] is not None:
                    gate = jnp.where(shown[i], gate, -NEGATIVE)
                part = dot_nt(q_v[h], keys_of(h, i, j)) - gate
                parts.append(jnp.where(causal, part, NEGATIVE) if first else part)
            widest = parts[0]
            for part in parts[1:]:
                widest = jnp.maximum(widest, part)
            top = jnp.max(widest, axis=-1, keepdims=True)
            if not first:
                old = m_v[h]
                top = jnp.maximum(old[:, :1], top)
            summed = None if first else acc_v[h] * jnp.exp(old - top)
            for i, (part, j) in enumerate(zip(parts, blocks)):
                weights = jnp.exp(part - top).astype(BF16)
                block = keys_of(h, i, j)
                ones = jnp.ones_like(block)
                right = jnp.where(low, ones, block) if h == 0 else jnp.where(low, block, ones)
                term = dot(weights, right)
                summed = term if summed is None else summed + term
            acc_v[h] = summed
            m_v[h] = jnp.broadcast_to(top, (ROWS, LANES))

    def to_peer(n, src, dst):
        return pltpu.make_async_remote_copy(
            src_ref=src, dst_ref=dst, send_sem=psem.at[n], recv_sem=precv.at[n],
            device_id=(sp, peer), device_id_type=MESH,
        )

    wor_copy = to_peer(0, wor.at[pl.ds(0, LANES)], wor.at[pl.ds(LANES, LANES)])
    woa_copy = to_peer(1, woa.at[pl.ds(0, LANES)], woa.at[pl.ds(LANES, LANES)])
    def share_weights():
        loads["woa"].wait()
        loads["wor"].wait()
        await_entry(core == 0, 2, 0)
        start(None, wor_copy)
        start(None, woa_copy)

    def shard_of(back, up):
        return ((z + RING - back) % RING) * RING + (y + up) % RING

    def relay_z(valid, h, j, back):
        if back == 1:
            send((z == 1) & (core == 0) | (z == 2) & (core == 0), h, j, (sp + RING) % SHARDS)
        if back == 3:
            send((z == 3) & (core == 1), h, j, 2 * RING + y)

    def handle(h, back, up):
        j = shard_of(back, up)
        if back == 0:
            wanted = y + up >= RING
            if up == 1:
                wanted = wanted | (y == 0) & (core == 1)
            arrive(wanted if h else wanted | (z < 3), h, j)
            if up == 3:
                onward = (core == 0) & ((y == 1) | (y == 2))
                send(onward if h else onward | (core == 0) & (z < 3), h, j, y_up)
            if up == 1:
                onward = (core == 1) & ((y == 3) | (y == 0))
                send(onward if h else onward | (core == 1) & (z < 3), h, j, y_down)
            if h == 0:
                send_along_z(h, j)
            return
        valid = z >= back
        arrive(valid, h, j)
        if h == 0:
            relay_z(valid, h, j, back)
        elif up == 0:
            relay_z(valid, h, j, back)
            send_along_y(valid, h, j)
        elif up == 3:
            send((core == 0) & valid, h, j, y_up)
        elif up == 1:
            send((core == 1) & valid, h, j, y_down)
        if back == 1 and (h == 0 or up == 0):
            through = (z == 0) & (core == 1)
            jj = RING + (y + up) % RING
            arrive(through, h, jj)
            send(through, h, jj, 3 * RING + y)

    def attend_group(places):
        kinds = {}
        for at in range(RING):
            kinds.setdefault(tuple(p for p in places if p[0] <= at), []).append(at)
        for here, zs in kinds.items():
            at = zs[0]
            inside = (z >= at) & (z <= zs[-1])

            @pl.when(inside & (y > 0) if all(b == 0 for b, _ in here) else inside)
            def _():
                for back in dict.fromkeys(b for b, _ in here):
                    if back:
                        gate_rows((z + RING - back) % RING, back).wait_recv()
                if here:
                    shown = [y + up >= RING if back == 0 else None for back, up in here]
                    attend([shard_of(*p) for p in here], shown=shown)


    def read_state(ref, j):
        tail = ref[j, LANES:].astype(F32)
        return ref[j, :LANES].astype(F32), tail[0:1] + tail[1:2] + tail[2:3]

    def combine_row():
        for n in range(1, RING):
            row_copy((y + n) % RING, sp, n).wait_recv()
        before, decay = jnp.zeros((LANES, LANES), F32), jnp.zeros((1, LANES), F32)
        mine, mine_decay = before, decay
        for k in range(RING):
            state, log = read_state(st_row, k)
            before = jnp.exp(log) * before + state
            decay = decay + log
            mine = jnp.where(k < y, before, mine)
            mine_decay = jnp.where(k < y, decay, mine_decay)
        in_v[0] = mine
        in_v[1, 0:1] = mine_decay
        body, tail = state_message(before, decay)
        st_col[z, :LANES] = body
        st_col[z, LANES:] = tail
        for n in range(1, RING):
            start(z + n < RING, col_copy(z, ((z + n) % RING) * RING + y, n))

    def combine_col():
        for n in range(1, RING):
            pl.when(z >= n)(col_copy((z + RING - n) % RING, sp, n).wait_recv)
        in_v[2] = jnp.zeros((LANES, LANES), F32)
        for k in range(RING - 1):

            @pl.when(k < z)
            def _():
                state, log = read_state(st_col, k)
                in_v[2] = jnp.exp(log) * in_v[2] + state

        incoming = jnp.exp(in_v[1, 0:1]) * in_v[2] + in_v[0]
        recurrent = rec_v[...] + dot_nt(visq_v[...], incoming.astype(BF16))
        mean = jnp.mean(recurrent * recurrent, axis=-1, keepdims=True)
        return (recurrent * lax.rsqrt(mean + EPSILON) * rg_v[...] * outgate_v[...]).astype(BF16)

    def by_owner(ref, rows):
        for b in range(8):
            ref[b % 2, 32 * (b // 2) : 32 * (b // 2) + 32, :] = rows[32 * b : 32 * b + 32]

    def share_recurrence():
        loads["rg"].wait()
        by_owner(act_r, combine_col())
        start(None, to_peer(2, act_r.at[1 - core], peer_r))

    def project_recurrence():
        wor_copy.wait_recv()
        to_peer(2, act_r.at[1 - core], peer_r).wait_recv()
        both = jnp.concatenate([act_r[core], peer_r[...]], axis=1)
        for c in range(CHUNKS):
            cols = slice(c * CHUNK, (c + 1) * CHUNK)
            product_v[:, cols] = dot(both, wor[:, cols]) + dot(act_a[core], woa[:LANES, cols])

    def handle_all(events):
        for h, back, up in events:
            handle(h, back, up)

    def share_gates():
        await_entry(z <= 1, 1, 2)
        for k in range(1, RING):
            gate_copy(z * RING + (y + k) % RING, k).wait_recv()
        for k in range(1, RING):
            start(z + k < RING, gate_rows(z, k))

    first_y()
    first_z()
    local = recurrence()
    last_y()
    share_row_gates()
    share_states()
    last_z()
    query_side(*local)
    handle_all((
        (1, 3, 0), (1, 1, 0), (0, 0, 3), (0, 0, 1), (0, 3, 0), (1, 2, 0), (1, 0, 1), (0, 1, 0),
    ))
    share_weights()
    handle_all((
        (0, 3, 3), (1, 3, 3),
    ))
    attend([sp], first=True)
    handle_all((
        (0, 1, 3),
    ))
    share_gates()
    handle_all((
        (0, 3, 1), (1, 0, 3), (1, 1, 3), (0, 0, 2),
    ))
    combine_row()
    handle_all((
        (1, 3, 1), (1, 1, 1), (0, 2, 0), (1, 2, 3), (1, 2, 1), (0, 1, 2), (1, 0, 2),
    ))
    attend_group(((0, 1), (0, 2), (0, 3)))
    handle_all((
        (0, 1, 1), (0, 3, 2), (1, 3, 2),
    ))
    attend_group(((3, 0), (3, 1), (3, 3), (3, 2)))
    handle_all((
        (1, 1, 2),
    ))
    attend_group(((1, 0), (1, 1), (1, 3), (1, 2)))
    share_recurrence()
    handle_all((
        (1, 2, 2), (0, 2, 3), (0, 2, 1), (0, 2, 2),
    ))
    attend_group(((2, 0), (2, 1), (2, 3), (2, 2)))

    a0, a1 = acc_v[0], acc_v[1]
    totals = jnp.where(low, a0, a1)
    loads["ag"].wait()
    attention = pltpu.roll(jnp.where(low, a1, a0), HALF, 1) / totals
    attn_out = half_rms(attention, ag_v[...]).astype(BF16)
    by_owner(act_a, attn_out)
    act_copy = to_peer(3, act_a.at[1 - core], peer_a)
    start(None, act_copy)
    await_entry(xc < 3, 2, 1)
    await_entry(xc == 0, 2, 3)
    project_recurrence()
    woa_copy.wait_recv()
    act_copy.wait_recv()

    far = (xc + 2) % RING
    sides = ((xc + 3) % RING, (xc + 1) % RING)

    def x_copy(kind, c, src, dst, target):
        return pltpu.make_async_remote_copy(
            src_ref=src, dst_ref=dst, send_sem=xsem.at[kind, c], recv_sem=xrecv.at[kind, c],
            device_id=(sp, target), device_id_type=MESH,
        )

    def transit(c):
        return x_copy(0, c, part.at[c, far], xt.at[c], 2 * sides[c % 2] + core)

    def direct(c):
        return x_copy(1, c, part.at[c, sides[1 - c % 2]], near.at[c], 2 * sides[1 - c % 2] + core)

    def summed(c):
        return x_copy(2, c, xsum.at[c], relayed.at[c], 2 * sides[c % 2] + core)

    theirs = peer_a[...]
    for c in range(CHUNKS):
        cols = slice(c * CHUNK, (c + 1) * CHUNK)
        product = product_v[:, cols] + dot(theirs, woa[LANES:, cols])
        for b in range(RING):
            part[c, b] = product[32 * b : 32 * b + 32].astype(BF16)
        start(None, transit(c))
    for c in range(CHUNKS):
        start(None, direct(c))
    log_sum = (jnp.where(low, m_v[0], m_v[1]) + jnp.log(totals)).T
    lse_ref[0:1, :] = log_sum[0:1, :] + gates[sp, 0:1, :]
    lse_ref[1:2, :] = log_sum[HALF : HALF + 1, :] + gates[sp, 1:2, :]
    for c in range(CHUNKS):
        transit(c).wait_recv()
        xsum[c] = (xt[c].astype(F32) + part[c, sides[c % 2]].astype(F32)).astype(BF16)
        start(None, summed(c))
    for c in range(CHUNKS):
        direct(c).wait_recv()
        summed(c).wait_recv()
        total = part[c, xc].astype(F32) + near[c].astype(F32) + relayed[c].astype(F32)
        mixed_ref[:, c * CHUNK : (c + 1) * CHUNK] = total.astype(BF16)
    for pred, cp in pending:
        if pred is None:
            cp.wait_send()
        else:
            pl.when(pred)(cp.wait_send)


def finish(mixed_v, lse_v, mixed_hbm, lse_hbm, sem):
    copies = [
        pltpu.make_async_copy(mixed_v, mixed_hbm, sem.at[0]),
        pltpu.make_async_copy(lse_v, lse_hbm, sem.at[1]),
    ]
    for cp in copies:
        cp.start()
    for cp in copies:
        cp.wait()


def body(*args):
    (
        layer_input_rows, input_norm_gain, query_weight, key_weight, value_weight, query_norm_gain,
        key_norm_gain, cumulative_gate, attention_norm_gain, recurrence_query_weight, forget_weight,
        recurrence_value_weight, output_gate_weight, gate_lower_slack, extra_log_decay,
        recurrence_norm_gain, attention_output_weight, recurrence_output_weight,
    ) = args
    operands = (
        layer_input_rows, input_norm_gain[None], query_weight, key_weight, value_weight,
        query_norm_gain[None], key_norm_gain[None], cumulative_gate.T, attention_norm_gain[None],
        recurrence_query_weight, forget_weight, recurrence_value_weight, output_gate_weight,
        gate_lower_slack[None], extra_log_decay.T, recurrence_norm_gain[None],
        attention_output_weight, recurrence_output_weight,
    )
    operands = [pltpu.with_memory_space_constraint(a, pltpu.HBM) for a in operands]
    dma = pltpu.SemaphoreType.DMA
    mixed, lse = pl.pallas_call(
        kernel,
        name="mixer",
        out_shape=(
            pltpu.VMEM((ROWS // 8, WIDTH), BF16),
            pltpu.VMEM((2, ROWS), F32),
        ),
        in_specs=[pl.BlockSpec(memory_space=pltpu.HBM)] * len(operands),
        out_specs=(pl.BlockSpec(memory_space=pltpu.VMEM),) * 2,
        scratch_shapes=[
            pltpu.VMEM((ROWS, WIDTH), BF16),
            pltpu.VMEM((ROWS, WIDTH), BF16),
            pltpu.VMEM((1, WIDTH), F32),
            pltpu.VMEM((1, HALF), F32),
            pltpu.VMEM((1, HALF), F32),
            pltpu.VMEM((1, LANES), F32),
            pltpu.VMEM((1, LANES), F32),
            pltpu.VMEM((1, ROWS), F32),
            pltpu.VMEM((1, LANES), F32),
            pltpu.VMEM((WIDTH, 2 * LANES), BF16),
            pltpu.VMEM((WIDTH, 2 * LANES), BF16),
            pltpu.VMEM((WIDTH, 2 * LANES), BF16),
            pltpu.VMEM((WIDTH, LANES), BF16),
            pltpu.VMEM((2 * LANES, WIDTH), BF16),
            pltpu.VMEM((2 * LANES, WIDTH), BF16),
            pltpu.VMEM((ROWS // 2, WIDTH), F32),
            pltpu.VMEM((SHARDS, 2, ROWS), F32),
            pltpu.VMEM((2, SHARDS, ROWS, LANES), BF16),
            pltpu.VMEM((2, ROWS, LANES), BF16),
            pltpu.VMEM((2, ROWS, LANES), F32),
            pltpu.VMEM((2, ROWS, LANES), F32),
            pltpu.VMEM((RING, STATE_MSG, LANES), BF16),
            pltpu.VMEM((RING, STATE_MSG, LANES), BF16),
            pltpu.VMEM((3, LANES, LANES), F32),
            pltpu.VMEM((ROWS, LANES), F32),
            pltpu.VMEM((ROWS, LANES), BF16),
            pltpu.VMEM((ROWS, LANES), F32),
            pltpu.VMEM((2, ROWS // 2, LANES), BF16),
            pltpu.VMEM((2, ROWS // 2, LANES), BF16),
            pltpu.VMEM((ROWS // 2, LANES), BF16),
            pltpu.VMEM((ROWS // 2, LANES), BF16),
            pltpu.VMEM((CHUNKS, RING, ROWS // 8, CHUNK), BF16),
            pltpu.VMEM((CHUNKS, ROWS // 8, CHUNK), BF16),
            pltpu.VMEM((CHUNKS, ROWS // 8, CHUNK), BF16),
            pltpu.VMEM((CHUNKS, ROWS // 8, CHUNK), BF16),
            pltpu.VMEM((CHUNKS, ROWS // 8, CHUNK), BF16),
            pltpu.SemaphoreType.REGULAR((3, RING)),
            dma((21,)),
            dma((2, RING)),
            dma((2, RING)),
            dma((KV_SENDS,)),
            dma((2, SHARDS)),
            dma((RING,)),
            dma((RING,)),
            dma((RING,)),
            dma((RING,)),
            dma((4,)),
            dma((4,)),
            dma((3, CHUNKS)),
            dma((3, CHUNKS)),
        ],
        compiler_params=pltpu.CompilerParams(
            collective_id=0, has_side_effects=True, vmem_limit_bytes=40 * 1024 * 1024
        ),
    )(*operands)
    mixed, lse = pl.pallas_call(
        finish,
        name="finish",
        out_shape=(
            jax.ShapeDtypeStruct((ROWS // 8, WIDTH), BF16),
            jax.ShapeDtypeStruct((2, ROWS), F32),
        ),
        in_specs=[pl.BlockSpec(memory_space=pltpu.VMEM)] * 2,
        out_specs=(pl.BlockSpec(memory_space=pltpu.HBM),) * 2,
        scratch_shapes=[pltpu.SemaphoreType.DMA((2,))],
    )(pltpu.with_memory_space_constraint(mixed, pltpu.VMEM), pltpu.with_memory_space_constraint(lse, pltpu.VMEM))
    return mixed, lse.T


def solution(mesh):
    both = P("sp", "tp")
    placed = (
        P("sp", None), P(), P(None, "tp"), P(None, "tp"), P(None, "tp"), P(), P(), both, P("tp"),
        P(None, "tp"), P(None, "tp"), P(None, "tp"), P(None, "tp"), P("tp"), both, P("tp"),
        P("tp", None), P("tp", None),
    )
    return jax.shard_map(
        body, mesh=mesh, in_specs=placed, out_specs=(P(("sp", "tp"), None), both), check_vma=False
    )
```
